512 devices in a mesh: sp: 16 (over z), fs: 4 (over y), tp: 8 (over x, core).
Axes of the slice: x: 4, y: 4, z: 16, core: 2. Of those that a mesh axis runs over, the one named last changes fastest.
Arguments:
- tokens: bfloat16 [4, 4096, 2048], P('fs', 'sp'), may hold values from -6 to 6
- norm_gain: float32 [2048], replicated, may hold values from 0.1 to 1.9
- query_weight: bfloat16 [2048, 1024], P(('sp', 'fs'), 'tp'), may hold values from -0.125 to 0.125
- key_weight: bfloat16 [2048, 1024], P(('sp', 'fs'), 'tp'), may hold values from -0.125 to 0.125
- value_weight: bfloat16 [2048, 1024], P(('sp', 'fs'), 'tp'), may hold values from -0.125 to 0.125
- outgate_weight: bfloat16 [2048, 1024], P(('sp', 'fs'), 'tp'), may hold values from -0.125 to 0.125
- gate_weight: bfloat16 [4, 8, 2048], P(None, 'tp'), may hold values from -0.125 to 0.125
- gate_bias: float32 [4, 8], P(None, 'tp'), may hold values from -1 to 100
- decay_extra: float32 [4, 2, 8, 4096], P('fs', None, 'tp', 'sp'), may hold values from -0.75 to 0
- init_memory: float32 [4, 2, 8, 128, 128], P('fs', None, 'tp'), may hold values from -96 to 96
- init_normalizer: float32 [4, 2, 8, 128], P('fs', None, 'tp'), may hold values from -96 to 96
- head_gain: float32 [8, 128], P('tp'), may hold values from 0.1 to 1.9
- pool_weight: bfloat16 [2048, 2048], P(('sp', 'fs'), 'tp'), may hold values from -0.125 to 0.125
- mem_out_weight: bfloat16 [2048, 1024], P(('sp', 'fs'), 'tp'), may hold values from -0.1875 to 0.1875
- pool_out_weight: bfloat16 [2048, 2048], P(('sp', 'fs'), 'tp'), may hold values from -0.125 to 0.125
Outputs:
- mixed: bfloat16 [4, 4096, 2048], P('fs', ('sp', 'tp'))
The draws below stay inside these ranges and needn't reach their ends.
All inputs are finite; a program needn't handle non-finite values.
Results may differ from the reference program's by a relative error of at most 0.014.
Values may be sent and summed in bfloat16 or wider, within the bound.
No kernel may reach another device: no remote copies, remote signals or barrier semaphores. Data moves between devices by JAX's collectives and lax.ppermute only.
A program may use at most 64 MiB of HBM per device.

```python
import math
from functools import partial
import jax
import jax.numpy as jnp
from jax import lax

D = 2048
MEMORY_HEADS = 8
HEAD_DIM = 128
HALO = 8
T_DEV = 256
MEM_W = 1024
TOKEN_LENGTH = 4096
SEQUENCE_COUNT = 4
N_TP = 8


def draw_gate_bias(key, part):
    rank_key, slow_key, fast_key, input_key, pick_key, strong_key = jax.random.split(key, 6)
    ranking = jax.random.permutation(rank_key, MEMORY_HEADS)
    picking = jax.random.permutation(pick_key, MEMORY_HEADS)
    slow_heads = ranking < MEMORY_HEADS // 2
    strong_heads = picking < 0
    slow_bias = math.log(3.3 * TOKEN_LENGTH) + jax.random.uniform(slow_key, (2, MEMORY_HEADS), jnp.float32, 0.0, 0.5)
    fast_bias = jax.random.uniform(fast_key, (2, MEMORY_HEADS), jnp.float32, math.log(50.0), math.log(165.0))
    forget_bias = jnp.where(slow_heads[None, :], slow_bias, fast_bias)
    gentle = jax.random.uniform(input_key, (2, MEMORY_HEADS), jnp.float32, -1.0, 1.0)
    strong_bias = jax.random.uniform(strong_key, (2, MEMORY_HEADS), jnp.float32, 80.0, 100.0)
    input_bias = jnp.where(strong_heads[None, :], strong_bias, gentle)
    return jnp.stack([input_bias[0], forget_bias[0], input_bias[1], forget_bias[1]]).astype(jnp.float32)


def draw_decay_extra(key, part):
    speed_key, spike_key, penalty_key = jax.random.split(key, 3)
    block_count = TOKEN_LENGTH // T_DEV
    rates = jnp.exp(jax.random.uniform(speed_key, (SEQUENCE_COUNT, 2, MEMORY_HEADS, block_count), jnp.float32, math.log(0.25), math.log(2.0)))
    stable_values = -0.5 / TOKEN_LENGTH * jnp.repeat(rates, T_DEV, axis=-1)
    spike_values = jax.random.bernoulli(spike_key, 2.0 / TOKEN_LENGTH, (SEQUENCE_COUNT, 2, MEMORY_HEADS, TOKEN_LENGTH))
    penalty_values = jax.random.uniform(penalty_key, (SEQUENCE_COUNT, 2, MEMORY_HEADS, TOKEN_LENGTH), jnp.float32, math.log(0.5), math.log(0.8))
    return (stable_values + jnp.where(spike_values, penalty_values, 0.0)).astype(jnp.float32)


def shard_levels(rng, shape, shards, least, high):
    def one(position, shards_of):
        steps = jax.random.uniform(jax.random.fold_in(jax.random.fold_in(rng, 6), position), (shards_of,), jnp.float32, least / len(shards), high / len(shards))
        return jnp.repeat(jnp.exp(steps), shape[position] // shards_of).reshape((-1,) + (1,) * (len(shape) - position - 1))

    level = one(*shards[0])
    for cut in shards[1:]:
        level = level * one(*cut)
    return level


def gaussian(key, extent, spread, bound, cuts=(), held_as=jnp.bfloat16):
    gain = shard_levels(key, extent, cuts, -0.22, 0.18) if cuts else 1.0
    drawn = jax.random.normal(key, extent, jnp.float32) * spread * gain
    return jnp.minimum(jnp.maximum(drawn, -bound), bound).astype(held_as)


def setup_inputs(seed: int = 0) -> dict:
    streams_of = jax.random.split(jax.random.key(seed), 16)
    tokens = gaussian(streams_of[0], (SEQUENCE_COUNT, TOKEN_LENGTH, D), 1.0, 6.0, ((0, 4), (1, 16)))
    norm_gain = jnp.clip(1.0 + 0.18 * jax.random.normal(streams_of[1], (D,), jnp.float32), 0.1, 1.9)
    query_weight = gaussian(streams_of[2], (D, MEM_W), D ** -0.5, 0.125, ((0, 64), (1, 8)))
    key_weight = gaussian(streams_of[3], (D, MEM_W), D ** -0.5, 0.125, ((0, 64), (1, 8)))
    value_weight = gaussian(streams_of[4], (D, MEM_W), D ** -0.5, 0.125, ((0, 64), (1, 8)))
    outgate_weight = gaussian(streams_of[5], (D, MEM_W), D ** -0.5, 0.125, ((0, 64), (1, 8)))
    gate_weight = gaussian(streams_of[6], (4, MEMORY_HEADS, D), D ** -0.5, 0.125, ((1, 8),))
    gate_bias = draw_gate_bias(jax.random.fold_in(streams_of[15], 71), 0)
    decay_extra = draw_decay_extra(jax.random.fold_in(streams_of[15], 71), 0)
    init_memory = gaussian(streams_of[9], (SEQUENCE_COUNT, 2, MEMORY_HEADS, HEAD_DIM, HEAD_DIM), (0.25 * TOKEN_LENGTH ** 0.5), 96.0, ((0, 4), (2, 8)), jnp.float32)
    init_normalizer = gaussian(streams_of[10], (SEQUENCE_COUNT, 2, MEMORY_HEADS, HEAD_DIM), (0.25 * TOKEN_LENGTH ** 0.5), 96.0, ((0, 4), (2, 8)), jnp.float32)
    head_gain = jnp.clip(1.0 + 0.18 * jax.random.normal(streams_of[11], (MEMORY_HEADS, HEAD_DIM), jnp.float32), 0.1, 1.9)
    pool_weight = gaussian(streams_of[12], (D, D), D ** -0.5, 0.125, ((0, 64), (1, 8)))
    mem_out_weight = gaussian(streams_of[13], (D, MEM_W), MEM_W ** -0.5, 0.1875, ((0, 64), (1, 8)))
    pool_out_weight = gaussian(streams_of[14], (D, D), D ** -0.5, 0.125, ((0, 64), (1, 8)))
    return dict(tokens=tokens, norm_gain=norm_gain, query_weight=query_weight, key_weight=key_weight, value_weight=value_weight, outgate_weight=outgate_weight, gate_weight=gate_weight, gate_bias=gate_bias, decay_extra=decay_extra, init_memory=init_memory, init_normalizer=init_normalizer, head_gain=head_gain, pool_weight=pool_weight, mem_out_weight=mem_out_weight, pool_out_weight=pool_out_weight)


norm_eps = 1e-06
exact_mode = lax.Precision.HIGHEST

def block_output(query_rows, key_rows, value_rows, input_gate, log_forget, memory, normalizer, stabilizer):
    block_len = query_rows.shape[1]
    key_scale = key_rows.shape[-1] ** (-0.5)
    lower_mask = jnp.tril(jnp.ones((block_len, block_len), dtype=bool))
    summed = jnp.cumsum(log_forget, axis=-1)
    log_decay = jnp.where(lower_mask, summed[:, :, None] - summed[:, None, :] + input_gate[:, None, :], -jnp.inf)
    log_carry = stabilizer[:, None] + summed
    running_max = jnp.maximum(log_carry, lax.optimization_barrier(jnp.max(log_decay, axis=-1)))
    query_wide = query_rows.astype(jnp.float32)
    scores = jnp.einsum('btd,bsd->bts', query_wide, key_rows.astype(jnp.float32), precision=exact_mode) * key_scale
    inner_weight = jnp.exp(log_decay - running_max[:, :, None]) * scores
    weight_rounded = lax.optimization_barrier(inner_weight.astype(jnp.bfloat16))
    carry_weight = jnp.exp(log_carry - running_max)
    numerator = carry_weight[:, :, None] * jnp.einsum('bed,btd->bte', memory, query_wide, precision=exact_mode)
    numerator = numerator + jnp.einsum('bts,bse->bte', weight_rounded.astype(jnp.float32), value_rows.astype(jnp.float32), precision=exact_mode)
    denominator = carry_weight * jnp.einsum('bd,btd->bt', normalizer, query_wide, precision=exact_mode)
    denominator = denominator + lax.optimization_barrier(jnp.sum(inner_weight, axis=-1))
    return numerator / jnp.maximum(jnp.abs(denominator), jnp.exp(-running_max))[:, :, None]

def block_summary(key_rows, value_rows, input_gate, log_forget):
    key_wide = key_rows.astype(jnp.float32) * key_rows.shape[-1] ** (-0.5)
    summed = jnp.cumsum(log_forget, axis=-1)
    forget_total = summed[:, -1]
    log_weight = forget_total[:, None] - summed + input_gate
    running_max = lax.optimization_barrier(jnp.max(log_weight, axis=-1))
    weights = jnp.exp(log_weight - running_max[:, None])
    memory = jnp.einsum('bse,bsd->bed', weights[:, :, None] * value_rows.astype(jnp.float32), key_wide, precision=exact_mode)
    normalizer = jnp.einsum('bs,bsd->bd', weights, key_wide, precision=exact_mode)
    return (memory, normalizer, running_max, forget_total)

def combine(earlier, latter):
    early_memory, early_norm, early_max, early_total = earlier
    late_memory, late_norm, late_max, late_total = latter
    joint_max = jnp.maximum(early_max + late_total, late_max)
    early_scale = jnp.exp(early_max + late_total - joint_max)
    late_scale = jnp.exp(late_max - joint_max)
    memory = early_scale[:, None, None] * early_memory + late_scale[:, None, None] * late_memory
    normalizer = early_scale[:, None] * early_norm + late_scale[:, None] * late_norm
    return (memory, normalizer, joint_max, early_total + late_total)

def span_sweep(query_rows, key_rows, value_rows, input_gate, log_forget, memory, normalizer, stabilizer, span):
    block_count = query_rows.shape[1] // span

    def to_blocks(array):
        shaped = array.reshape((array.shape[0], block_count, span) + array.shape[2:])
        return jnp.moveaxis(shaped, 1, 0)

    def advance(carried, pieces):
        query_blk, key_blk, value_blk, gate_blk, forget_blk = pieces
        result = block_output(query_blk, key_blk, value_blk, gate_blk, forget_blk, carried[0], carried[1], carried[2])
        return (combine(carried, block_summary(key_blk, value_blk, gate_blk, forget_blk)), result)
    initial = (memory, normalizer, stabilizer, jnp.zeros_like(stabilizer))
    ignored, outputs = lax.scan(advance, initial, tuple((to_blocks(array) for array in (query_rows, key_rows, value_rows, input_gate, log_forget))))
    return jnp.moveaxis(outputs, 0, 1).reshape(query_rows.shape[:2] + (value_rows.shape[2],))

def direction_sweep(query_rows, key_rows, value_rows, input_gate, log_forget, memory, normalizer):
    zero_rows = jnp.zeros((memory.shape[0],), jnp.float32)
    return span_sweep(query_rows, key_rows, value_rows, input_gate, log_forget, memory, normalizer, zero_rows, math.gcd(T_DEV, 256))

def reverse_time(array):
    return jnp.flip(array, axis=1)

def pool_window(padded, positions, channels, seq_len, group_size):
    row_count = positions.shape[0]
    group_index = channels // group_size
    reach_left = jnp.left_shift(jnp.ones_like(group_index), group_index)
    reach_right = reach_left - 1
    window_sum = jnp.zeros((row_count, channels.shape[0]), jnp.float32)
    for offset in range(-HALO, HALO):
        inside = ((offset >= -reach_left) & (offset <= reach_right)).astype(jnp.float32)
        window_sum = window_sum + inside * padded[HALO + offset:HALO + offset + row_count]
    first_pos = jnp.maximum(positions[:, None] - reach_left[None, :], 0)
    last_pos = jnp.minimum(positions[:, None] + reach_right[None, :], seq_len - 1)
    counted = (last_pos - first_pos + 1).astype(jnp.float32)
    centre = padded[HALO:HALO + row_count]
    return (window_sum / counted - centre).astype(jnp.bfloat16)

def output_project(memory_out, pool_out, mem_out_weight, pool_out_weight):
    row_count = memory_out.shape[0]
    model_width = pool_out.shape[1]

    def grouped(matrix):
        return jnp.moveaxis(matrix.reshape(matrix.shape[0], N_TP, matrix.shape[1] // N_TP), 1, 0)

    def accumulate(running, pieces):
        mem_rows, pool_rows, mem_cols, pool_cols = pieces
        group_sum = lax.dot_general(mem_rows, mem_cols, (((1,), (1,)), ((), ())), preferred_element_type=jnp.float32)
        group_sum = group_sum + lax.dot_general(pool_rows, pool_cols, (((1,), (1,)), ((), ())), preferred_element_type=jnp.float32)
        rounded = lax.optimization_barrier(group_sum.astype(jnp.bfloat16))
        return (running + rounded.astype(jnp.float32), None)
    running, ignored = lax.scan(accumulate, jnp.zeros((row_count, model_width), jnp.float32), (grouped(memory_out), grouped(pool_out), grouped(mem_out_weight), grouped(pool_out_weight)))
    return running.astype(jnp.bfloat16)

def reference(tokens, norm_gain, query_weight, key_weight, value_weight, outgate_weight, gate_weight, gate_bias, decay_extra, init_memory, init_normalizer, head_gain, pool_weight, mem_out_weight, pool_out_weight):
    seq_count, seq_len, model_width = tokens.shape
    head_count, head_width = head_gain.shape
    flattened = tokens.reshape(seq_count * seq_len, model_width).astype(jnp.float32)
    normed = (flattened * lax.rsqrt(lax.optimization_barrier(jnp.mean(flattened * flattened, axis=-1, keepdims=True)) + norm_eps) * norm_gain).astype(jnp.bfloat16)

    def project(weight):
        return jnp.dot(normed, weight, preferred_element_type=jnp.float32).astype(jnp.bfloat16)
    query_proj = project(query_weight)
    key_proj = project(key_weight)
    value_proj = project(value_weight)
    outgate = project(outgate_weight)
    pool_input = project(pool_weight)
    gate_pre = lax.dot_general(normed, gate_weight.reshape(4 * head_count, model_width), (((1,), (1,)), ((), ())), preferred_element_type=jnp.float32) + gate_bias.reshape(4 * head_count)
    gate_pre = gate_pre.reshape(seq_count, seq_len, 4, head_count).transpose(2, 0, 3, 1).reshape(4, seq_count * head_count, seq_len)

    def to_heads(matrix):
        shaped = matrix.reshape(seq_count, seq_len, head_count, head_width).transpose(0, 2, 1, 3)
        return shaped.reshape(seq_count * head_count, seq_len, head_width)
    query_heads = to_heads(query_proj)
    key_heads = to_heads(key_proj)
    value_heads = to_heads(value_proj)
    extra_decay = decay_extra.transpose(1, 0, 2, 3).reshape(2, seq_count * head_count, seq_len)
    forward_forget = jax.nn.log_sigmoid(gate_pre[1]) + extra_decay[0]
    backward_forget = jax.nn.log_sigmoid(gate_pre[3]) + extra_decay[1]
    start_memory = init_memory.reshape(seq_count, 2, head_count, head_width, head_width)
    start_norm = init_normalizer.reshape(seq_count, 2, head_count, head_width)
    forward = direction_sweep(query_heads, key_heads, value_heads, gate_pre[0], forward_forget, start_memory[:, 0].reshape(-1, head_width, head_width), start_norm[:, 0].reshape(-1, head_width))
    backward = reverse_time(direction_sweep(reverse_time(query_heads), reverse_time(key_heads), reverse_time(value_heads), reverse_time(gate_pre[2]), reverse_time(backward_forget), start_memory[:, 1].reshape(-1, head_width, head_width), start_norm[:, 1].reshape(-1, head_width)))
    summed_dirs = (forward + backward).reshape(seq_count, head_count, seq_len, head_width).transpose(0, 2, 1, 3)
    summed_dirs = summed_dirs.reshape(seq_count * seq_len, head_count, head_width)
    normed_heads = summed_dirs * lax.rsqrt(lax.optimization_barrier(jnp.mean(summed_dirs * summed_dirs, axis=-1, keepdims=True)) + norm_eps) * head_gain
    out_gate = jax.nn.sigmoid(outgate.astype(jnp.float32).reshape(seq_count * seq_len, head_count, head_width))
    memory_out = (normed_heads * out_gate).astype(jnp.bfloat16).reshape(seq_count * seq_len, head_count * head_width)
    padded = jnp.pad(pool_input.reshape(seq_count, seq_len, model_width).astype(jnp.float32), ((0, 0), (HALO, HALO), (0, 0)))
    window_fn = partial(pool_window, positions=jnp.arange(seq_len, dtype=jnp.int32), channels=jnp.arange(model_width, dtype=jnp.int32), seq_len=seq_len, group_size=model_width // 4)
    pool_out = jax.vmap(window_fn)(padded).reshape(seq_count * seq_len, model_width)
    mixed = output_project(memory_out, pool_out, mem_out_weight, pool_out_weight)
    return mixed.reshape(seq_count, seq_len, model_width)
```

```python
import jax
import jax.numpy as jnp
from jax import lax
from jax.experimental import pallas as pl
from jax.experimental.pallas import tpu as pltpu
from jax.sharding import PartitionSpec as P

HALO = 8
norm_eps = 1e-06
NZ = 16
NY = 4
ROWS = 32
LOWEST = -1e30
PACKET = 144

f32 = jnp.float32
bf16 = jnp.bfloat16
smem = pl.BlockSpec(memory_space=pltpu.SMEM)
vmem = pl.BlockSpec(memory_space=pltpu.VMEM)


def from_everyone(x, axis):
    copies = jnp.broadcast_to(x, (lax.axis_size(axis), *x.shape))
    return lax.all_to_all(copies, axis, split_axis=0, concat_axis=0, tiled=True)


def pack_kernel(k_ref, v_ref, q_ref, o_ref, p_ref, m_ref, po_ref, kv_ref, rest_ref):
    kv_ref[:, :128] = k_ref[...]
    kv_ref[:, 128:] = v_ref[...]
    at = 0
    for ref in (q_ref, o_ref, p_ref, m_ref, po_ref):
        width = ref.shape[1]
        rest_ref[:, at : at + width] = ref[...]
        at += width


def in_order(w_ref, lo, hi):
    return jnp.concatenate(
        [w_ref[y, z * ROWS : (z + 1) * ROWS, lo:hi] for z in range(NZ) for y in range(NY)], axis=0
    )


def log_sigmoid(x):
    return jnp.minimum(x, 0.0) - jnp.log1p(jnp.exp(-jnp.abs(x)))


def gates_kernel(tok_ref, gain_ref, gw_ref, bias_ref, decay_ref, normed_ref, cols_ref, rows_ref):
    x = tok_ref[...].astype(f32)
    count = x.shape[0]
    normed = x * lax.rsqrt(jnp.mean(x * x, axis=-1, keepdims=True) + norm_eps) * gain_ref[...]
    normed = normed.astype(bf16)
    normed_ref[...] = normed
    pre = lax.dot_general(
        gw_ref[...], normed, (((1,), (1,)), ((), ())), preferred_element_type=f32
    )
    pre = pre + bias_ref[...]
    in_rows = (pre[0:1], pre[2:3])
    lf_rows = (
        log_sigmoid(pre[1:2]) + decay_ref[0:1],
        log_sigmoid(pre[3:4]) + decay_ref[1:2],
    )
    stacked = jnp.concatenate(
        [in_rows[0], in_rows[1], lf_rows[0], lf_rows[1], jnp.zeros((124, count), f32)], axis=0
    )
    turned = stacked.T
    first = lax.broadcasted_iota(jnp.int32, (count, count), 0)
    second = lax.broadcasted_iota(jnp.int32, (count, count), 1)
    lane = lax.broadcasted_iota(jnp.int32, (count, 128), 1)
    cols = jnp.zeros((count, 128), f32)
    rows = []
    tails = []
    for r in range(2):
        reach = second <= first if r == 0 else second >= first
        reach_t = first <= second if r == 0 else first >= second
        lf_row = lf_rows[r]
        lf_col = turned[:, 2 + r : 3 + r]
        b_col = jnp.sum(jnp.where(reach, lf_row, 0.0), axis=1, keepdims=True)
        b_row = jnp.sum(jnp.where(reach_t, lf_col, 0.0), axis=0, keepdims=True)
        a_row = in_rows[r] - b_row
        a_col = turned[:, r : r + 1] - b_col
        m_col = jnp.max(jnp.where(reach, a_row, LOWEST), axis=1, keepdims=True)
        top = jnp.max(a_row, axis=1, keepdims=True)
        w_col = jnp.exp(a_col - top)
        total = jnp.sum(lf_row, axis=1, keepdims=True)
        for n, col in enumerate((b_col, m_col, w_col)):
            cols = jnp.where(lane == 3 * r + n, col, cols)
        rows.append(a_row)
        tails.append(jnp.broadcast_to(total + top, (1, count)))
        tails.append(jnp.broadcast_to(total, (1, count)))
    cols_ref[...] = cols
    rows_ref[...] = jnp.concatenate(rows + tails + [jnp.zeros((2, count), f32)], axis=0)


def in_three(x):
    high = x.astype(bf16).astype(f32)
    rest = x - high
    mid = rest.astype(bf16).astype(f32)
    low = (rest - mid).astype(bf16).astype(f32)
    return [high, mid, low]


def state_kernel(z_ref, w_ref, normed_ref, cols_ref, rows_ref, k_ref, v_ref, out_ref):
    position = z_ref[0]
    weight = in_order(w_ref, 0, 256)
    kv = jnp.dot(normed_ref[...], weight, preferred_element_type=f32).astype(bf16)
    k = kv[:, :128]
    v = kv[:, 128:]
    k_ref[...] = k
    v_ref[...] = v
    scale = 128**-0.5
    k_wide = k.astype(f32)
    v_wide = v.astype(f32)
    packets = []
    for r in range(2):
        w = cols_ref[:, 3 * r + 2 : 3 * r + 3]
        wv = w * v_wide
        high = wv.astype(bf16)
        low = (wv - high.astype(f32)).astype(bf16)
        over_time = (((0,), (0,)), ((), ()))
        memory = lax.dot_general(high, k, over_time, preferred_element_type=f32)
        memory = memory + lax.dot_general(low, k, over_time, preferred_element_type=f32)
        norm = jnp.sum(w * k_wide, axis=0, keepdims=True) * scale
        extra = in_three(norm)
        extra = extra + in_three(rows_ref[2 + 2 * r : 3 + 2 * r, :128])
        extra = extra + in_three(rows_ref[3 + 2 * r : 4 + 2 * r, :128])
        extra = jnp.concatenate(extra + [jnp.zeros((7, 128), f32)], axis=0)
        packets.append(jnp.concatenate([memory * scale, extra], axis=0).astype(bf16))
    for j in range(NZ):

        @pl.when(j > position)
        def _():
            out_ref[j] = packets[0]

        @pl.when(j <= position)
        def _():
            out_ref[j] = packets[1]


def local_kernel(
    w_ref, normed_ref, k_ref, v_ref, cols_ref, rows_ref,
    q_ref, o_ref, p_ref, num_ref, den_ref,
):
    weight = w_ref[:, :512]
    both = jnp.dot(normed_ref[...], weight, preferred_element_type=f32).astype(bf16)
    q = both[:, :128]
    q_ref[...] = q
    o_ref[...] = both[:, 128:256]
    p_ref[...] = both[:, 256:512]
    count = q.shape[0]
    scores = lax.dot_general(
        q, k_ref[...], (((1,), (1,)), ((), ())), preferred_element_type=f32
    ) * (128**-0.5)
    first = lax.broadcasted_iota(jnp.int32, (count, count), 0)
    second = lax.broadcasted_iota(jnp.int32, (count, count), 1)
    lane = lax.broadcasted_iota(jnp.int32, (count, 128), 1)
    dens = jnp.zeros((count, 128), f32)
    for r in range(2):
        reach = second <= first if r == 0 else second >= first
        m_col = cols_ref[:, 3 * r + 1 : 3 * r + 2]
        a_row = rows_ref[r : r + 1]
        weights = jnp.exp(jnp.where(reach, a_row - m_col, LOWEST)) * scores
        num_ref[r] = jnp.dot(weights.astype(bf16), v_ref[...], preferred_element_type=f32)
        dens = jnp.where(lane == r, jnp.sum(weights, axis=1, keepdims=True), dens)
    den_ref[...] = dens


def pool_kernel(s_ref, p_ref, lo_ref, hi_ref, out_ref, a_ref, b_ref):
    count = p_ref.shape[0]
    group = s_ref[1]
    centre = p_ref[...].astype(f32)
    a_ref[0:8] = jnp.zeros_like(a_ref[0:8])
    a_ref[8:16] = lo_ref[...].astype(f32)
    a_ref[16 : 16 + count] = centre
    a_ref[16 + count : 24 + count] = hi_ref[...].astype(f32)
    a_ref[24 + count : 32 + count] = jnp.zeros_like(a_ref[0:8])
    width = count + 16
    b_ref[...] = jnp.zeros_like(b_ref)
    b_ref[8 : 8 + width] = a_ref[7 : 7 + width] + a_ref[8 : 8 + width]
    total = b_ref[16 : 16 + count]
    refs = (b_ref, a_ref)
    for g in range(1, 4):
        step = 1 << (g - 1)
        src, dst = refs[(g - 1) % 2], refs[g % 2]
        dst[8 : 8 + width] = src[8 - step : 8 - step + width] + src[8 + step : 8 + step + width]
        total = jnp.where(group == g, dst[16 : 16 + count], total)
    left = jnp.left_shift(1, group)
    position = s_ref[0] * count + lax.broadcasted_iota(jnp.int32, (count, 1), 0)
    begin = jnp.maximum(position - left, 0)
    end = jnp.minimum(position + left - 1, NZ * count - 1)
    counted = (end - begin + 1).astype(f32)
    out_ref[...] = (total / counted - centre).astype(bf16)


def final_kernel(
    s_ref, got_ref, mem_ref, nrm_ref, cols_ref, q_ref, o_ref, num_ref, den_ref,
    gain_ref, pool_ref, w_ref, out_ref,
):
    position = s_ref[0]
    got_n, got_m, got_f = [], [], []
    for j in range(NZ):
        extra = got_ref[j, 128:PACKET].astype(f32)
        got_n.append(extra[0:1] + extra[1:2] + extra[2:3])
        got_m.append(extra[3:4] + extra[4:5] + extra[5:6])
        got_f.append(extra[6:7] + extra[7:8] + extra[8:9])
    q = q_ref[...]
    q_wide = q.astype(f32)
    last = (((1,), (1,)), ((), ()))
    summed = None
    for r in range(2):
        order = range(NZ - 1, -1, -1) if r == 0 else range(NZ)
        levels = [None] * NZ
        passed = jnp.zeros((1, 128), f32)
        for j in order:
            ahead = j < position if r == 0 else j > position
            levels[j] = jnp.where(ahead, got_m[j] + passed, LOWEST)
            passed = passed + jnp.where(ahead, got_f[j], 0.0)
        top = passed
        for j in range(NZ):
            top = jnp.maximum(top, levels[j])
        share = jnp.exp(passed - top)
        memory = share * mem_ref[r]
        norm = share * nrm_ref[r : r + 1]
        for j in range(NZ):
            share = jnp.exp(levels[j] - top)
            memory = memory + share * got_ref[j, 0:128].astype(f32)
            norm = norm + share * got_n[j]
        high = memory.astype(bf16)
        low = (memory - high.astype(f32)).astype(bf16)
        carried = lax.dot_general(q, high, last, preferred_element_type=f32)
        carried = carried + lax.dot_general(q, low, last, preferred_element_type=f32)
        carried_den = jnp.sum(q_wide * norm, axis=1, keepdims=True)
        b_col = cols_ref[:, 3 * r : 3 * r + 1]
        m_col = cols_ref[:, 3 * r + 1 : 3 * r + 2]
        stab = top[:, 0:1]
        joint = jnp.maximum(stab, m_col)
        carry = jnp.exp(stab - joint)
        keep = jnp.exp(m_col - joint)
        numerator = carry * carried + keep * num_ref[r]
        denominator = carry * carried_den + keep * den_ref[:, r : r + 1]
        floor = jnp.exp(-(b_col + joint))
        part = numerator / jnp.maximum(jnp.abs(denominator), floor)
        summed = part if summed is None else summed + part
    scaled = summed * lax.rsqrt(jnp.mean(summed * summed, axis=-1, keepdims=True) + norm_eps)
    gate = 1.0 / (1.0 + jnp.exp(-o_ref[...].astype(f32)))
    memory_out = (scaled * gain_ref[...] * gate).astype(bf16)
    result = lax.dot_general(memory_out, w_ref[:, 512:640], last, preferred_element_type=f32)
    result = result + lax.dot_general(pool_ref[...], w_ref[:, 640:], last, preferred_element_type=f32)
    out_ref[...] = result.astype(bf16)


def sds(shape, dtype):
    return jax.ShapeDtypeStruct(shape, dtype)


def call(kernel, name, outs, scalars, *args, flops=0, scratch=()):
    many = isinstance(outs, tuple)
    return pl.pallas_call(
        kernel,
        in_specs=[smem] * len(scalars) + [vmem] * len(args),
        out_specs=(vmem,) * len(outs) if many else vmem,
        out_shape=outs,
        scratch_shapes=list(scratch),
        cost_estimate=pl.CostEstimate(flops=flops, bytes_accessed=0, transcendentals=0),
        name=name,
    )(*scalars, *args)


def per_device(
    tokens,
    norm_gain,
    query_weight,
    key_weight,
    value_weight,
    outgate_weight,
    gate_weight,
    gate_bias,
    decay_extra,
    init_memory,
    init_normalizer,
    head_gain,
    pool_weight,
    mem_out_weight,
    pool_out_weight,
):
    count, width = tokens.shape[1:]
    z = lax.axis_index("sp")
    scalars = jnp.stack([z, lax.axis_index("tp") // 2]).astype(jnp.int32)
    packed, packed_rest = call(
        pack_kernel, "pack", (sds((ROWS, 256), bf16), sds((ROWS, 896), bf16)), (),
        key_weight, value_weight, query_weight, outgate_weight, pool_weight, mem_out_weight,
        pool_out_weight,
        flops=10**6,
    )
    along_y = lax.all_gather(packed_rest, "fs", axis=0, tiled=True)
    rest = lax.all_gather(along_y, "sp", axis=0, tiled=True)
    packed, along_y = lax.optimization_barrier((packed, along_y))
    along_z = lax.all_gather(packed, "sp", axis=0, tiled=True)
    kv_weight = from_everyone(along_z, "fs")
    own_tokens, along_z = lax.optimization_barrier((tokens[0], along_z))
    normed, cols, rows = call(
        gates_kernel, "gates",
        (sds((count, width), bf16), sds((count, 128), f32), sds((8, count), f32)), (),
        own_tokens,
        norm_gain[None],
        jnp.pad(gate_weight[:, 0], ((0, 4), (0, 0))),
        jnp.pad(gate_bias, ((0, 4), (0, 0))),
        decay_extra[0, :, 0],
        flops=4 * 10**9,
    )
    k, v, packets = call(
        state_kernel, "state",
        (sds((count, 128), bf16), sds((count, 128), bf16), sds((NZ, PACKET, 128), bf16)),
        (scalars,), kv_weight, normed, cols, rows,
        flops=2 * 10**9,
    )
    got = lax.all_to_all(packets, "sp", 0, 0, tiled=True)
    q, outgate, pool_in, nums, dens = call(
        local_kernel, "local",
        (
            sds((count, 128), bf16),
            sds((count, 128), bf16),
            sds((count, 256), bf16),
            sds((2, count, 128), f32),
            sds((count, 128), f32),
        ),
        (), rest, normed, k, v, cols, rows,
        flops=5 * 10**9,
    )
    length = lax.axis_size("sp")
    up = [(i, i + 1) for i in range(length - 1)]
    down = [(i + 1, i) for i in range(length - 1)]
    low = lax.ppermute(pool_in[count - HALO :], "sp", up)
    high = lax.ppermute(pool_in[:HALO], "sp", down)
    pool_out = call(
        pool_kernel, "pool", sds((count, 256), bf16), (scalars,), pool_in, low, high,
        flops=10**9, scratch=[pltpu.VMEM((count + 32, 256), f32)] * 2,
    )
    partial = call(
        final_kernel, "final", sds((count, width), bf16), (scalars,),
        got, init_memory[0, :, 0], init_normalizer[0, :, 0], cols, q, outgate,
        nums, dens, head_gain, pool_out, rest,
        flops=2 * 10**9,
    )
    own = count // lax.axis_size("tp")
    parts = lax.all_to_all(partial.reshape(-1, own, width), "tp", 0, 0, tiled=True)
    mixed = jnp.sum(parts.astype(f32), axis=0).astype(bf16)
    return mixed.reshape(1, own, width)


def solution(mesh):
    placed = (
        P("fs", "sp", None),
        P(),
        P(("sp", "fs"), "tp"),
        P(("sp", "fs"), "tp"),
        P(("sp", "fs"), "tp"),
        P(("sp", "fs"), "tp"),
        P(None, "tp", None),
        P(None, "tp"),
        P("fs", None, "tp", "sp"),
        P("fs", None, "tp", None, None),
        P("fs", None, "tp", None),
        P("tp", None),
        P(("sp", "fs"), "tp"),
        P(("sp", "fs"), "tp"),
        P(("sp", "fs"), "tp"),
    )
    return jax.shard_map(
        per_device,
        mesh=mesh,
        in_specs=placed,
        out_specs=P("fs", ("sp", "tp"), None),
        check_vma=False,
    )
```

```python
import jax
import jax.numpy as jnp
from jax import lax
from jax.experimental import pallas as pl
from jax.experimental.pallas import tpu as pltpu
from jax.sharding import PartitionSpec as P

HALO = 8
norm_eps = 1e-06
NZ = 16
NY = 4
ROWS = 32
LOWEST = -1e30
PACKET = 144

f32 = jnp.float32
bf16 = jnp.bfloat16
smem = pl.BlockSpec(memory_space=pltpu.SMEM)
vmem = pl.BlockSpec(memory_space=pltpu.VMEM)


def from_everyone(x, axis):
    copies = jnp.broadcast_to(x, (lax.axis_size(axis), *x.shape))
    return lax.all_to_all(copies, axis, split_axis=0, concat_axis=0, tiled=True)


def pack_kernel(k_ref, v_ref, q_ref, o_ref, p_ref, m_ref, out_ref):
    at = 0
    for ref in (k_ref, v_ref, q_ref, o_ref, p_ref, m_ref):
        width = ref.shape[1]
        out_ref[:, at : at + width] = ref[...]
        at += width


def in_order(w_ref):
    return jnp.concatenate(
        [w_ref[y, z * ROWS : (z + 1) * ROWS] for z in range(NZ) for y in range(NY)], axis=0
    )


def around(x, axis):
    count = lax.axis_size(axis)
    return [x] + [lax.ppermute(x, axis, [(i, (i + s) % count) for i in range(count)]) for s in (1, 2, 3)]


def placed_by_source(y, refs, out_ref):
    for shift, ref in enumerate(refs):
        out_ref[lax.rem(y + NY - shift, NY)] = ref[...]


def rms_normed(x, gain):
    return x * lax.rsqrt(jnp.mean(x * x, axis=-1, keepdims=True) + norm_eps) * gain


def log_sigmoid(x):
    return jnp.minimum(x, 0.0) - jnp.log1p(jnp.exp(-jnp.abs(x)))


def gates_kernel(tok_ref, gain_ref, gw_ref, bias_ref, decay_ref, normed_ref, cols_ref, rows_ref):
    x = tok_ref[...].astype(f32)
    count = x.shape[0]
    normed = rms_normed(x, gain_ref[...]).astype(bf16)
    normed_ref[...] = normed
    pre = lax.dot_general(
        gw_ref[...], normed, (((1,), (1,)), ((), ())), preferred_element_type=f32
    )
    pre = pre + bias_ref[...]
    in_rows = (pre[0:1], pre[2:3])
    lf_rows = (
        log_sigmoid(pre[1:2]) + decay_ref[0:1],
        log_sigmoid(pre[3:4]) + decay_ref[1:2],
    )
    stacked = jnp.concatenate(
        [in_rows[0], in_rows[1], lf_rows[0], lf_rows[1], jnp.zeros((124, count), f32)], axis=0
    )
    turned = stacked.T
    first = lax.broadcasted_iota(jnp.int32, (count, count), 0)
    second = lax.broadcasted_iota(jnp.int32, (count, count), 1)
    lane = lax.broadcasted_iota(jnp.int32, (count, 128), 1)
    cols = jnp.zeros((count, 128), f32)
    rows = []
    tails = []
    for r in range(2):
        reach = second <= first if r == 0 else second >= first
        reach_t = first <= second if r == 0 else first >= second
        lf_row = lf_rows[r]
        lf_col = turned[:, 2 + r : 3 + r]
        b_col = jnp.sum(jnp.where(reach, lf_row, 0.0), axis=1, keepdims=True)
        b_row = jnp.sum(jnp.where(reach_t, lf_col, 0.0), axis=0, keepdims=True)
        a_row = in_rows[r] - b_row
        a_col = turned[:, r : r + 1] - b_col
        m_col = jnp.max(jnp.where(reach, a_row, LOWEST), axis=1, keepdims=True)
        top = jnp.max(a_row, axis=1, keepdims=True)
        w_col = jnp.exp(a_col - top)
        total = jnp.sum(lf_row, axis=1, keepdims=True)
        for n, col in enumerate((b_col, m_col, w_col)):
            cols = jnp.where(lane == 3 * r + n, col, cols)
        rows.append(a_row)
        tails.append(jnp.broadcast_to(total + top, (1, count)))
        tails.append(jnp.broadcast_to(total, (1, count)))
    cols_ref[...] = cols
    rows_ref[...] = jnp.concatenate(rows + tails + [jnp.zeros((2, count), f32)], axis=0)


def in_three(x):
    high = x.astype(bf16).astype(f32)
    rest = x - high
    mid = rest.astype(bf16).astype(f32)
    low = (rest - mid).astype(bf16).astype(f32)
    return [high, mid, low]


def state_kernel(z_ref, w_ref, normed_ref, cols_ref, rows_ref, k_ref, v_ref, out_ref):
    position = z_ref[0]
    weight = in_order(w_ref)
    kv = jnp.dot(normed_ref[...], weight, preferred_element_type=f32).astype(bf16)
    k = kv[:, :128]
    v = kv[:, 128:]
    k_ref[...] = k
    v_ref[...] = v
    scale = 128**-0.5
    k_wide = k.astype(f32)
    v_wide = v.astype(f32)
    packets = []
    for r in range(2):
        w = cols_ref[:, 3 * r + 2 : 3 * r + 3]
        wv = w * v_wide
        high = wv.astype(bf16)
        low = (wv - high.astype(f32)).astype(bf16)
        over_time = (((0,), (0,)), ((), ()))
        memory = lax.dot_general(high, k, over_time, preferred_element_type=f32)
        memory = memory + lax.dot_general(low, k, over_time, preferred_element_type=f32)
        norm = jnp.sum(w * k_wide, axis=0, keepdims=True) * scale
        extra = in_three(norm)
        extra = extra + in_three(rows_ref[2 + 2 * r : 3 + 2 * r, :128])
        extra = extra + in_three(rows_ref[3 + 2 * r : 4 + 2 * r, :128])
        extra = jnp.concatenate(extra + [jnp.zeros((7, 128), f32)], axis=0)
        packets.append(jnp.concatenate([memory * scale, extra], axis=0).astype(bf16))
    for j in range(NZ):

        @pl.when(j > position)
        def _():
            out_ref[j] = packets[0]

        @pl.when(j <= position)
        def _():
            out_ref[j] = packets[1]


def pooled(position, group, centre, low, high, a_ref, b_ref):
    count = centre.shape[0]
    a_ref[0:8] = jnp.zeros_like(a_ref[0:8])
    a_ref[8:16] = low
    a_ref[16 : 16 + count] = centre
    a_ref[16 + count : 24 + count] = high
    a_ref[24 + count : 32 + count] = jnp.zeros_like(a_ref[0:8])
    width = count + 16
    b_ref[...] = jnp.zeros_like(b_ref)
    b_ref[8 : 8 + width] = a_ref[7 : 7 + width] + a_ref[8 : 8 + width]
    total = b_ref[16 : 16 + count]
    refs = (b_ref, a_ref)
    for g in range(1, 4):
        step = 1 << (g - 1)
        src, dst = refs[(g - 1) % 2], refs[g % 2]
        dst[8 : 8 + width] = src[8 - step : 8 - step + width] + src[8 + step : 8 + step + width]
        total = jnp.where(group == g, dst[16 : 16 + count], total)
    left = jnp.left_shift(1, group)
    place = position * count + lax.broadcasted_iota(jnp.int32, (count, 1), 0)
    begin = jnp.maximum(place - left, 0)
    end = jnp.minimum(place + left - 1, NZ * count - 1)
    counted = (end - begin + 1).astype(f32)
    return (total / counted - centre).astype(bf16)


def local_kernel(
    s_ref, w0_ref, w1_ref, w2_ref, w3_ref, normed_ref, lo_ref, hi_ref, gain_ref,
    k_ref, v_ref, cols_ref, rows_ref,
    q_ref, o_ref, pool_ref, num_ref, den_ref, w_ref, a_ref, b_ref,
):
    placed_by_source(s_ref[2], (w0_ref, w1_ref, w2_ref, w3_ref), w_ref)
    weight = in_order(w_ref)
    halo = jnp.concatenate([lo_ref[...], hi_ref[...]], axis=0).astype(f32)
    halo = rms_normed(halo, gain_ref[...]).astype(bf16)
    left = jnp.concatenate([normed_ref[...], halo], axis=0)
    all_three = jnp.dot(left, weight, preferred_element_type=f32).astype(bf16)
    count = normed_ref.shape[0]
    q = all_three[:count, :128]
    q_ref[...] = q
    o_ref[...] = all_three[:count, 128:256]
    p = all_three[:, 256:512].astype(f32)
    pool_ref[...] = pooled(
        s_ref[0], s_ref[1], p[:count], p[count : count + HALO], p[count + HALO :], a_ref, b_ref
    )
    scores = lax.dot_general(
        q, k_ref[...], (((1,), (1,)), ((), ())), preferred_element_type=f32
    ) * (128**-0.5)
    first = lax.broadcasted_iota(jnp.int32, (count, count), 0)
    second = lax.broadcasted_iota(jnp.int32, (count, count), 1)
    lane = lax.broadcasted_iota(jnp.int32, (count, 128), 1)
    dens = jnp.zeros((count, 128), f32)
    for r in range(2):
        reach = second <= first if r == 0 else second >= first
        m_col = cols_ref[:, 3 * r + 1 : 3 * r + 2]
        a_row = rows_ref[r : r + 1]
        weights = jnp.exp(jnp.where(reach, a_row - m_col, LOWEST)) * scores
        num_ref[r] = jnp.dot(weights.astype(bf16), v_ref[...], preferred_element_type=f32)
        dens = jnp.where(lane == r, jnp.sum(weights, axis=1, keepdims=True), dens)
    den_ref[...] = dens


def final_kernel(
    s_ref, got_ref, mem_ref, nrm_ref, cols_ref, q_ref, o_ref, num_ref, den_ref,
    gain_ref, pool_ref, w0_ref, w1_ref, w2_ref, w3_ref, out_ref, w_ref,
):
    placed_by_source(s_ref[2], (w0_ref, w1_ref, w2_ref, w3_ref), w_ref)
    position = s_ref[0]
    got_n, got_m, got_f = [], [], []
    for j in range(NZ):
        extra = got_ref[j, 128:PACKET].astype(f32)
        got_n.append(extra[0:1] + extra[1:2] + extra[2:3])
        got_m.append(extra[3:4] + extra[4:5] + extra[5:6])
        got_f.append(extra[6:7] + extra[7:8] + extra[8:9])
    q = q_ref[...]
    q_wide = q.astype(f32)
    last = (((1,), (1,)), ((), ()))
    summed = None
    for r in range(2):
        order = range(NZ - 1, -1, -1) if r == 0 else range(NZ)
        levels = [None] * NZ
        passed = jnp.zeros((1, 128), f32)
        for j in order:
            ahead = j < position if r == 0 else j > position
            levels[j] = jnp.where(ahead, got_m[j] + passed, LOWEST)
            passed = passed + jnp.where(ahead, got_f[j], 0.0)
        top = passed
        for j in range(NZ):
            top = jnp.maximum(top, levels[j])
        share = jnp.exp(passed - top)
        memory = share * mem_ref[r]
        norm = share * nrm_ref[r : r + 1]
        for j in range(NZ):
            share = jnp.exp(levels[j] - top)
            memory = memory + share * got_ref[j, 0:128].astype(f32)
            norm = norm + share * got_n[j]
        high = memory.astype(bf16)
        low = (memory - high.astype(f32)).astype(bf16)
        carried = lax.dot_general(q, high, last, preferred_element_type=f32)
        carried = carried + lax.dot_general(q, low, last, preferred_element_type=f32)
        carried_den = jnp.sum(q_wide * norm, axis=1, keepdims=True)
        b_col = cols_ref[:, 3 * r : 3 * r + 1]
        m_col = cols_ref[:, 3 * r + 1 : 3 * r + 2]
        stab = top[:, 0:1]
        joint = jnp.maximum(stab, m_col)
        carry = jnp.exp(stab - joint)
        keep = jnp.exp(m_col - joint)
        numerator = carry * carried + keep * num_ref[r]
        denominator = carry * carried_den + keep * den_ref[:, r : r + 1]
        floor = jnp.exp(-(b_col + joint))
        part = numerator / jnp.maximum(jnp.abs(denominator), floor)
        summed = part if summed is None else summed + part
    scaled = summed * lax.rsqrt(jnp.mean(summed * summed, axis=-1, keepdims=True) + norm_eps)
    gate = 1.0 / (1.0 + jnp.exp(-o_ref[...].astype(f32)))
    memory_out = (scaled * gain_ref[...] * gate).astype(bf16)
    weight = in_order(w_ref)
    result = lax.dot_general(memory_out, weight[:, :128], last, preferred_element_type=f32)
    result = result + lax.dot_general(pool_ref[...], weight[:, 128:], last, preferred_element_type=f32)
    out_ref[...] = result.astype(bf16)


def sds(shape, dtype):
    return jax.ShapeDtypeStruct(shape, dtype)


def call(kernel, name, outs, scalars, *args, flops=0, scratch=()):
    many = isinstance(outs, tuple)
    return pl.pallas_call(
        kernel,
        in_specs=[smem] * len(scalars) + [vmem] * len(args),
        out_specs=(vmem,) * len(outs) if many else vmem,
        out_shape=outs,
        scratch_shapes=list(scratch),
        cost_estimate=pl.CostEstimate(flops=flops, bytes_accessed=0, transcendentals=0),
        name=name,
    )(*scalars, *args)


def per_device(
    tokens,
    norm_gain,
    query_weight,
    key_weight,
    value_weight,
    outgate_weight,
    gate_weight,
    gate_bias,
    decay_extra,
    init_memory,
    init_normalizer,
    head_gain,
    pool_weight,
    mem_out_weight,
    pool_out_weight,
):
    count, width = tokens.shape[1:]
    scalars = jnp.stack(
        [lax.axis_index("sp"), lax.axis_index("tp") // 2, lax.axis_index("fs")]
    ).astype(jnp.int32)
    packed = call(
        pack_kernel, "pack", sds((ROWS, 896), bf16), (),
        key_weight, value_weight, query_weight, outgate_weight, pool_weight, mem_out_weight,
        flops=10**6,
    )
    pool_z = from_everyone(pool_out_weight, "sp").reshape(NZ * ROWS, 256)
    along_z = lax.all_gather(packed, "sp", axis=0, tiled=True)
    kv_z, pool_z = lax.optimization_barrier((along_z[:, :256], pool_z))
    kv_weight = from_everyone(kv_z, "fs")
    own_tokens, along_z = lax.optimization_barrier((tokens[0], along_z))
    normed, cols, rows = call(
        gates_kernel, "gates",
        (sds((count, width), bf16), sds((count, 128), f32), sds((8, count), f32)), (),
        own_tokens,
        norm_gain[None],
        jnp.pad(gate_weight[:, 0], ((0, 4), (0, 0))),
        jnp.pad(gate_bias, ((0, 4), (0, 0))),
        decay_extra[0, :, 0],
        flops=4 * 10**9,
    )
    k, v, packets = call(
        state_kernel, "state",
        (sds((count, 128), bf16), sds((count, 128), bf16), sds((NZ, PACKET, 128), bf16)),
        (scalars,), kv_weight, normed, cols, rows,
        flops=2 * 10**9,
    )
    got = lax.all_to_all(packets, "sp", 0, 0, tiled=True)
    ends, first_rest, last_rest, k = lax.optimization_barrier(
        (
            (own_tokens[:HALO], own_tokens[count - HALO :]),
            along_z[:, 256:768],
            jnp.concatenate([along_z[:, 768:], pool_z], axis=1),
            k,
        )
    )
    length = lax.axis_size("sp")
    first_rest = around(first_rest, "fs")
    low = lax.ppermute(ends[1], "sp", [(i, i + 1) for i in range(length - 1)])
    high = lax.ppermute(ends[0], "sp", [(i + 1, i) for i in range(length - 1)])
    last_rest = around(last_rest, "fs")
    q, outgate, pool_out, nums, dens = call(
        local_kernel, "local",
        (
            sds((count, 128), bf16),
            sds((count, 128), bf16),
            sds((count, 256), bf16),
            sds((2, count, 128), f32),
            sds((count, 128), f32),
        ),
        (scalars,), *first_rest, normed, low, high, norm_gain[None], k, v, cols, rows,
        flops=5 * 10**9,
        scratch=[pltpu.VMEM((NY, NZ * ROWS, 512), bf16)]
        + [pltpu.VMEM((count + 32, 256), f32)] * 2,
    )
    partial = call(
        final_kernel, "final", sds((count, width), bf16), (scalars,),
        got, init_memory[0, :, 0], init_normalizer[0, :, 0], cols, q, outgate,
        nums, dens, head_gain, pool_out, *last_rest,
        flops=2 * 10**9,
        scratch=[pltpu.VMEM((NY, NZ * ROWS, 384), bf16)],
    )
    own = count // lax.axis_size("tp")
    parts = lax.all_to_all(partial.reshape(-1, own, width), "tp", 0, 0, tiled=True)
    mixed = jnp.sum(parts.astype(f32), axis=0).astype(bf16)
    return mixed.reshape(1, own, width)


def solution(mesh):
    placed = (
        P("fs", "sp", None),
        P(),
        P(("sp", "fs"), "tp"),
        P(("sp", "fs"), "tp"),
        P(("sp", "fs"), "tp"),
        P(("sp", "fs"), "tp"),
        P(None, "tp", None),
        P(None, "tp"),
        P("fs", None, "tp", "sp"),
        P("fs", None, "tp", None, None),
        P("fs", None, "tp", None),
        P("tp", None),
        P(("sp", "fs"), "tp"),
        P(("sp", "fs"), "tp"),
        P(("sp", "fs"), "tp"),
    )
    return jax.shard_map(
        per_device,
        mesh=mesh,
        in_specs=placed,
        out_specs=P("fs", ("sp", "tp"), None),
        check_vma=False,
    )
```

```python
import jax
import jax.numpy as jnp
from jax import lax
from jax.experimental import pallas as pl
from jax.experimental.pallas import tpu as pltpu
from jax.sharding import PartitionSpec as P


HALO = 8
norm_eps = 1e-06
NZ = 16
NY = 4
ROWS = 32
LOWEST = -1e30
PACKET = 144

f32 = jnp.float32
bf16 = jnp.bfloat16
smem = pl.BlockSpec(memory_space=pltpu.SMEM)
vmem = pl.BlockSpec(memory_space=pltpu.VMEM)


def from_everyone(x, axis):
    copies = jnp.broadcast_to(x, (lax.axis_size(axis), *x.shape))
    return lax.all_to_all(copies, axis, split_axis=0, concat_axis=0, tiled=True)


def pack_kernel(k_ref, v_ref, q_ref, o_ref, p_ref, m_ref, po_ref, out_ref, copies_ref):
    for z in range(NZ):
        copies_ref[z] = po_ref[...]
    at = 0
    for ref in (k_ref, v_ref, q_ref, o_ref, p_ref, m_ref):
        width = ref.shape[1]
        out_ref[:, at : at + width] = ref[...]
        at += width


def in_order(w_ref):
    return jnp.concatenate(
        [w_ref[y, z * ROWS : (z + 1) * ROWS] for z in range(NZ) for y in range(NY)], axis=0
    )


def from_shift(x, axis, shift):
    count = lax.axis_size(axis)
    return lax.ppermute(x, axis, [(i, (i + shift) % count) for i in range(count)])


def placed_by_source(y, refs, out_ref):
    for shift, ref in enumerate(refs):
        out_ref[lax.rem(y + NY - shift, NY)] = ref[...]


def rms_normed(x, gain):
    return x * lax.rsqrt(jnp.mean(x * x, axis=-1, keepdims=True) + norm_eps) * gain


def log_sigmoid(x):
    return jnp.minimum(x, 0.0) - jnp.log1p(jnp.exp(-jnp.abs(x)))


def gates_kernel(bias_ref, tok_ref, gain_ref, gw_ref, decay_ref, normed_ref, cols_ref, rows_ref):
    x = tok_ref[...].astype(f32)
    count = x.shape[0]
    normed = rms_normed(x, gain_ref[...]).astype(bf16)
    normed_ref[...] = normed
    pre = lax.dot_general(
        gw_ref[...], normed, (((1,), (1,)), ((), ())), preferred_element_type=f32
    )
    pre = [pre[g : g + 1] + bias_ref[g] for g in range(4)]
    in_rows = (pre[0], pre[2])
    lf_rows = (log_sigmoid(pre[1]) + decay_ref[0], log_sigmoid(pre[3]) + decay_ref[1])
    stacked = jnp.concatenate(
        [in_rows[0], in_rows[1], lf_rows[0], lf_rows[1], jnp.zeros((124, count), f32)], axis=0
    )
    turned = stacked.T
    first = lax.broadcasted_iota(jnp.int32, (count, count), 0)
    second = lax.broadcasted_iota(jnp.int32, (count, count), 1)
    lane = lax.broadcasted_iota(jnp.int32, (count, 128), 1)
    cols = jnp.zeros((count, 128), f32)
    rows = []
    tails = []
    for r in range(2):
        reach = second <= first if r == 0 else second >= first
        reach_t = first <= second if r == 0 else first >= second
        lf_row = lf_rows[r]
        lf_col = turned[:, 2 + r : 3 + r]
        b_col = jnp.sum(jnp.where(reach, lf_row, 0.0), axis=1, keepdims=True)
        b_row = jnp.sum(jnp.where(reach_t, lf_col, 0.0), axis=0, keepdims=True)
        a_row = in_rows[r] - b_row
        a_col = turned[:, r : r + 1] - b_col
        m_col = jnp.max(jnp.where(reach, a_row, LOWEST), axis=1, keepdims=True)
        top = jnp.max(a_row, axis=1, keepdims=True)
        w_col = jnp.exp(a_col - top)
        total = jnp.sum(lf_row, axis=1, keepdims=True)
        for n, col in enumerate((b_col, m_col, w_col)):
            cols = jnp.where(lane == 3 * r + n, col, cols)
        rows.append(a_row)
        tails.append(jnp.broadcast_to(total + top, (1, count)))
        tails.append(jnp.broadcast_to(total, (1, count)))
    cols_ref[...] = cols
    rows_ref[...] = jnp.concatenate(rows + tails + [jnp.zeros((2, count), f32)], axis=0)


def in_three(x):
    high = x.astype(bf16).astype(f32)
    rest = x - high
    mid = rest.astype(bf16).astype(f32)
    low = (rest - mid).astype(bf16).astype(f32)
    return [high, mid, low]


def state_kernel(w_ref, normed_ref, cols_ref, rows_ref, k_ref, v_ref, out_ref):
    position = lax.axis_index("sp")
    weight = in_order(w_ref)
    kv = jnp.dot(normed_ref[...], weight, preferred_element_type=f32).astype(bf16)
    k = kv[:, :128]
    v = kv[:, 128:]
    k_ref[...] = k
    v_ref[...] = v
    scale = 128**-0.5
    k_wide = k.astype(f32)
    v_wide = v.astype(f32)
    packets = []
    for r in range(2):
        w = cols_ref[:, 3 * r + 2 : 3 * r + 3]
        wv = w * v_wide
        high = wv.astype(bf16)
        low = (wv - high.astype(f32)).astype(bf16)
        over_time = (((0,), (0,)), ((), ()))
        memory = lax.dot_general(high, k, over_time, preferred_element_type=f32)
        memory = memory + lax.dot_general(low, k, over_time, preferred_element_type=f32)
        norm = jnp.sum(w * k_wide, axis=0, keepdims=True) * scale
        extra = in_three(norm)
        extra = extra + in_three(rows_ref[2 + 2 * r : 3 + 2 * r, :128])
        extra = extra + in_three(rows_ref[3 + 2 * r : 4 + 2 * r, :128])
        extra = jnp.concatenate(extra + [jnp.zeros((7, 128), f32)], axis=0)
        packets.append(jnp.concatenate([memory * scale, extra], axis=0).astype(bf16))
    for j in range(NZ):

        @pl.when(j > position)
        def _():
            out_ref[j] = packets[0]

        @pl.when(j <= position)
        def _():
            out_ref[j] = packets[1]


def pooled(position, group, centre, low, high, a_ref, b_ref):
    count = centre.shape[0]
    a_ref[0:8] = jnp.zeros_like(a_ref[0:8])
    a_ref[8:16] = low
    a_ref[16 : 16 + count] = centre
    a_ref[16 + count : 24 + count] = high
    a_ref[24 + count : 32 + count] = jnp.zeros_like(a_ref[0:8])
    width = count + 16
    b_ref[...] = jnp.zeros_like(b_ref)
    b_ref[8 : 8 + width] = a_ref[7 : 7 + width] + a_ref[8 : 8 + width]
    total = b_ref[16 : 16 + count]
    refs = (b_ref, a_ref)
    for g in range(1, 4):
        step = 1 << (g - 1)
        src, dst = refs[(g - 1) % 2], refs[g % 2]
        dst[8 : 8 + width] = src[8 - step : 8 - step + width] + src[8 + step : 8 + step + width]
        total = jnp.where(group == g, dst[16 : 16 + count], total)
    left = jnp.left_shift(1, group)
    place = position * count + lax.broadcasted_iota(jnp.int32, (count, 1), 0)
    begin = jnp.maximum(place - left, 0)
    end = jnp.minimum(place + left - 1, NZ * count - 1)
    counted = (end - begin + 1).astype(f32)
    return (total / counted - centre).astype(bf16)


def local_kernel(
    w0_ref, w1_ref, w2_ref, w3_ref, normed_ref, lo_ref, hi_ref, gain_ref,
    k_ref, v_ref, cols_ref, rows_ref,
    q_ref, o_ref, pool_ref, num_ref, den_ref, wm_ref, w_ref, a_ref, b_ref,
):
    placed_by_source(lax.axis_index("fs"), (w0_ref, w1_ref, w2_ref, w3_ref), w_ref)
    weight = in_order(w_ref)
    wm_ref[...] = weight[:, 512:]
    weight = weight[:, :512]
    halo = jnp.concatenate([lo_ref[...], hi_ref[...]], axis=0).astype(f32)
    halo = rms_normed(halo, gain_ref[...]).astype(bf16)
    left = jnp.concatenate([normed_ref[...], halo], axis=0)
    all_three = jnp.dot(left, weight, preferred_element_type=f32).astype(bf16)
    count = normed_ref.shape[0]
    q = all_three[:count, :128]
    q_ref[...] = q
    o_ref[...] = all_three[:count, 128:256]
    p = all_three[:, 256:512].astype(f32)
    pool_ref[...] = pooled(
        lax.axis_index("sp"), lax.div(lax.axis_index("tp"), 2), p[:count], p[count : count + HALO], p[count + HALO :], a_ref, b_ref
    )
    scores = lax.dot_general(
        q, k_ref[...], (((1,), (1,)), ((), ())), preferred_element_type=f32
    ) * (128**-0.5)
    first = lax.broadcasted_iota(jnp.int32, (count, count), 0)
    second = lax.broadcasted_iota(jnp.int32, (count, count), 1)
    lane = lax.broadcasted_iota(jnp.int32, (count, 128), 1)
    dens = jnp.zeros((count, 128), f32)
    for r in range(2):
        reach = second <= first if r == 0 else second >= first
        m_col = cols_ref[:, 3 * r + 1 : 3 * r + 2]
        a_row = rows_ref[r : r + 1]
        weights = jnp.exp(jnp.where(reach, a_row - m_col, LOWEST)) * scores
        num_ref[r] = jnp.dot(weights.astype(bf16), v_ref[...], preferred_element_type=f32)
        dens = jnp.where(lane == r, jnp.sum(weights, axis=1, keepdims=True), dens)
    den_ref[...] = dens


def final_kernel(
    got_ref, mem_ref, nrm_ref, cols_ref, q_ref, o_ref, num_ref, den_ref,
    gain_ref, pool_ref, wm_ref, w0_ref, w1_ref, w2_ref, w3_ref, keep_ref, give_ref, w_ref,
):
    placed_by_source(lax.axis_index("fs"), (w0_ref, w1_ref, w2_ref, w3_ref), w_ref)
    position = lax.axis_index("sp")
    got_n, got_m, got_f = [], [], []
    for j in range(NZ):
        extra = got_ref[j, 128:PACKET].astype(f32)
        got_n.append(extra[0:1] + extra[1:2] + extra[2:3])
        got_m.append(extra[3:4] + extra[4:5] + extra[5:6])
        got_f.append(extra[6:7] + extra[7:8] + extra[8:9])
    q = q_ref[...]
    q_wide = q.astype(f32)
    last = (((1,), (1,)), ((), ()))
    summed = None
    for r in range(2):
        order = range(NZ - 1, -1, -1) if r == 0 else range(NZ)
        levels = [None] * NZ
        passed = jnp.zeros((1, 128), f32)
        for j in order:
            ahead = j < position if r == 0 else j > position
            levels[j] = jnp.where(ahead, got_m[j] + passed, LOWEST)
            passed = passed + jnp.where(ahead, got_f[j], 0.0)
        top = passed
        for j in range(NZ):
            top = jnp.maximum(top, levels[j])
        share = jnp.exp(passed - top)
        memory = share * mem_ref[r]
        norm = share * nrm_ref[r]
        for j in range(NZ):
            share = jnp.exp(levels[j] - top)
            memory = memory + share * got_ref[j, 0:128].astype(f32)
            norm = norm + share * got_n[j]
        high = memory.astype(bf16)
        low = (memory - high.astype(f32)).astype(bf16)
        carried = lax.dot_general(q, high, last, preferred_element_type=f32)
        carried = carried + lax.dot_general(q, low, last, preferred_element_type=f32)
        carried_den = jnp.sum(q_wide * norm, axis=1, keepdims=True)
        b_col = cols_ref[:, 3 * r : 3 * r + 1]
        m_col = cols_ref[:, 3 * r + 1 : 3 * r + 2]
        stab = top[:, 0:1]
        joint = jnp.maximum(stab, m_col)
        carry = jnp.exp(stab - joint)
        keep = jnp.exp(m_col - joint)
        numerator = carry * carried + keep * num_ref[r]
        denominator = carry * carried_den + keep * den_ref[:, r : r + 1]
        floor = jnp.exp(-(b_col + joint))
        part = numerator / jnp.maximum(jnp.abs(denominator), floor)
        summed = part if summed is None else summed + part
    scaled = summed * lax.rsqrt(jnp.mean(summed * summed, axis=-1, keepdims=True) + norm_eps)
    gate = 1.0 / (1.0 + jnp.exp(-o_ref[...].astype(f32)))
    memory_out = (scaled * gain_ref[...] * gate).astype(bf16)
    result = lax.dot_general(memory_out, wm_ref[...], last, preferred_element_type=f32)
    result = result + lax.dot_general(
        pool_ref[...], in_order(w_ref), last, preferred_element_type=f32
    )
    core = lax.rem(lax.axis_index("tp"), 2)
    own = keep_ref.shape[1]
    for x in range(keep_ref.shape[0]):
        south = result[2 * x * own : (2 * x + 1) * own]
        north = result[(2 * x + 1) * own : (2 * x + 2) * own]
        keep_ref[x] = jnp.where(core == 0, south, north).astype(bf16)
        give_ref[x] = jnp.where(core == 0, north, south).astype(bf16)


def sds(shape, dtype):
    return jax.ShapeDtypeStruct(shape, dtype)


def call(kernel, outs, scalars, *args, flops=0, scratch=()):
    many = isinstance(outs, tuple)
    return pl.pallas_call(
        kernel,
        in_specs=[smem] * len(scalars) + [vmem] * len(args),
        out_specs=(vmem,) * len(outs) if many else vmem,
        out_shape=outs,
        scratch_shapes=list(scratch),
        cost_estimate=pl.CostEstimate(flops=flops, bytes_accessed=0, transcendentals=0),
    )(*scalars, *args)


def per_device(
    tokens,
    norm_gain,
    query_weight,
    key_weight,
    value_weight,
    outgate_weight,
    gate_weight,
    gate_bias,
    decay_extra,
    init_memory,
    init_normalizer,
    head_gain,
    pool_weight,
    mem_out_weight,
    pool_out_weight,
):
    count, width = tokens.shape[1:]
    packed, pool_copies = call(
        pack_kernel, (sds((ROWS, 896), bf16), sds((NZ, ROWS, 256), bf16)), (),
        key_weight, value_weight, query_weight, outgate_weight, pool_weight, mem_out_weight,
        pool_out_weight,
        flops=10**6,
    )
    pool_z = lax.all_to_all(pool_copies, "sp", 0, 0, tiled=True).reshape(NZ * ROWS, 256)
    along_z = lax.all_gather(packed, "sp", axis=0, tiled=True)
    kv_z, pool_z = lax.optimization_barrier((along_z[:, :256], pool_z))
    kv_weight = from_everyone(kv_z, "fs")
    own_tokens, along_z = lax.optimization_barrier((tokens[0], along_z))
    normed, cols, rows = call(
        gates_kernel,
        (sds((count, width), bf16), sds((count, 128), f32), sds((8, count), f32)),
        (gate_bias.reshape(4),),
        own_tokens,
        norm_gain[None],
        gate_weight[:, 0],
        decay_extra[0, :, 0][:, None],
        flops=4 * 10**9,
    )
    first_rest, rows = lax.optimization_barrier((along_z[:, 256:], rows))
    first_from = {}
    for shift in (1, 3):
        first_from[shift] = from_shift(first_rest, "fs", shift)
    k, v, packets = call(
        state_kernel,
        (sds((count, 128), bf16), sds((count, 128), bf16), sds((NZ, PACKET, 128), bf16)),
        (), kv_weight, normed, cols, rows,
        flops=2 * 10**9,
    )
    got = lax.all_to_all(packets, "sp", 0, 0, tiled=True)
    ends, later_rest, pool_z, k = lax.optimization_barrier(
        ((own_tokens[:HALO], own_tokens[count - HALO :]), first_rest, pool_z, k)
    )
    length = lax.axis_size("sp")
    first_from[2] = from_shift(later_rest, "fs", 2)
    low = lax.ppermute(ends[1], "sp", [(i, i + 1) for i in range(length - 1)])
    high = lax.ppermute(ends[0], "sp", [(i + 1, i) for i in range(length - 1)])
    last_from = [pool_z] + [from_shift(pool_z, "fs", s) for s in (1, 2, 3)]
    q, outgate, pool_out, nums, dens, wm = call(
        local_kernel,
        (
            sds((count, 128), bf16),
            sds((count, 128), bf16),
            sds((count, 256), bf16),
            sds((2, count, 128), f32),
            sds((count, 128), f32),
            sds((width, 128), bf16),
        ),
        (), first_rest, first_from[1], first_from[2], first_from[3], normed, low, high,
        norm_gain[None], k, v, cols, rows,
        flops=5 * 10**9,
        scratch=[pltpu.VMEM((NY, NZ * ROWS, 640), bf16)]
        + [pltpu.VMEM((count + 32, 256), f32)] * 2,
    )
    cores = 2
    chips = lax.axis_size("tp") // cores
    own = count // (chips * cores)
    keep, give = call(
        final_kernel, (sds((chips, own, width), bf16),) * 2, (),
        got, init_memory[0, :, 0], init_normalizer[0, :, 0][:, None], cols, q, outgate,
        nums, dens, head_gain, pool_out, wm, *last_from,
        flops=2 * 10**9,
        scratch=[pltpu.VMEM((NY, NZ * ROWS, 256), bf16)],
    )
    swap = [(i, i ^ 1) for i in range(chips * cores)]
    taken = lax.ppermute(give, "tp", swap)
    pairs = (keep.astype(f32) + taken.astype(f32)).astype(bf16)
    groups = [list(range(c, chips * cores, cores)) for c in range(cores)]
    parts = lax.all_to_all(pairs, "tp", 0, 0, axis_index_groups=groups, tiled=True)
    mixed = jnp.sum(parts.astype(f32), axis=0).astype(bf16)
    return mixed.reshape(1, own, width)


def solution(mesh):
    placed = (
        P("fs", "sp", None),
        P(),
        P(("sp", "fs"), "tp"),
        P(("sp", "fs"), "tp"),
        P(("sp", "fs"), "tp"),
        P(("sp", "fs"), "tp"),
        P(None, "tp", None),
        P(None, "tp"),
        P("fs", None, "tp", "sp"),
        P("fs", None, "tp", None, None),
        P("fs", None, "tp", None),
        P("tp", None),
        P(("sp", "fs"), "tp"),
        P(("sp", "fs"), "tp"),
        P(("sp", "fs"), "tp"),
    )

    return jax.shard_map(
        per_device,
        mesh=mesh,
        in_specs=placed,
        out_specs=P("fs", ("sp", "tp"), None),
        check_vma=False,
    )
```

```python
import jax
import jax.numpy as jnp
from jax import lax
from jax.experimental import pallas as pl
from jax.experimental.pallas import tpu as pltpu
from jax.sharding import PartitionSpec as P


HALO = 8
norm_eps = 1e-06
NZ = 16
NY = 4
ROWS = 32
LOWEST = -1e30
PACKET = 144

f32 = jnp.float32
bf16 = jnp.bfloat16
smem = pl.BlockSpec(memory_space=pltpu.SMEM)
vmem = pl.BlockSpec(memory_space=pltpu.VMEM)


def from_everyone(x, axis):
    copies = jnp.broadcast_to(x, (lax.axis_size(axis), *x.shape))
    return lax.all_to_all(copies, axis, split_axis=0, concat_axis=0, tiled=True)


def pack_kernel(k_ref, v_ref, q_ref, o_ref, p_ref, m_ref, po_ref, out_ref, copies_ref):
    for z in range(NZ):
        copies_ref[z] = po_ref[...]
    at = 0
    for ref in (k_ref, v_ref, q_ref, o_ref, p_ref, m_ref):
        width = ref.shape[1]
        out_ref[:, at : at + width] = ref[...]
        at += width


def in_order(w_ref):
    return jnp.concatenate(
        [w_ref[y, z * ROWS : (z + 1) * ROWS] for z in range(NZ) for y in range(NY)], axis=0
    )


def from_shift(x, axis, shift):
    count = lax.axis_size(axis)
    return lax.ppermute(x, axis, [(i, (i + shift) % count) for i in range(count)])


def placed_by_source(y, refs, out_ref):
    for shift, ref in enumerate(refs):
        out_ref[lax.rem(y + NY - shift, NY)] = ref[...]


def rms_normed(x, gain):
    return x * lax.rsqrt(jnp.mean(x * x, axis=-1, keepdims=True) + norm_eps) * gain


def log_sigmoid(x):
    return jnp.minimum(x, 0.0) - jnp.log1p(jnp.exp(-jnp.abs(x)))


def gates_kernel(bias_ref, tok_ref, gain_ref, gw_ref, decay_ref, normed_ref, cols_ref, rows_ref, ends_ref):
    x = tok_ref[...].astype(f32)
    ends_ref[:HALO] = tok_ref[:HALO]
    ends_ref[HALO:] = tok_ref[tok_ref.shape[0] - HALO :]
    count = x.shape[0]
    normed = rms_normed(x, gain_ref[...]).astype(bf16)
    normed_ref[...] = normed
    pre = lax.dot_general(
        gw_ref[...], normed, (((1,), (1,)), ((), ())), preferred_element_type=f32
    )
    pre = [pre[g : g + 1] + bias_ref[g] for g in range(4)]
    in_rows = (pre[0], pre[2])
    lf_rows = (log_sigmoid(pre[1]) + decay_ref[0], log_sigmoid(pre[3]) + decay_ref[1])
    stacked = jnp.concatenate(
        [in_rows[0], in_rows[1], lf_rows[0], lf_rows[1], jnp.zeros((124, count), f32)], axis=0
    )
    turned = stacked.T
    first = lax.broadcasted_iota(jnp.int32, (count, count), 0)
    second = lax.broadcasted_iota(jnp.int32, (count, count), 1)
    lane = lax.broadcasted_iota(jnp.int32, (count, 128), 1)
    cols = jnp.zeros((count, 128), f32)
    rows = []
    tails = []
    for r in range(2):
        reach = second <= first if r == 0 else second >= first
        reach_t = first <= second if r == 0 else first >= second
        lf_row = lf_rows[r]
        lf_col = turned[:, 2 + r : 3 + r]
        b_col = jnp.sum(jnp.where(reach, lf_row, 0.0), axis=1, keepdims=True)
        b_row = jnp.sum(jnp.where(reach_t, lf_col, 0.0), axis=0, keepdims=True)
        a_row = in_rows[r] - b_row
        a_col = turned[:, r : r + 1] - b_col
        m_col = jnp.max(jnp.where(reach, a_row, LOWEST), axis=1, keepdims=True)
        top = jnp.max(a_row, axis=1, keepdims=True)
        w_col = jnp.exp(a_col - top)
        total = jnp.sum(lf_row, axis=1, keepdims=True)
        for n, col in enumerate((b_col, m_col, w_col)):
            cols = jnp.where(lane == 3 * r + n, col, cols)
        rows.append(a_row)
        tails.append(jnp.broadcast_to(total + top, (1, count)))
        tails.append(jnp.broadcast_to(total, (1, count)))
    cols_ref[...] = cols
    rows_ref[...] = jnp.concatenate(rows + tails + [jnp.zeros((2, count), f32)], axis=0)


def in_three(x):
    high = x.astype(bf16).astype(f32)
    rest = x - high
    mid = rest.astype(bf16).astype(f32)
    low = (rest - mid).astype(bf16).astype(f32)
    return [high, mid, low]


def state_kernel(w_ref, normed_ref, cols_ref, rows_ref, k_ref, v_ref, out_ref):
    position = lax.axis_index("sp")
    weight = in_order(w_ref)
    kv = jnp.dot(normed_ref[...], weight, preferred_element_type=f32).astype(bf16)
    k = kv[:, :128]
    v = kv[:, 128:]
    k_ref[...] = k
    v_ref[...] = v
    scale = 128**-0.5
    k_wide = k.astype(f32)
    v_wide = v.astype(f32)
    packets = []
    for r in range(2):
        w = cols_ref[:, 3 * r + 2 : 3 * r + 3]
        wv = w * v_wide
        high = wv.astype(bf16)
        low = (wv - high.astype(f32)).astype(bf16)
        over_time = (((0,), (0,)), ((), ()))
        memory = lax.dot_general(high, k, over_time, preferred_element_type=f32)
        memory = memory + lax.dot_general(low, k, over_time, preferred_element_type=f32)
        norm = jnp.sum(w * k_wide, axis=0, keepdims=True) * scale
        extra = in_three(norm)
        extra = extra + in_three(rows_ref[2 + 2 * r : 3 + 2 * r, :128])
        extra = extra + in_three(rows_ref[3 + 2 * r : 4 + 2 * r, :128])
        extra = jnp.concatenate(extra + [jnp.zeros((7, 128), f32)], axis=0)
        packets.append(jnp.concatenate([memory * scale, extra], axis=0).astype(bf16))
    for j in range(NZ):

        @pl.when(j > position)
        def _():
            out_ref[j] = packets[0]

        @pl.when(j <= position)
        def _():
            out_ref[j] = packets[1]


def pooled(position, group, centre, low, high, a_ref, b_ref):
    count = centre.shape[0]
    a_ref[0:8] = jnp.zeros_like(a_ref[0:8])
    a_ref[8:16] = low
    a_ref[16 : 16 + count] = centre
    a_ref[16 + count : 24 + count] = high
    a_ref[24 + count : 32 + count] = jnp.zeros_like(a_ref[0:8])
    width = count + 16
    b_ref[...] = jnp.zeros_like(b_ref)
    b_ref[8 : 8 + width] = a_ref[7 : 7 + width] + a_ref[8 : 8 + width]
    total = b_ref[16 : 16 + count]
    refs = (b_ref, a_ref)
    for g in range(1, 4):
        step = 1 << (g - 1)
        src, dst = refs[(g - 1) % 2], refs[g % 2]
        dst[8 : 8 + width] = src[8 - step : 8 - step + width] + src[8 + step : 8 + step + width]
        total = jnp.where(group == g, dst[16 : 16 + count], total)
    left = jnp.left_shift(1, group)
    place = position * count + lax.broadcasted_iota(jnp.int32, (count, 1), 0)
    begin = jnp.maximum(place - left, 0)
    end = jnp.minimum(place + left - 1, NZ * count - 1)
    counted = (end - begin + 1).astype(f32)
    return (total / counted - centre).astype(bf16)


def local_kernel(
    w0_ref, w1_ref, w2_ref, w3_ref, normed_ref, lo_ref, hi_ref, gain_ref,
    k_ref, v_ref, cols_ref, rows_ref,
    q_ref, o_ref, pool_ref, num_ref, den_ref, w_ref, a_ref, b_ref,
):
    placed_by_source(lax.axis_index("fs"), (w0_ref, w1_ref, w2_ref, w3_ref), w_ref)
    weight = in_order(w_ref)
    halo = jnp.concatenate([lo_ref[...], hi_ref[...]], axis=0).astype(f32)
    halo = rms_normed(halo, gain_ref[...]).astype(bf16)
    left = jnp.concatenate([normed_ref[...], halo], axis=0)
    all_three = jnp.dot(left, weight, preferred_element_type=f32).astype(bf16)
    count = normed_ref.shape[0]
    q = all_three[:count, :128]
    q_ref[...] = q
    o_ref[...] = all_three[:count, 128:256]
    p = all_three[:, 256:512].astype(f32)
    pool_ref[...] = pooled(
        lax.axis_index("sp"), lax.div(lax.axis_index("tp"), 2), p[:count], p[count : count + HALO], p[count + HALO :], a_ref, b_ref
    )
    scores = lax.dot_general(
        q, k_ref[...], (((1,), (1,)), ((), ())), preferred_element_type=f32
    ) * (128**-0.5)
    first = lax.broadcasted_iota(jnp.int32, (count, count), 0)
    second = lax.broadcasted_iota(jnp.int32, (count, count), 1)
    lane = lax.broadcasted_iota(jnp.int32, (count, 128), 1)
    dens = jnp.zeros((count, 128), f32)
    for r in range(2):
        reach = second <= first if r == 0 else second >= first
        m_col = cols_ref[:, 3 * r + 1 : 3 * r + 2]
        a_row = rows_ref[r : r + 1]
        weights = jnp.exp(jnp.where(reach, a_row - m_col, LOWEST)) * scores
        num_ref[r] = jnp.dot(weights.astype(bf16), v_ref[...], preferred_element_type=f32)
        dens = jnp.where(lane == r, jnp.sum(weights, axis=1, keepdims=True), dens)
    den_ref[...] = dens


def final_kernel(
    got_ref, mem_ref, nrm_ref, cols_ref, q_ref, o_ref, num_ref, den_ref,
    gain_ref, pool_ref, w0_ref, w1_ref, w2_ref, w3_ref, keep_ref, give_ref, w_ref,
):
    placed_by_source(lax.axis_index("fs"), (w0_ref, w1_ref, w2_ref, w3_ref), w_ref)
    position = lax.axis_index("sp")
    got_n, got_m, got_f = [], [], []
    for j in range(NZ):
        extra = got_ref[j, 128:PACKET].astype(f32)
        got_n.append(extra[0:1] + extra[1:2] + extra[2:3])
        got_m.append(extra[3:4] + extra[4:5] + extra[5:6])
        got_f.append(extra[6:7] + extra[7:8] + extra[8:9])
    q = q_ref[...]
    q_wide = q.astype(f32)
    last = (((1,), (1,)), ((), ()))
    summed = None
    for r in range(2):
        order = range(NZ - 1, -1, -1) if r == 0 else range(NZ)
        levels = [None] * NZ
        passed = jnp.zeros((1, 128), f32)
        for j in order:
            ahead = j < position if r == 0 else j > position
            levels[j] = jnp.where(ahead, got_m[j] + passed, LOWEST)
            passed = passed + jnp.where(ahead, got_f[j], 0.0)
        top = passed
        for j in range(NZ):
            top = jnp.maximum(top, levels[j])
        share = jnp.exp(passed - top)
        memory = share * mem_ref[r]
        norm = share * nrm_ref[r]
        for j in range(NZ):
            share = jnp.exp(levels[j] - top)
            memory = memory + share * got_ref[j, 0:128].astype(f32)
            norm = norm + share * got_n[j]
        high = memory.astype(bf16)
        low = (memory - high.astype(f32)).astype(bf16)
        carried = lax.dot_general(q, high, last, preferred_element_type=f32)
        carried = carried + lax.dot_general(q, low, last, preferred_element_type=f32)
        carried_den = jnp.sum(q_wide * norm, axis=1, keepdims=True)
        b_col = cols_ref[:, 3 * r : 3 * r + 1]
        m_col = cols_ref[:, 3 * r + 1 : 3 * r + 2]
        stab = top[:, 0:1]
        joint = jnp.maximum(stab, m_col)
        carry = jnp.exp(stab - joint)
        keep = jnp.exp(m_col - joint)
        numerator = carry * carried + keep * num_ref[r]
        denominator = carry * carried_den + keep * den_ref[:, r : r + 1]
        floor = jnp.exp(-(b_col + joint))
        part = numerator / jnp.maximum(jnp.abs(denominator), floor)
        summed = part if summed is None else summed + part
    scaled = summed * lax.rsqrt(jnp.mean(summed * summed, axis=-1, keepdims=True) + norm_eps)
    gate = 1.0 / (1.0 + jnp.exp(-o_ref[...].astype(f32)))
    memory_out = (scaled * gain_ref[...] * gate).astype(bf16)
    features = jnp.concatenate([memory_out, pool_ref[...]], axis=1)
    result = lax.dot_general(features, in_order(w_ref), last, preferred_element_type=f32)
    core = lax.rem(lax.axis_index("tp"), 2)
    own = keep_ref.shape[1]
    for x in range(keep_ref.shape[0]):
        south = result[2 * x * own : (2 * x + 1) * own]
        north = result[(2 * x + 1) * own : (2 * x + 2) * own]
        keep_ref[x] = jnp.where(core == 0, south, north).astype(bf16)
        give_ref[x] = jnp.where(core == 0, north, south).astype(bf16)


def sds(shape, dtype):
    return jax.ShapeDtypeStruct(shape, dtype)


def call(kernel, outs, scalars, *args, flops=0, scratch=()):
    many = isinstance(outs, tuple)
    return pl.pallas_call(
        kernel,
        in_specs=[smem] * len(scalars) + [vmem] * len(args),
        out_specs=(vmem,) * len(outs) if many else vmem,
        out_shape=outs,
        scratch_shapes=list(scratch),
        cost_estimate=pl.CostEstimate(flops=flops, bytes_accessed=0, transcendentals=0),
    )(*scalars, *args)


def per_device(
    tokens,
    norm_gain,
    query_weight,
    key_weight,
    value_weight,
    outgate_weight,
    gate_weight,
    gate_bias,
    decay_extra,
    init_memory,
    init_normalizer,
    head_gain,
    pool_weight,
    mem_out_weight,
    pool_out_weight,
):
    count, width = tokens.shape[1:]
    packed, pool_copies = call(
        pack_kernel, (sds((ROWS, 896), bf16), sds((NZ, ROWS, 256), bf16)), (),
        key_weight, value_weight, query_weight, outgate_weight, pool_weight, mem_out_weight,
        pool_out_weight,
        flops=10**6,
    )
    pool_z = lax.all_to_all(pool_copies, "sp", 0, 0, tiled=True).reshape(NZ * ROWS, 256)
    along_z = lax.all_gather(packed, "sp", axis=0, tiled=True)
    kv_z, pool_z = lax.optimization_barrier((along_z[:, :256], pool_z))
    kv_weight = from_everyone(kv_z, "fs")
    own_tokens, along_z = lax.optimization_barrier((tokens[0], along_z))
    normed, cols, rows, ends = call(
        gates_kernel,
        (
            sds((count, width), bf16),
            sds((count, 128), f32),
            sds((8, count), f32),
            sds((2 * HALO, width), bf16),
        ),
        (gate_bias.reshape(4),),
        own_tokens,
        norm_gain[None],
        gate_weight[:, 0],
        decay_extra[0, :, 0][:, None],
        flops=4 * 10**9,
    )
    first_rest, rows = lax.optimization_barrier((along_z[:, 256:768], rows))
    first_from = {}
    for shift in (1, 2, 3):
        first_from[shift] = from_shift(first_rest, "fs", shift)
    k, v, packets = call(
        state_kernel,
        (sds((count, 128), bf16), sds((count, 128), bf16), sds((NZ, PACKET, 128), bf16)),
        (), kv_weight, normed, cols, rows,
        flops=2 * 10**9,
    )
    got = lax.all_to_all(packets, "sp", 0, 0, tiled=True)
    last_rest, k = lax.optimization_barrier(
        (jnp.concatenate([along_z[:, 768:], pool_z], axis=1), k)
    )
    length = lax.axis_size("sp")
    last_from = [last_rest]
    for shift in (1, 2, 3):
        last_from.append(from_shift(last_rest, "fs", shift))
    low = lax.ppermute(ends[HALO:], "sp", [(i, i + 1) for i in range(length - 1)])
    high = lax.ppermute(ends[:HALO], "sp", [(i + 1, i) for i in range(length - 1)])
    q, outgate, pool_out, nums, dens = call(
        local_kernel,
        (
            sds((count, 128), bf16),
            sds((count, 128), bf16),
            sds((count, 256), bf16),
            sds((2, count, 128), f32),
            sds((count, 128), f32),
        ),
        (), first_rest, *(first_from[s] for s in (1, 2, 3)), normed, low, high,
        norm_gain[None], k, v, cols, rows,
        flops=5 * 10**9,
        scratch=[pltpu.VMEM((NY, NZ * ROWS, 512), bf16)]
        + [pltpu.VMEM((count + 32, 256), f32)] * 2,
    )
    cores = 2
    chips = lax.axis_size("tp") // cores
    own = count // (chips * cores)
    keep, give = call(
        final_kernel, (sds((chips, own, width), bf16),) * 2, (),
        got, init_memory[0, :, 0], init_normalizer[0, :, 0][:, None], cols, q, outgate,
        nums, dens, head_gain, pool_out, *last_from,
        flops=2 * 10**9,
        scratch=[pltpu.VMEM((NY, NZ * ROWS, 384), bf16)],
    )
    swap = [(i, i ^ 1) for i in range(chips * cores)]
    taken = lax.ppermute(give, "tp", swap)
    pairs = (keep.astype(f32) + taken.astype(f32)).astype(bf16)
    groups = [list(range(c, chips * cores, cores)) for c in range(cores)]
    parts = lax.all_to_all(pairs, "tp", 0, 0, axis_index_groups=groups, tiled=True)
    mixed = jnp.sum(parts.astype(f32), axis=0).astype(bf16)
    return mixed.reshape(1, own, width)


def solution(mesh):
    placed = (
        P("fs", "sp", None),
        P(),
        P(("sp", "fs"), "tp"),
        P(("sp", "fs"), "tp"),
        P(("sp", "fs"), "tp"),
        P(("sp", "fs"), "tp"),
        P(None, "tp", None),
        P(None, "tp"),
        P("fs", None, "tp", "sp"),
        P("fs", None, "tp", None, None),
        P("fs", None, "tp", None),
        P("tp", None),
        P(("sp", "fs"), "tp"),
        P(("sp", "fs"), "tp"),
        P(("sp", "fs"), "tp"),
    )

    return jax.shard_map(
        per_device,
        mesh=mesh,
        in_specs=placed,
        out_specs=P("fs", ("sp", "tp"), None),
        check_vma=False,
    )
```

```python
import jax
import jax.numpy as jnp
from jax import lax
from jax.experimental import pallas as pl
from jax.experimental.pallas import tpu as pltpu
from jax.sharding import PartitionSpec as P


HALO = 8
norm_eps = 1e-06
NZ = 16
NY = 4
ROWS = 32
LOWEST = -1e30
PACKET = 144

f32 = jnp.float32
bf16 = jnp.bfloat16
smem = pl.BlockSpec(memory_space=pltpu.SMEM)
vmem = pl.BlockSpec(memory_space=pltpu.VMEM)


def from_everyone(x, axis):
    copies = jnp.broadcast_to(x, (lax.axis_size(axis), *x.shape))
    return lax.all_to_all(copies, axis, split_axis=0, concat_axis=0, tiled=True)


def pack_kernel(k_ref, v_ref, q_ref, o_ref, p_ref, m_ref, po_ref, out_ref, copies_ref):
    for z in range(NZ):
        copies_ref[z] = po_ref[...]
    at = 0
    for ref in (k_ref, v_ref, q_ref, o_ref, p_ref, m_ref):
        width = ref.shape[1]
        out_ref[:, at : at + width] = ref[...]
        at += width


def in_order(w_ref):
    return jnp.concatenate(
        [w_ref[y, z * ROWS : (z + 1) * ROWS] for z in range(NZ) for y in range(NY)], axis=0
    )


def from_shift(x, axis, shift):
    count = lax.axis_size(axis)
    return lax.ppermute(x, axis, [(i, (i + shift) % count) for i in range(count)])


def placed_by_source(y, refs, out_ref):
    for shift, ref in enumerate(refs):
        out_ref[lax.rem(y + NY - shift, NY)] = ref[...]


def rms_normed(x, gain):
    return x * lax.rsqrt(jnp.mean(x * x, axis=-1, keepdims=True) + norm_eps) * gain


def log_sigmoid(x):
    return jnp.minimum(x, 0.0) - jnp.log1p(jnp.exp(-jnp.abs(x)))


def gates_kernel(bias_ref, tok_ref, gain_ref, gw_ref, decay_ref, normed_ref, cols_ref, rows_ref, ends_ref):
    x = tok_ref[...].astype(f32)
    ends_ref[:HALO] = tok_ref[:HALO]
    ends_ref[HALO:] = tok_ref[tok_ref.shape[0] - HALO :]
    count = x.shape[0]
    normed = rms_normed(x, gain_ref[...]).astype(bf16)
    normed_ref[...] = normed
    pre = lax.dot_general(
        gw_ref[...], normed, (((1,), (1,)), ((), ())), preferred_element_type=f32
    )
    pre = [pre[g : g + 1] + bias_ref[g] for g in range(4)]
    in_rows = (pre[0], pre[2])
    lf_rows = (log_sigmoid(pre[1]) + decay_ref[0], log_sigmoid(pre[3]) + decay_ref[1])
    stacked = jnp.concatenate(
        [in_rows[0], in_rows[1], lf_rows[0], lf_rows[1], jnp.zeros((124, count), f32)], axis=0
    )
    turned = stacked.T
    first = lax.broadcasted_iota(jnp.int32, (count, count), 0)
    second = lax.broadcasted_iota(jnp.int32, (count, count), 1)
    lane = lax.broadcasted_iota(jnp.int32, (count, 128), 1)
    cols = jnp.zeros((count, 128), f32)
    rows = []
    tails = []
    for r in range(2):
        reach = second <= first if r == 0 else second >= first
        reach_t = first <= second if r == 0 else first >= second
        lf_row = lf_rows[r]
        lf_col = turned[:, 2 + r : 3 + r]
        b_col = jnp.sum(jnp.where(reach, lf_row, 0.0), axis=1, keepdims=True)
        b_row = jnp.sum(jnp.where(reach_t, lf_col, 0.0), axis=0, keepdims=True)
        a_row = in_rows[r] - b_row
        a_col = turned[:, r : r + 1] - b_col
        m_col = jnp.max(jnp.where(reach, a_row, LOWEST), axis=1, keepdims=True)
        top = jnp.max(a_row, axis=1, keepdims=True)
        w_col = jnp.exp(a_col - top)
        total = jnp.sum(lf_row, axis=1, keepdims=True)
        for n, col in enumerate((b_col, m_col, w_col)):
            cols = jnp.where(lane == 3 * r + n, col, cols)
        rows.append(a_row)
        tails.append(jnp.broadcast_to(total + top, (1, count)))
        tails.append(jnp.broadcast_to(total, (1, count)))
    cols_ref[...] = cols
    rows_ref[...] = jnp.concatenate(rows + tails + [jnp.zeros((2, count), f32)], axis=0)


def in_three(x):
    high = x.astype(bf16).astype(f32)
    rest = x - high
    mid = rest.astype(bf16).astype(f32)
    low = (rest - mid).astype(bf16).astype(f32)
    return [high, mid, low]


def state_kernel(w_ref, normed_ref, cols_ref, rows_ref, k_ref, v_ref, out_ref):
    position = lax.axis_index("sp")
    weight = in_order(w_ref)
    kv = jnp.dot(normed_ref[...], weight, preferred_element_type=f32).astype(bf16)
    k = kv[:, :128]
    v = kv[:, 128:]
    k_ref[...] = k
    v_ref[...] = v
    scale = 128**-0.5
    k_wide = k.astype(f32)
    v_wide = v.astype(f32)
    packets = []
    for r in range(2):
        w = cols_ref[:, 3 * r + 2 : 3 * r + 3]
        wv = w * v_wide
        high = wv.astype(bf16)
        low = (wv - high.astype(f32)).astype(bf16)
        over_time = (((0,), (0,)), ((), ()))
        memory = lax.dot_general(high, k, over_time, preferred_element_type=f32)
        memory = memory + lax.dot_general(low, k, over_time, preferred_element_type=f32)
        norm = jnp.sum(w * k_wide, axis=0, keepdims=True) * scale
        extra = in_three(norm)
        extra = extra + in_three(rows_ref[2 + 2 * r : 3 + 2 * r, :128])
        extra = extra + in_three(rows_ref[3 + 2 * r : 4 + 2 * r, :128])
        extra = jnp.concatenate(extra + [jnp.zeros((7, 128), f32)], axis=0)
        packets.append(jnp.concatenate([memory * scale, extra], axis=0).astype(bf16))
    for j in range(NZ):

        @pl.when(j > position)
        def _():
            out_ref[j] = packets[0]

        @pl.when(j <= position)
        def _():
            out_ref[j] = packets[1]


def pooled(position, group, centre, low, high, a_ref, b_ref):
    count = centre.shape[0]
    a_ref[0:8] = jnp.zeros_like(a_ref[0:8])
    a_ref[8:16] = low
    a_ref[16 : 16 + count] = centre
    a_ref[16 + count : 24 + count] = high
    a_ref[24 + count : 32 + count] = jnp.zeros_like(a_ref[0:8])
    width = count + 16
    b_ref[...] = jnp.zeros_like(b_ref)
    b_ref[8 : 8 + width] = a_ref[7 : 7 + width] + a_ref[8 : 8 + width]
    total = b_ref[16 : 16 + count]
    refs = (b_ref, a_ref)
    for g in range(1, 4):
        step = 1 << (g - 1)
        src, dst = refs[(g - 1) % 2], refs[g % 2]
        dst[8 : 8 + width] = src[8 - step : 8 - step + width] + src[8 + step : 8 + step + width]
        total = jnp.where(group == g, dst[16 : 16 + count], total)
    left = jnp.left_shift(1, group)
    place = position * count + lax.broadcasted_iota(jnp.int32, (count, 1), 0)
    begin = jnp.maximum(place - left, 0)
    end = jnp.minimum(place + left - 1, NZ * count - 1)
    counted = (end - begin + 1).astype(f32)
    return (total / counted - centre).astype(bf16)


def local_kernel(
    w0_ref, w1_ref, w2_ref, w3_ref, normed_ref, lo_ref, hi_ref, gain_ref,
    k_ref, v_ref, cols_ref, rows_ref,
    q_ref, o_ref, pool_ref, num_ref, den_ref, wo_ref, w_ref, a_ref, b_ref,
):
    placed_by_source(lax.axis_index("fs"), (w0_ref, w1_ref, w2_ref, w3_ref), w_ref)
    weight = in_order(w_ref)
    wo_ref[...] = weight[:, 512:]
    weight = weight[:, :512]
    halo = jnp.concatenate([lo_ref[...], hi_ref[...]], axis=0).astype(f32)
    halo = rms_normed(halo, gain_ref[...]).astype(bf16)
    left = jnp.concatenate([normed_ref[...], halo], axis=0)
    all_three = jnp.dot(left, weight, preferred_element_type=f32).astype(bf16)
    count = normed_ref.shape[0]
    q = all_three[:count, :128]
    q_ref[...] = q
    o_ref[...] = all_three[:count, 128:256]
    p = all_three[:, 256:512].astype(f32)
    pool_ref[...] = pooled(
        lax.axis_index("sp"), lax.div(lax.axis_index("tp"), 2), p[:count], p[count : count + HALO], p[count + HALO :], a_ref, b_ref
    )
    scores = lax.dot_general(
        q, k_ref[...], (((1,), (1,)), ((), ())), preferred_element_type=f32
    ) * (128**-0.5)
    first = lax.broadcasted_iota(jnp.int32, (count, count), 0)
    second = lax.broadcasted_iota(jnp.int32, (count, count), 1)
    lane = lax.broadcasted_iota(jnp.int32, (count, 128), 1)
    dens = jnp.zeros((count, 128), f32)
    for r in range(2):
        reach = second <= first if r == 0 else second >= first
        m_col = cols_ref[:, 3 * r + 1 : 3 * r + 2]
        a_row = rows_ref[r : r + 1]
        weights = jnp.exp(jnp.where(reach, a_row - m_col, LOWEST)) * scores
        num_ref[r] = jnp.dot(weights.astype(bf16), v_ref[...], preferred_element_type=f32)
        dens = jnp.where(lane == r, jnp.sum(weights, axis=1, keepdims=True), dens)
    den_ref[...] = dens


def final_kernel(
    got_ref, mem_ref, nrm_ref, cols_ref, q_ref, o_ref, num_ref, den_ref,
    gain_ref, pool_ref, wo_ref, keep_ref, give_ref,
):
    position = lax.axis_index("sp")
    got_n, got_m, got_f = [], [], []
    for j in range(NZ):
        extra = got_ref[j, 128:PACKET].astype(f32)
        got_n.append(extra[0:1] + extra[1:2] + extra[2:3])
        got_m.append(extra[3:4] + extra[4:5] + extra[5:6])
        got_f.append(extra[6:7] + extra[7:8] + extra[8:9])
    q = q_ref[...]
    q_wide = q.astype(f32)
    last = (((1,), (1,)), ((), ()))
    summed = None
    for r in range(2):
        order = range(NZ - 1, -1, -1) if r == 0 else range(NZ)
        levels = [None] * NZ
        passed = jnp.zeros((1, 128), f32)
        for j in order:
            ahead = j < position if r == 0 else j > position
            levels[j] = jnp.where(ahead, got_m[j] + passed, LOWEST)
            passed = passed + jnp.where(ahead, got_f[j], 0.0)
        top = passed
        for j in range(NZ):
            top = jnp.maximum(top, levels[j])
        share = jnp.exp(passed - top)
        memory = share * mem_ref[r]
        norm = share * nrm_ref[r]
        for j in range(NZ):
            share = jnp.exp(levels[j] - top)
            memory = memory + share * got_ref[j, 0:128].astype(f32)
            norm = norm + share * got_n[j]
        high = memory.astype(bf16)
        low = (memory - high.astype(f32)).astype(bf16)
        carried = lax.dot_general(q, high, last, preferred_element_type=f32)
        carried = carried + lax.dot_general(q, low, last, preferred_element_type=f32)
        carried_den = jnp.sum(q_wide * norm, axis=1, keepdims=True)
        b_col = cols_ref[:, 3 * r : 3 * r + 1]
        m_col = cols_ref[:, 3 * r + 1 : 3 * r + 2]
        stab = top[:, 0:1]
        joint = jnp.maximum(stab, m_col)
        carry = jnp.exp(stab - joint)
        keep = jnp.exp(m_col - joint)
        numerator = carry * carried + keep * num_ref[r]
        denominator = carry * carried_den + keep * den_ref[:, r : r + 1]
        floor = jnp.exp(-(b_col + joint))
        part = numerator / jnp.maximum(jnp.abs(denominator), floor)
        summed = part if summed is None else summed + part
    scaled = summed * lax.rsqrt(jnp.mean(summed * summed, axis=-1, keepdims=True) + norm_eps)
    gate = 1.0 / (1.0 + jnp.exp(-o_ref[...].astype(f32)))
    memory_out = (scaled * gain_ref[...] * gate).astype(bf16)
    features = jnp.concatenate([memory_out, pool_ref[...]], axis=1)
    result = lax.dot_general(features, wo_ref[...], last, preferred_element_type=f32)
    core = lax.rem(lax.axis_index("tp"), 2)
    own = keep_ref.shape[1]
    for x in range(keep_ref.shape[0]):
        south = result[2 * x * own : (2 * x + 1) * own]
        north = result[(2 * x + 1) * own : (2 * x + 2) * own]
        keep_ref[x] = jnp.where(core == 0, south, north).astype(bf16)
        give_ref[x] = jnp.where(core == 0, north, south).astype(bf16)


def sds(shape, dtype):
    return jax.ShapeDtypeStruct(shape, dtype)


def call(kernel, outs, scalars, *args, flops=0, scratch=()):
    many = isinstance(outs, tuple)
    return pl.pallas_call(
        kernel,
        in_specs=[smem] * len(scalars) + [vmem] * len(args),
        out_specs=(vmem,) * len(outs) if many else vmem,
        out_shape=outs,
        scratch_shapes=list(scratch),
        cost_estimate=pl.CostEstimate(flops=flops, bytes_accessed=0, transcendentals=0),
    )(*scalars, *args)


def per_device(
    tokens,
    norm_gain,
    query_weight,
    key_weight,
    value_weight,
    outgate_weight,
    gate_weight,
    gate_bias,
    decay_extra,
    init_memory,
    init_normalizer,
    head_gain,
    pool_weight,
    mem_out_weight,
    pool_out_weight,
):
    count, width = tokens.shape[1:]
    packed, pool_copies = call(
        pack_kernel, (sds((ROWS, 896), bf16), sds((NZ, ROWS, 256), bf16)), (),
        key_weight, value_weight, query_weight, outgate_weight, pool_weight, mem_out_weight,
        pool_out_weight,
        flops=10**6,
    )
    pool_z = lax.all_to_all(pool_copies, "sp", 0, 0, tiled=True).reshape(NZ * ROWS, 256)
    along_z = lax.all_gather(packed, "sp", axis=0, tiled=True)
    kv_z, pool_z = lax.optimization_barrier((along_z[:, :256], pool_z))
    kv_weight = from_everyone(kv_z, "fs")
    own_tokens, along_z = lax.optimization_barrier((tokens[0], along_z))
    normed, cols, rows, ends = call(
        gates_kernel,
        (
            sds((count, width), bf16),
            sds((count, 128), f32),
            sds((8, count), f32),
            sds((2 * HALO, width), bf16),
        ),
        (gate_bias.reshape(4),),
        own_tokens,
        norm_gain[None],
        gate_weight[:, 0],
        decay_extra[0, :, 0][:, None],
        flops=4 * 10**9,
    )
    first_rest, rows = lax.optimization_barrier(
        (jnp.concatenate([along_z[:, 256:], pool_z], axis=1), rows)
    )
    first_from = {}
    for shift in (1, 3):
        first_from[shift] = from_shift(first_rest, "fs", shift)
    k, v, packets = call(
        state_kernel,
        (sds((count, 128), bf16), sds((count, 128), bf16), sds((NZ, PACKET, 128), bf16)),
        (), kv_weight, normed, cols, rows,
        flops=2 * 10**9,
    )
    got = lax.all_to_all(packets, "sp", 0, 0, tiled=True)
    later_rest, k = lax.optimization_barrier((first_rest, k))
    length = lax.axis_size("sp")
    first_from[2] = from_shift(later_rest, "fs", 2)
    low = lax.ppermute(ends[HALO:], "sp", [(i, i + 1) for i in range(length - 1)])
    high = lax.ppermute(ends[:HALO], "sp", [(i + 1, i) for i in range(length - 1)])
    q, outgate, pool_out, nums, dens, wo = call(
        local_kernel,
        (
            sds((count, 128), bf16),
            sds((count, 128), bf16),
            sds((count, 256), bf16),
            sds((2, count, 128), f32),
            sds((count, 128), f32),
            sds((width, 384), bf16),
        ),
        (), first_rest, *(first_from[s] for s in (1, 2, 3)), normed, low, high,
        norm_gain[None], k, v, cols, rows,
        flops=5 * 10**9,
        scratch=[pltpu.VMEM((NY, NZ * ROWS, 896), bf16)]
        + [pltpu.VMEM((count + 32, 256), f32)] * 2,
    )
    cores = 2
    chips = lax.axis_size("tp") // cores
    own = count // (chips * cores)
    keep, give = call(
        final_kernel, (sds((chips, own, width), bf16),) * 2, (),
        got, init_memory[0, :, 0], init_normalizer[0, :, 0][:, None], cols, q, outgate,
        nums, dens, head_gain, pool_out, wo,
        flops=2 * 10**9,
    )
    swap = [(i, i ^ 1) for i in range(chips * cores)]
    taken = lax.ppermute(give, "tp", swap)
    pairs = (keep.astype(f32) + taken.astype(f32)).astype(bf16)
    groups = [list(range(c, chips * cores, cores)) for c in range(cores)]
    parts = lax.all_to_all(pairs, "tp", 0, 0, axis_index_groups=groups, tiled=True)
    mixed = jnp.sum(parts.astype(f32), axis=0).astype(bf16)
    return mixed.reshape(1, own, width)


def solution(mesh):
    placed = (
        P("fs", "sp", None),
        P(),
        P(("sp", "fs"), "tp"),
        P(("sp", "fs"), "tp"),
        P(("sp", "fs"), "tp"),
        P(("sp", "fs"), "tp"),
        P(None, "tp", None),
        P(None, "tp"),
        P("fs", None, "tp", "sp"),
        P("fs", None, "tp", None, None),
        P("fs", None, "tp", None),
        P("tp", None),
        P(("sp", "fs"), "tp"),
        P(("sp", "fs"), "tp"),
        P(("sp", "fs"), "tp"),
    )

    return jax.shard_map(
        per_device,
        mesh=mesh,
        in_specs=placed,
        out_specs=P("fs", ("sp", "tp"), None),
        check_vma=False,
    )
```

```python
import jax
import jax.numpy as jnp
from jax import lax
from jax.experimental import pallas as pl
from jax.experimental.pallas import tpu as pltpu
from jax.sharding import PartitionSpec as P


HALO = 8
norm_eps = 1e-06
NZ = 16
NY = 4
ROWS = 32
LOWEST = -1e30
PACKET = 144

f32 = jnp.float32
bf16 = jnp.bfloat16
smem = pl.BlockSpec(memory_space=pltpu.SMEM)
vmem = pl.BlockSpec(memory_space=pltpu.VMEM)


def from_everyone(x, axis):
    copies = jnp.broadcast_to(x, (lax.axis_size(axis), *x.shape))
    return lax.all_to_all(copies, axis, split_axis=0, concat_axis=0, tiled=True)


def pack_kernel(k_ref, v_ref, q_ref, o_ref, p_ref, m_ref, po_ref, out_ref, copies_ref):
    for z in range(NZ):
        copies_ref[z] = po_ref[...]
    at = 0
    for ref in (k_ref, v_ref, q_ref, o_ref, p_ref, m_ref):
        width = ref.shape[1]
        out_ref[:, at : at + width] = ref[...]
        at += width


def in_order(w_ref):
    return jnp.concatenate(
        [w_ref[y, z * ROWS : (z + 1) * ROWS] for z in range(NZ) for y in range(NY)], axis=0
    )


def from_shift(x, axis, shift):
    count = lax.axis_size(axis)
    return lax.ppermute(x, axis, [(i, (i + shift) % count) for i in range(count)])


def placed_by_source(y, refs, out_ref, lo, hi):
    for shift, ref in enumerate(refs):
        piece = ref[...] if ref.shape[1] == hi - lo else ref[:, lo:hi]
        out_ref[lax.rem(y + NY - shift, NY)] = piece


def rms_normed(x, gain):
    return x * lax.rsqrt(jnp.mean(x * x, axis=-1, keepdims=True) + norm_eps) * gain


def log_sigmoid(x):
    return jnp.minimum(x, 0.0) - jnp.log1p(jnp.exp(-jnp.abs(x)))


def gates_kernel(bias_ref, tok_ref, gain_ref, gw_ref, decay_ref, normed_ref, cols_ref, rows_ref, ends_ref):
    x = tok_ref[...].astype(f32)
    ends_ref[:HALO] = tok_ref[:HALO]
    ends_ref[HALO:] = tok_ref[tok_ref.shape[0] - HALO :]
    count = x.shape[0]
    normed = rms_normed(x, gain_ref[...]).astype(bf16)
    normed_ref[...] = normed
    pre = lax.dot_general(
        gw_ref[...], normed, (((1,), (1,)), ((), ())), preferred_element_type=f32
    )
    pre = [pre[g : g + 1] + bias_ref[g] for g in range(4)]
    in_rows = (pre[0], pre[2])
    lf_rows = (log_sigmoid(pre[1]) + decay_ref[0], log_sigmoid(pre[3]) + decay_ref[1])
    stacked = jnp.concatenate(
        [in_rows[0], in_rows[1], lf_rows[0], lf_rows[1], jnp.zeros((124, count), f32)], axis=0
    )
    turned = stacked.T
    first = lax.broadcasted_iota(jnp.int32, (count, count), 0)
    second = lax.broadcasted_iota(jnp.int32, (count, count), 1)
    lane = lax.broadcasted_iota(jnp.int32, (count, 128), 1)
    cols = jnp.zeros((count, 128), f32)
    rows = []
    tails = []
    for r in range(2):
        reach = second <= first if r == 0 else second >= first
        reach_t = first <= second if r == 0 else first >= second
        lf_row = lf_rows[r]
        lf_col = turned[:, 2 + r : 3 + r]
        b_col = jnp.sum(jnp.where(reach, lf_row, 0.0), axis=1, keepdims=True)
        b_row = jnp.sum(jnp.where(reach_t, lf_col, 0.0), axis=0, keepdims=True)
        a_row = in_rows[r] - b_row
        a_col = turned[:, r : r + 1] - b_col
        m_col = jnp.max(jnp.where(reach, a_row, LOWEST), axis=1, keepdims=True)
        top = jnp.max(a_row, axis=1, keepdims=True)
        w_col = jnp.exp(a_col - top)
        total = jnp.sum(lf_row, axis=1, keepdims=True)
        for n, col in enumerate((b_col, m_col, w_col)):
            cols = jnp.where(lane == 3 * r + n, col, cols)
        rows.append(a_row)
        tails.append(jnp.broadcast_to(total + top, (1, count)))
        tails.append(jnp.broadcast_to(total, (1, count)))
    cols_ref[...] = cols
    rows_ref[...] = jnp.concatenate(rows + tails + [jnp.zeros((2, count), f32)], axis=0)


def in_three(x):
    high = x.astype(bf16).astype(f32)
    rest = x - high
    mid = rest.astype(bf16).astype(f32)
    low = (rest - mid).astype(bf16).astype(f32)
    return [high, mid, low]


def state_kernel(w_ref, normed_ref, cols_ref, rows_ref, k_ref, v_ref, out_ref):
    position = lax.axis_index("sp")
    weight = in_order(w_ref)
    kv = jnp.dot(normed_ref[...], weight, preferred_element_type=f32).astype(bf16)
    k = kv[:, :128]
    v = kv[:, 128:]
    k_ref[...] = k
    v_ref[...] = v
    scale = 128**-0.5
    k_wide = k.astype(f32)
    v_wide = v.astype(f32)
    packets = []
    for r in range(2):
        w = cols_ref[:, 3 * r + 2 : 3 * r + 3]
        wv = w * v_wide
        high = wv.astype(bf16)
        low = (wv - high.astype(f32)).astype(bf16)
        over_time = (((0,), (0,)), ((), ()))
        memory = lax.dot_general(high, k, over_time, preferred_element_type=f32)
        memory = memory + lax.dot_general(low, k, over_time, preferred_element_type=f32)
        norm = jnp.sum(w * k_wide, axis=0, keepdims=True) * scale
        extra = in_three(norm)
        extra = extra + in_three(rows_ref[2 + 2 * r : 3 + 2 * r, :128])
        extra = extra + in_three(rows_ref[3 + 2 * r : 4 + 2 * r, :128])
        extra = jnp.concatenate(extra + [jnp.zeros((7, 128), f32)], axis=0)
        packets.append(jnp.concatenate([memory * scale, extra], axis=0).astype(bf16))
    for j in range(NZ):

        @pl.when(j > position)
        def _():
            out_ref[j] = packets[0]

        @pl.when(j <= position)
        def _():
            out_ref[j] = packets[1]


def pooled(position, group, centre, low, high, a_ref, b_ref):
    count = centre.shape[0]
    a_ref[0:8] = jnp.zeros_like(a_ref[0:8])
    a_ref[8:16] = low
    a_ref[16 : 16 + count] = centre
    a_ref[16 + count : 24 + count] = high
    a_ref[24 + count : 32 + count] = jnp.zeros_like(a_ref[0:8])
    width = count + 16
    b_ref[...] = jnp.zeros_like(b_ref)
    b_ref[8 : 8 + width] = a_ref[7 : 7 + width] + a_ref[8 : 8 + width]
    total = b_ref[16 : 16 + count]
    refs = (b_ref, a_ref)
    for g in range(1, 4):
        step = 1 << (g - 1)
        src, dst = refs[(g - 1) % 2], refs[g % 2]
        dst[8 : 8 + width] = src[8 - step : 8 - step + width] + src[8 + step : 8 + step + width]
        total = jnp.where(group == g, dst[16 : 16 + count], total)
    left = jnp.left_shift(1, group)
    place = position * count + lax.broadcasted_iota(jnp.int32, (count, 1), 0)
    begin = jnp.maximum(place - left, 0)
    end = jnp.minimum(place + left - 1, NZ * count - 1)
    counted = (end - begin + 1).astype(f32)
    return (total / counted - centre).astype(bf16)


def local_kernel(
    w0_ref, w1_ref, w2_ref, w3_ref, normed_ref, lo_ref, hi_ref, gain_ref,
    k_ref, v_ref, cols_ref, rows_ref,
    q_ref, o_ref, pool_ref, num_ref, den_ref, w_ref, a_ref, b_ref,
):
    placed_by_source(lax.axis_index("fs"), (w0_ref, w1_ref, w2_ref, w3_ref), w_ref, 0, 512)
    weight = in_order(w_ref)
    halo = jnp.concatenate([lo_ref[...], hi_ref[...]], axis=0).astype(f32)
    halo = rms_normed(halo, gain_ref[...]).astype(bf16)
    left = jnp.concatenate([normed_ref[...], halo], axis=0)
    all_three = jnp.dot(left, weight, preferred_element_type=f32).astype(bf16)
    count = normed_ref.shape[0]
    q = all_three[:count, :128]
    q_ref[...] = q
    o_ref[...] = all_three[:count, 128:256]
    p = all_three[:, 256:512].astype(f32)
    pool_ref[...] = pooled(
        lax.axis_index("sp"), lax.div(lax.axis_index("tp"), 2), p[:count], p[count : count + HALO], p[count + HALO :], a_ref, b_ref
    )
    scores = lax.dot_general(
        q, k_ref[...], (((1,), (1,)), ((), ())), preferred_element_type=f32
    ) * (128**-0.5)
    first = lax.broadcasted_iota(jnp.int32, (count, count), 0)
    second = lax.broadcasted_iota(jnp.int32, (count, count), 1)
    lane = lax.broadcasted_iota(jnp.int32, (count, 128), 1)
    dens = jnp.zeros((count, 128), f32)
    for r in range(2):
        reach = second <= first if r == 0 else second >= first
        m_col = cols_ref[:, 3 * r + 1 : 3 * r + 2]
        a_row = rows_ref[r : r + 1]
        weights = jnp.exp(jnp.where(reach, a_row - m_col, LOWEST)) * scores
        num_ref[r] = jnp.dot(weights.astype(bf16), v_ref[...], preferred_element_type=f32)
        dens = jnp.where(lane == r, jnp.sum(weights, axis=1, keepdims=True), dens)
    den_ref[...] = dens


def outs_kernel(w0_ref, w1_ref, w2_ref, w3_ref, out_ref, w_ref):
    placed_by_source(lax.axis_index("fs"), (w0_ref, w1_ref, w2_ref, w3_ref), w_ref, 512, 896)
    out_ref[...] = in_order(w_ref)


def final_kernel(
    got_ref, mem_ref, nrm_ref, cols_ref, q_ref, o_ref, num_ref, den_ref,
    gain_ref, pool_ref, wo_ref, keep_ref, give_ref,
):
    position = lax.axis_index("sp")
    got_n, got_m, got_f = [], [], []
    for j in range(NZ):
        extra = got_ref[j, 128:PACKET].astype(f32)
        got_n.append(extra[0:1] + extra[1:2] + extra[2:3])
        got_m.append(extra[3:4] + extra[4:5] + extra[5:6])
        got_f.append(extra[6:7] + extra[7:8] + extra[8:9])
    q = q_ref[...]
    q_wide = q.astype(f32)
    last = (((1,), (1,)), ((), ()))
    summed = None
    for r in range(2):
        order = range(NZ - 1, -1, -1) if r == 0 else range(NZ)
        levels = [None] * NZ
        passed = jnp.zeros((1, 128), f32)
        for j in order:
            ahead = j < position if r == 0 else j > position
            levels[j] = jnp.where(ahead, got_m[j] + passed, LOWEST)
            passed = passed + jnp.where(ahead, got_f[j], 0.0)
        top = passed
        for j in range(NZ):
            top = jnp.maximum(top, levels[j])
        share = jnp.exp(passed - top)
        memory = share * mem_ref[r]
        norm = share * nrm_ref[r]
        for j in range(NZ):
            share = jnp.exp(levels[j] - top)
            memory = memory + share * got_ref[j, 0:128].astype(f32)
            norm = norm + share * got_n[j]
        high = memory.astype(bf16)
        low = (memory - high.astype(f32)).astype(bf16)
        carried = lax.dot_general(q, high, last, preferred_element_type=f32)
        carried = carried + lax.dot_general(q, low, last, preferred_element_type=f32)
        carried_den = jnp.sum(q_wide * norm, axis=1, keepdims=True)
        b_col = cols_ref[:, 3 * r : 3 * r + 1]
        m_col = cols_ref[:, 3 * r + 1 : 3 * r + 2]
        stab = top[:, 0:1]
        joint = jnp.maximum(stab, m_col)
        carry = jnp.exp(stab - joint)
        keep = jnp.exp(m_col - joint)
        numerator = carry * carried + keep * num_ref[r]
        denominator = carry * carried_den + keep * den_ref[:, r : r + 1]
        floor = jnp.exp(-(b_col + joint))
        part = numerator / jnp.maximum(jnp.abs(denominator), floor)
        summed = part if summed is None else summed + part
    scaled = summed * lax.rsqrt(jnp.mean(summed * summed, axis=-1, keepdims=True) + norm_eps)
    gate = 1.0 / (1.0 + jnp.exp(-o_ref[...].astype(f32)))
    memory_out = (scaled * gain_ref[...] * gate).astype(bf16)
    features = jnp.concatenate([memory_out, pool_ref[...]], axis=1)
    result = lax.dot_general(features, wo_ref[...], last, preferred_element_type=f32)
    core = lax.rem(lax.axis_index("tp"), 2)
    own = keep_ref.shape[1]
    for x in range(keep_ref.shape[0]):
        south = result[2 * x * own : (2 * x + 1) * own]
        north = result[(2 * x + 1) * own : (2 * x + 2) * own]
        keep_ref[x] = jnp.where(core == 0, south, north).astype(bf16)
        give_ref[x] = jnp.where(core == 0, north, south).astype(bf16)


def sds(shape, dtype):
    return jax.ShapeDtypeStruct(shape, dtype)


def call(kernel, outs, scalars, *args, flops=0, scratch=()):
    many = isinstance(outs, tuple)
    return pl.pallas_call(
        kernel,
        in_specs=[smem] * len(scalars) + [vmem] * len(args),
        out_specs=(vmem,) * len(outs) if many else vmem,
        out_shape=outs,
        scratch_shapes=list(scratch),
        cost_estimate=pl.CostEstimate(flops=flops, bytes_accessed=0, transcendentals=0),
    )(*scalars, *args)


def per_device(
    tokens,
    norm_gain,
    query_weight,
    key_weight,
    value_weight,
    outgate_weight,
    gate_weight,
    gate_bias,
    decay_extra,
    init_memory,
    init_normalizer,
    head_gain,
    pool_weight,
    mem_out_weight,
    pool_out_weight,
):
    count, width = tokens.shape[1:]
    packed, pool_copies = call(
        pack_kernel, (sds((ROWS, 896), bf16), sds((NZ, ROWS, 256), bf16)), (),
        key_weight, value_weight, query_weight, outgate_weight, pool_weight, mem_out_weight,
        pool_out_weight,
        flops=10**6,
    )
    pool_z = lax.all_to_all(pool_copies, "sp", 0, 0, tiled=True).reshape(NZ * ROWS, 256)
    along_z = lax.all_gather(packed, "sp", axis=0, tiled=True)
    kv_z, pool_z = lax.optimization_barrier((along_z[:, :256], pool_z))
    kv_weight = from_everyone(kv_z, "fs")
    own_tokens, along_z = lax.optimization_barrier((tokens[0], along_z))
    normed, cols, rows, ends = call(
        gates_kernel,
        (
            sds((count, width), bf16),
            sds((count, 128), f32),
            sds((8, count), f32),
            sds((2 * HALO, width), bf16),
        ),
        (gate_bias.reshape(4),),
        own_tokens,
        norm_gain[None],
        gate_weight[:, 0],
        decay_extra[0, :, 0][:, None],
        flops=4 * 10**9,
    )
    first_rest, rows = lax.optimization_barrier(
        (jnp.concatenate([along_z[:, 256:], pool_z], axis=1), rows)
    )
    first_from = {}
    for shift in (1, 3):
        first_from[shift] = from_shift(first_rest, "fs", shift)
    length = lax.axis_size("sp")
    low = lax.ppermute(ends[HALO:], "sp", [(i, i + 1) for i in range(length - 1)])
    high = lax.ppermute(ends[:HALO], "sp", [(i + 1, i) for i in range(length - 1)])
    k, v, packets = call(
        state_kernel,
        (sds((count, 128), bf16), sds((count, 128), bf16), sds((NZ, PACKET, 128), bf16)),
        (), kv_weight, normed, cols, rows,
        flops=2 * 10**9,
    )
    got = lax.all_to_all(packets, "sp", 0, 0, tiled=True)
    later_rest, k = lax.optimization_barrier((first_rest, k))
    first_from[2] = from_shift(later_rest[:, :512], "fs", 2)
    last_two = from_shift(later_rest[:, 512:], "fs", 2)
    q, outgate, pool_out, nums, dens = call(
        local_kernel,
        (
            sds((count, 128), bf16),
            sds((count, 128), bf16),
            sds((count, 256), bf16),
            sds((2, count, 128), f32),
            sds((count, 128), f32),
        ),
        (), first_rest, *(first_from[s] for s in (1, 2, 3)), normed, low, high,
        norm_gain[None], k, v, cols, rows,
        flops=5 * 10**9,
        scratch=[pltpu.VMEM((NY, NZ * ROWS, 512), bf16)]
        + [pltpu.VMEM((count + 32, 256), f32)] * 2,
    )
    wo = call(
        outs_kernel, sds((width, 384), bf16), (),
        first_rest, first_from[1], last_two, first_from[3],
        flops=10**8, scratch=[pltpu.VMEM((NY, NZ * ROWS, 384), bf16)],
    )
    cores = 2
    chips = lax.axis_size("tp") // cores
    own = count // (chips * cores)
    keep, give = call(
        final_kernel, (sds((chips, own, width), bf16),) * 2, (),
        got, init_memory[0, :, 0], init_normalizer[0, :, 0][:, None], cols, q, outgate,
        nums, dens, head_gain, pool_out, wo,
        flops=2 * 10**9,
    )
    swap = [(i, i ^ 1) for i in range(chips * cores)]
    taken = lax.ppermute(give, "tp", swap)
    pairs = (keep.astype(f32) + taken.astype(f32)).astype(bf16)
    groups = [list(range(c, chips * cores, cores)) for c in range(cores)]
    parts = lax.all_to_all(pairs, "tp", 0, 0, axis_index_groups=groups, tiled=True)
    mixed = jnp.sum(parts.astype(f32), axis=0).astype(bf16)
    return mixed.reshape(1, own, width)


def solution(mesh):
    placed = (
        P("fs", "sp", None),
        P(),
        P(("sp", "fs"), "tp"),
        P(("sp", "fs"), "tp"),
        P(("sp", "fs"), "tp"),
        P(("sp", "fs"), "tp"),
        P(None, "tp", None),
        P(None, "tp"),
        P("fs", None, "tp", "sp"),
        P("fs", None, "tp", None, None),
        P("fs", None, "tp", None),
        P("tp", None),
        P(("sp", "fs"), "tp"),
        P(("sp", "fs"), "tp"),
        P(("sp", "fs"), "tp"),
    )

    return jax.shard_map(
        per_device,
        mesh=mesh,
        in_specs=placed,
        out_specs=P("fs", ("sp", "tp"), None),
        check_vma=False,
    )
```

```python
import jax
import jax.numpy as jnp
from jax import lax
from jax.experimental import pallas as pl
from jax.experimental.pallas import tpu as pltpu
from jax.sharding import PartitionSpec as P


HALO = 8
norm_eps = 1e-06
NZ = 16
NY = 4
ROWS = 32
LOWEST = -1e30
PACKET = 144

f32 = jnp.float32
bf16 = jnp.bfloat16
smem = pl.BlockSpec(memory_space=pltpu.SMEM)
vmem = pl.BlockSpec(memory_space=pltpu.VMEM)
first_columns = pl.BlockSpec((NZ * ROWS, 384), lambda i: (0, 0), memory_space=pltpu.VMEM)


def from_everyone(x, axis):
    copies = jnp.broadcast_to(x, (lax.axis_size(axis), *x.shape))
    return lax.all_to_all(copies, axis, split_axis=0, concat_axis=0, tiled=True)


def pack_kernel(k_ref, v_ref, q_ref, o_ref, p_ref, m_ref, po_ref, out_ref, copies_ref):
    for z in range(NZ):
        copies_ref[z] = po_ref[...]
    at = 0
    for ref in (k_ref, v_ref, m_ref, q_ref, o_ref, p_ref):
        width = ref.shape[1]
        out_ref[:, at : at + width] = ref[...]
        at += width


def in_order(w_ref):
    return jnp.concatenate(
        [w_ref[y, z * ROWS : (z + 1) * ROWS] for z in range(NZ) for y in range(NY)], axis=0
    )


def from_shift(x, axis, shift):
    count = lax.axis_size(axis)
    return lax.ppermute(x, axis, [(i, (i + shift) % count) for i in range(count)])


def placed_by_source(y, refs, out_ref, lo, hi):
    for shift, ref in enumerate(refs):
        piece = ref[...] if ref.shape[1] == hi - lo else ref[:, lo:hi]
        out_ref[lax.rem(y + NY - shift, NY)] = piece


def rms_normed(x, gain):
    return x * lax.rsqrt(jnp.mean(x * x, axis=-1, keepdims=True) + norm_eps) * gain


def log_sigmoid(x):
    return jnp.minimum(x, 0.0) - jnp.log1p(jnp.exp(-jnp.abs(x)))


def gates_kernel(
    bias_ref, tok_ref, gain_ref, gw_ref, decay_ref, normed_ref, cols_ref, rows_ref,
    begin_ref, end_ref,
):
    x = tok_ref[...].astype(f32)
    begin_ref[...] = tok_ref[:HALO]
    end_ref[...] = tok_ref[tok_ref.shape[0] - HALO :]
    count = x.shape[0]
    normed = rms_normed(x, gain_ref[...]).astype(bf16)
    normed_ref[...] = normed
    pre = lax.dot_general(
        gw_ref[...], normed, (((1,), (1,)), ((), ())), preferred_element_type=f32
    )
    pre = [pre[g : g + 1] + bias_ref[g] for g in range(4)]
    in_rows = (pre[0], pre[2])
    lf_rows = (log_sigmoid(pre[1]) + decay_ref[0], log_sigmoid(pre[3]) + decay_ref[1])
    stacked = jnp.concatenate(
        [in_rows[0], in_rows[1], lf_rows[0], lf_rows[1], jnp.zeros((124, count), f32)], axis=0
    )
    turned = stacked.T
    first = lax.broadcasted_iota(jnp.int32, (count, count), 0)
    second = lax.broadcasted_iota(jnp.int32, (count, count), 1)
    lane = lax.broadcasted_iota(jnp.int32, (count, 128), 1)
    cols = jnp.zeros((count, 128), f32)
    rows = []
    tails = []
    for r in range(2):
        reach = second <= first if r == 0 else second >= first
        reach_t = first <= second if r == 0 else first >= second
        lf_row = lf_rows[r]
        lf_col = turned[:, 2 + r : 3 + r]
        b_col = jnp.sum(jnp.where(reach, lf_row, 0.0), axis=1, keepdims=True)
        b_row = jnp.sum(jnp.where(reach_t, lf_col, 0.0), axis=0, keepdims=True)
        a_row = in_rows[r] - b_row
        a_col = turned[:, r : r + 1] - b_col
        m_col = jnp.max(jnp.where(reach, a_row, LOWEST), axis=1, keepdims=True)
        top = jnp.max(a_row, axis=1, keepdims=True)
        w_col = jnp.exp(a_col - top)
        total = jnp.sum(lf_row, axis=1, keepdims=True)
        for n, col in enumerate((b_col, m_col, w_col)):
            cols = jnp.where(lane == 3 * r + n, col, cols)
        rows.append(a_row)
        tails.append(jnp.broadcast_to(total + top, (1, count)))
        tails.append(jnp.broadcast_to(total, (1, count)))
    cols_ref[...] = cols
    rows_ref[...] = jnp.concatenate(rows + tails + [jnp.zeros((2, count), f32)], axis=0)


def in_three(x):
    high = x.astype(bf16).astype(f32)
    rest = x - high
    mid = rest.astype(bf16).astype(f32)
    low = (rest - mid).astype(bf16).astype(f32)
    return [high, mid, low]


def state_kernel(w_ref, normed_ref, cols_ref, rows_ref, k_ref, v_ref, out_ref):
    position = lax.axis_index("sp")
    weight = in_order(w_ref)
    kv = jnp.dot(normed_ref[...], weight, preferred_element_type=f32).astype(bf16)
    k = kv[:, :128]
    v = kv[:, 128:]
    k_ref[...] = k
    v_ref[...] = v
    scale = 128**-0.5
    k_wide = k.astype(f32)
    v_wide = v.astype(f32)
    packets = []
    for r in range(2):
        w = cols_ref[:, 3 * r + 2 : 3 * r + 3]
        wv = w * v_wide
        high = wv.astype(bf16)
        low = (wv - high.astype(f32)).astype(bf16)
        over_time = (((0,), (0,)), ((), ()))
        memory = lax.dot_general(high, k, over_time, preferred_element_type=f32)
        memory = memory + lax.dot_general(low, k, over_time, preferred_element_type=f32)
        norm = jnp.sum(w * k_wide, axis=0, keepdims=True) * scale
        extra = in_three(norm)
        extra = extra + in_three(rows_ref[2 + 2 * r : 3 + 2 * r, :128])
        extra = extra + in_three(rows_ref[3 + 2 * r : 4 + 2 * r, :128])
        extra = jnp.concatenate(extra + [jnp.zeros((7, 128), f32)], axis=0)
        packets.append(jnp.concatenate([memory * scale, extra], axis=0).astype(bf16))
    for j in range(NZ):

        @pl.when(j > position)
        def _():
            out_ref[j] = packets[0]

        @pl.when(j <= position)
        def _():
            out_ref[j] = packets[1]


def pooled(position, group, centre, low, high, a_ref, b_ref):
    count = centre.shape[0]
    a_ref[0:8] = jnp.zeros_like(a_ref[0:8])
    a_ref[8:16] = low
    a_ref[16 : 16 + count] = centre
    a_ref[16 + count : 24 + count] = high
    a_ref[24 + count : 32 + count] = jnp.zeros_like(a_ref[0:8])
    width = count + 16
    b_ref[...] = jnp.zeros_like(b_ref)
    b_ref[8 : 8 + width] = a_ref[7 : 7 + width] + a_ref[8 : 8 + width]
    total = b_ref[16 : 16 + count]
    refs = (b_ref, a_ref)
    for g in range(1, 4):
        step = 1 << (g - 1)
        src, dst = refs[(g - 1) % 2], refs[g % 2]
        dst[8 : 8 + width] = src[8 - step : 8 - step + width] + src[8 + step : 8 + step + width]
        total = jnp.where(group == g, dst[16 : 16 + count], total)
    left = jnp.left_shift(1, group)
    place = position * count + lax.broadcasted_iota(jnp.int32, (count, 1), 0)
    begin = jnp.maximum(place - left, 0)
    end = jnp.minimum(place + left - 1, NZ * count - 1)
    counted = (end - begin + 1).astype(f32)
    return (total / counted - centre).astype(bf16)


def local_kernel(
    w0_ref, w1_ref, w2_ref, w3_ref, normed_ref, lo_ref, hi_ref, gain_ref,
    k_ref, v_ref, cols_ref, rows_ref,
    q_ref, o_ref, pool_ref, num_ref, den_ref, w_ref, a_ref, b_ref,
):
    placed_by_source(lax.axis_index("fs"), (w0_ref, w1_ref, w2_ref, w3_ref), w_ref, 384, 896)
    weight = in_order(w_ref)
    halo = jnp.concatenate([lo_ref[...], hi_ref[...]], axis=0).astype(f32)
    halo = rms_normed(halo, gain_ref[...]).astype(bf16)
    left = jnp.concatenate([normed_ref[...], halo], axis=0)
    all_three = jnp.dot(left, weight, preferred_element_type=f32).astype(bf16)
    count = normed_ref.shape[0]
    q = all_three[:count, :128]
    q_ref[...] = q
    o_ref[...] = all_three[:count, 128:256]
    p = all_three[:, 256:512].astype(f32)
    pool_ref[...] = pooled(
        lax.axis_index("sp"), lax.div(lax.axis_index("tp"), 2), p[:count], p[count : count + HALO], p[count + HALO :], a_ref, b_ref
    )
    scores = lax.dot_general(
        q, k_ref[...], (((1,), (1,)), ((), ())), preferred_element_type=f32
    ) * (128**-0.5)
    first = lax.broadcasted_iota(jnp.int32, (count, count), 0)
    second = lax.broadcasted_iota(jnp.int32, (count, count), 1)
    lane = lax.broadcasted_iota(jnp.int32, (count, 128), 1)
    dens = jnp.zeros((count, 128), f32)
    for r in range(2):
        reach = second <= first if r == 0 else second >= first
        m_col = cols_ref[:, 3 * r + 1 : 3 * r + 2]
        a_row = rows_ref[r : r + 1]
        weights = jnp.exp(jnp.where(reach, a_row - m_col, LOWEST)) * scores
        num_ref[r] = jnp.dot(weights.astype(bf16), v_ref[...], preferred_element_type=f32)
        dens = jnp.where(lane == r, jnp.sum(weights, axis=1, keepdims=True), dens)
    den_ref[...] = dens


def final_kernel(
    got_ref, mem_ref, nrm_ref, cols_ref, q_ref, o_ref, num_ref, den_ref,
    gain_ref, pool_ref, w0_ref, w1_ref, w2_ref, w3_ref, keep_ref, give_ref, w_ref,
):
    placed_by_source(lax.axis_index("fs"), (w0_ref, w1_ref, w2_ref, w3_ref), w_ref, 0, 384)
    position = lax.axis_index("sp")
    got_n, got_m, got_f = [], [], []
    for j in range(NZ):
        extra = got_ref[j, 128:PACKET].astype(f32)
        got_n.append(extra[0:1] + extra[1:2] + extra[2:3])
        got_m.append(extra[3:4] + extra[4:5] + extra[5:6])
        got_f.append(extra[6:7] + extra[7:8] + extra[8:9])
    q = q_ref[...]
    q_wide = q.astype(f32)
    last = (((1,), (1,)), ((), ()))
    summed = None
    for r in range(2):
        order = range(NZ - 1, -1, -1) if r == 0 else range(NZ)
        levels = [None] * NZ
        passed = jnp.zeros((1, 128), f32)
        for j in order:
            ahead = j < position if r == 0 else j > position
            levels[j] = jnp.where(ahead, got_m[j] + passed, LOWEST)
            passed = passed + jnp.where(ahead, got_f[j], 0.0)
        top = passed
        for j in range(NZ):
            top = jnp.maximum(top, levels[j])
        share = jnp.exp(passed - top)
        memory = share * mem_ref[r]
        norm = share * nrm_ref[r]
        for j in range(NZ):
            share = jnp.exp(levels[j] - top)
            memory = memory + share * got_ref[j, 0:128].astype(f32)
            norm = norm + share * got_n[j]
        high = memory.astype(bf16)
        low = (memory - high.astype(f32)).astype(bf16)
        carried = lax.dot_general(q, high, last, preferred_element_type=f32)
        carried = carried + lax.dot_general(q, low, last, preferred_element_type=f32)
        carried_den = jnp.sum(q_wide * norm, axis=1, keepdims=True)
        b_col = cols_ref[:, 3 * r : 3 * r + 1]
        m_col = cols_ref[:, 3 * r + 1 : 3 * r + 2]
        stab = top[:, 0:1]
        joint = jnp.maximum(stab, m_col)
        carry = jnp.exp(stab - joint)
        keep = jnp.exp(m_col - joint)
        numerator = carry * carried + keep * num_ref[r]
        denominator = carry * carried_den + keep * den_ref[:, r : r + 1]
        floor = jnp.exp(-(b_col + joint))
        part = numerator / jnp.maximum(jnp.abs(denominator), floor)
        summed = part if summed is None else summed + part
    scaled = summed * lax.rsqrt(jnp.mean(summed * summed, axis=-1, keepdims=True) + norm_eps)
    gate = 1.0 / (1.0 + jnp.exp(-o_ref[...].astype(f32)))
    memory_out = (scaled * gain_ref[...] * gate).astype(bf16)
    features = jnp.concatenate([pool_ref[...], memory_out], axis=1)
    result = lax.dot_general(features, in_order(w_ref), last, preferred_element_type=f32)
    core = lax.rem(lax.axis_index("tp"), 2)
    own = keep_ref.shape[1]
    for x in range(keep_ref.shape[0]):
        south = result[2 * x * own : (2 * x + 1) * own]
        north = result[(2 * x + 1) * own : (2 * x + 2) * own]
        keep_ref[x] = jnp.where(core == 0, south, north).astype(bf16)
        give_ref[x] = jnp.where(core == 0, north, south).astype(bf16)


def sds(shape, dtype):
    return jax.ShapeDtypeStruct(shape, dtype)


def call(kernel, outs, scalars, *args, flops=0, scratch=(), specs=None):
    many = isinstance(outs, tuple)
    return pl.pallas_call(
        kernel,
        grid=(1,) if specs else (),
        in_specs=specs or [smem] * len(scalars) + [vmem] * len(args),
        out_specs=(vmem,) * len(outs) if many else vmem,
        out_shape=outs,
        scratch_shapes=list(scratch),
        cost_estimate=pl.CostEstimate(flops=flops, bytes_accessed=0, transcendentals=0),
    )(*scalars, *args)


def per_device(
    tokens,
    norm_gain,
    query_weight,
    key_weight,
    value_weight,
    outgate_weight,
    gate_weight,
    gate_bias,
    decay_extra,
    init_memory,
    init_normalizer,
    head_gain,
    pool_weight,
    mem_out_weight,
    pool_out_weight,
):
    count, width = tokens.shape[1:]
    packed, pool_copies = call(
        pack_kernel, (sds((ROWS, 896), bf16), sds((NZ, ROWS, 256), bf16)), (),
        key_weight, value_weight, query_weight, outgate_weight, pool_weight, mem_out_weight,
        pool_out_weight,
        flops=10**6,
    )
    pool_z = lax.all_to_all(pool_copies, "sp", 0, 0, tiled=True).reshape(NZ * ROWS, 256)
    along_z = lax.all_gather(packed, "sp", axis=0, tiled=True)
    kv_z, pool_z = lax.optimization_barrier((along_z[:, :256], pool_z))
    kv_weight = from_everyone(kv_z, "fs")
    own_tokens, along_z = lax.optimization_barrier((tokens[0], along_z))
    normed, cols, rows, begin, end = call(
        gates_kernel,
        (
            sds((count, width), bf16),
            sds((count, 128), f32),
            sds((8, count), f32),
            sds((HALO, width), bf16),
            sds((HALO, width), bf16),
        ),
        (gate_bias.reshape(4),),
        own_tokens,
        norm_gain[None],
        gate_weight[:, 0],
        decay_extra[0, :, 0][:, None],
        flops=4 * 10**9,
    )
    first_rest, rows = lax.optimization_barrier(
        (jnp.concatenate([pool_z, along_z[:, 256:]], axis=1), rows)
    )
    first_from = {}
    for shift in (1, 3):
        first_from[shift] = from_shift(first_rest, "fs", shift)
    length = lax.axis_size("sp")
    low = lax.ppermute(end, "sp", [(i, i + 1) for i in range(length - 1)])
    high = lax.ppermute(begin, "sp", [(i + 1, i) for i in range(length - 1)])
    k, v, packets = call(
        state_kernel,
        (sds((count, 128), bf16), sds((count, 128), bf16), sds((NZ, PACKET, 128), bf16)),
        (), kv_weight, normed, cols, rows,
        flops=2 * 10**9,
    )
    got = lax.all_to_all(packets, "sp", 0, 0, tiled=True)
    later_rest, k = lax.optimization_barrier((first_rest, k))
    first_from[2] = from_shift(later_rest[:, 384:], "fs", 2)
    last_two = from_shift(later_rest[:, :384], "fs", 2)
    q, outgate, pool_out, nums, dens = call(
        local_kernel,
        (
            sds((count, 128), bf16),
            sds((count, 128), bf16),
            sds((count, 256), bf16),
            sds((2, count, 128), f32),
            sds((count, 128), f32),
        ),
        (), first_rest, *(first_from[s] for s in (1, 2, 3)), normed, low, high,
        norm_gain[None], k, v, cols, rows,
        flops=5 * 10**9,
        scratch=[pltpu.VMEM((NY, NZ * ROWS, 512), bf16)]
        + [pltpu.VMEM((count + 32, 256), f32)] * 2,
    )
    cores = 2
    chips = lax.axis_size("tp") // cores
    own = count // (chips * cores)
    keep, give = call(
        final_kernel, (sds((chips, own, width), bf16),) * 2, (),
        got, init_memory[0, :, 0], init_normalizer[0, :, 0][:, None], cols, q, outgate,
        nums, dens, head_gain, pool_out,
        first_rest, first_from[1], last_two, first_from[3],
        flops=2 * 10**9, specs=[vmem] * 10 + [first_columns] * 4,
        scratch=[pltpu.VMEM((NY, NZ * ROWS, 384), bf16)],
    )
    swap = [(i, i ^ 1) for i in range(chips * cores)]
    taken = lax.ppermute(give, "tp", swap)
    pairs = (keep.astype(f32) + taken.astype(f32)).astype(bf16)
    groups = [list(range(c, chips * cores, cores)) for c in range(cores)]
    parts = lax.all_to_all(pairs, "tp", 0, 0, axis_index_groups=groups, tiled=True)
    mixed = jnp.sum(parts.astype(f32), axis=0).astype(bf16)
    return mixed.reshape(1, own, width)


def solution(mesh):
    placed = (
        P("fs", "sp", None),
        P(),
        P(("sp", "fs"), "tp"),
        P(("sp", "fs"), "tp"),
        P(("sp", "fs"), "tp"),
        P(("sp", "fs"), "tp"),
        P(None, "tp", None),
        P(None, "tp"),
        P("fs", None, "tp", "sp"),
        P("fs", None, "tp", None, None),
        P("fs", None, "tp", None),
        P("tp", None),
        P(("sp", "fs"), "tp"),
        P(("sp", "fs"), "tp"),
        P(("sp", "fs"), "tp"),
    )

    return jax.shard_map(
        per_device,
        mesh=mesh,
        in_specs=placed,
        out_specs=P("fs", ("sp", "tp"), None),
        check_vma=False,
    )
```

```python
import jax
import jax.numpy as jnp
from jax import lax
from jax.experimental import pallas as pl
from jax.experimental.pallas import tpu as pltpu
from jax.sharding import PartitionSpec as P


HALO = 8
norm_eps = 1e-06
NZ = 16
NY = 4
ROWS = 32
LOWEST = -1e30
PACKET = 136

f32 = jnp.float32
bf16 = jnp.bfloat16
smem = pl.BlockSpec(memory_space=pltpu.SMEM)
vmem = pl.BlockSpec(memory_space=pltpu.VMEM)
first_columns = pl.BlockSpec((NZ * ROWS, 384), lambda i: (0, 0), memory_space=pltpu.VMEM)


def from_everyone(x, axis):
    copies = jnp.broadcast_to(x, (lax.axis_size(axis), *x.shape))
    return lax.all_to_all(copies, axis, split_axis=0, concat_axis=0, tiled=True)


def pack_kernel(k_ref, v_ref, q_ref, o_ref, p_ref, m_ref, po_ref, out_ref, copies_ref):
    for z in range(NZ):
        copies_ref[z] = po_ref[...]
    at = 0
    for ref in (k_ref, v_ref, m_ref, q_ref, o_ref, p_ref):
        width = ref.shape[1]
        out_ref[:, at : at + width] = ref[...]
        at += width


def in_order(w_ref):
    return jnp.concatenate(
        [w_ref[y, z * ROWS : (z + 1) * ROWS] for z in range(NZ) for y in range(NY)], axis=0
    )


def from_shift(x, axis, shift):
    count = lax.axis_size(axis)
    return lax.ppermute(x, axis, [(i, (i + shift) % count) for i in range(count)])


def placed_by_source(y, refs, out_ref, lo, hi):
    for shift, ref in enumerate(refs):
        piece = ref[...] if ref.shape[1] == hi - lo else ref[:, lo:hi]
        out_ref[lax.rem(y + NY - shift, NY)] = piece


def rms_normed(x, gain):
    return x * lax.rsqrt(jnp.mean(x * x, axis=-1, keepdims=True) + norm_eps) * gain


def log_sigmoid(x):
    return jnp.minimum(x, 0.0) - jnp.log1p(jnp.exp(-jnp.abs(x)))


def gates_kernel(
    bias_ref, tok_ref, gain_ref, gw_ref, decay_ref, normed_ref, cols_ref, rows_ref,
    begin_ref, end_ref,
):
    x = tok_ref[...].astype(f32)
    begin_ref[...] = tok_ref[:HALO]
    end_ref[...] = tok_ref[tok_ref.shape[0] - HALO :]
    count = x.shape[0]
    normed = rms_normed(x, gain_ref[...]).astype(bf16)
    normed_ref[...] = normed
    pre = lax.dot_general(
        gw_ref[...], normed, (((1,), (1,)), ((), ())), preferred_element_type=f32
    )
    pre = [pre[g : g + 1] + bias_ref[g] for g in range(4)]
    in_rows = (pre[0], pre[2])
    lf_rows = (log_sigmoid(pre[1]) + decay_ref[0], log_sigmoid(pre[3]) + decay_ref[1])
    stacked = jnp.concatenate(
        [in_rows[0], in_rows[1], lf_rows[0], lf_rows[1], jnp.zeros((124, count), f32)], axis=0
    )
    turned = stacked.T
    first = lax.broadcasted_iota(jnp.int32, (count, count), 0)
    second = lax.broadcasted_iota(jnp.int32, (count, count), 1)
    lane = lax.broadcasted_iota(jnp.int32, (count, 128), 1)
    cols = jnp.zeros((count, 128), f32)
    rows = []
    tails = []
    for r in range(2):
        reach = second <= first if r == 0 else second >= first
        reach_t = first <= second if r == 0 else first >= second
        lf_row = lf_rows[r]
        lf_col = turned[:, 2 + r : 3 + r]
        b_col = jnp.sum(jnp.where(reach, lf_row, 0.0), axis=1, keepdims=True)
        b_row = jnp.sum(jnp.where(reach_t, lf_col, 0.0), axis=0, keepdims=True)
        a_row = in_rows[r] - b_row
        a_col = turned[:, r : r + 1] - b_col
        m_col = jnp.max(jnp.where(reach, a_row, LOWEST), axis=1, keepdims=True)
        top = jnp.max(a_row, axis=1, keepdims=True)
        w_col = jnp.exp(a_col - top)
        total = jnp.sum(lf_row, axis=1, keepdims=True)
        for n, col in enumerate((b_col, m_col, w_col)):
            cols = jnp.where(lane == 3 * r + n, col, cols)
        rows.append(a_row)
        tails.append(jnp.broadcast_to(total + top, (1, count)))
        tails.append(jnp.broadcast_to(total, (1, count)))
    cols_ref[...] = cols
    rows_ref[...] = jnp.concatenate(rows + tails + [jnp.zeros((2, count), f32)], axis=0)


def in_three(x):
    high = x.astype(bf16).astype(f32)
    rest = x - high
    mid = rest.astype(bf16).astype(f32)
    low = (rest - mid).astype(bf16).astype(f32)
    return [high, mid, low]


def state_kernel(w_ref, normed_ref, cols_ref, rows_ref, k_ref, v_ref, out_ref):
    position = lax.axis_index("sp")
    weight = in_order(w_ref)
    kv = jnp.dot(normed_ref[...], weight, preferred_element_type=f32).astype(bf16)
    k = kv[:, :128]
    v = kv[:, 128:]
    k_ref[...] = k
    v_ref[...] = v
    scale = 128**-0.5
    k_wide = k.astype(f32)
    v_wide = v.astype(f32)
    packets = []
    for r in range(2):
        w = cols_ref[:, 3 * r + 2 : 3 * r + 3]
        wv = w * v_wide
        high = wv.astype(bf16)
        low = (wv - high.astype(f32)).astype(bf16)
        over_time = (((0,), (0,)), ((), ()))
        memory = lax.dot_general(high, k, over_time, preferred_element_type=f32)
        memory = memory + lax.dot_general(low, k, over_time, preferred_element_type=f32)
        norm = jnp.sum(w * k_wide, axis=0, keepdims=True) * scale
        extra = in_three(norm)
        level = rows_ref[2 + 2 * r : 3 + 2 * r, :128]
        total = rows_ref[3 + 2 * r : 4 + 2 * r, :128]
        lane = lax.broadcasted_iota(jnp.int32, (1, 128), 1)
        extra = extra + in_three(jnp.where(lane < 64, level, total))
        extra = jnp.concatenate(extra + [jnp.zeros((2, 128), f32)], axis=0)
        packets.append(jnp.concatenate([memory * scale, extra], axis=0).astype(bf16))
    for j in range(NZ):

        @pl.when(j > position)
        def _():
            out_ref[j] = packets[0]

        @pl.when(j <= position)
        def _():
            out_ref[j] = packets[1]


def pooled(position, group, centre, low, high, a_ref, b_ref):
    count = centre.shape[0]
    a_ref[0:8] = jnp.zeros_like(a_ref[0:8])
    a_ref[8:16] = low
    a_ref[16 : 16 + count] = centre
    a_ref[16 + count : 24 + count] = high
    a_ref[24 + count : 32 + count] = jnp.zeros_like(a_ref[0:8])
    width = count + 16
    b_ref[...] = jnp.zeros_like(b_ref)
    b_ref[8 : 8 + width] = a_ref[7 : 7 + width] + a_ref[8 : 8 + width]
    total = b_ref[16 : 16 + count]
    refs = (b_ref, a_ref)
    for g in range(1, 4):
        step = 1 << (g - 1)
        src, dst = refs[(g - 1) % 2], refs[g % 2]
        dst[8 : 8 + width] = src[8 - step : 8 - step + width] + src[8 + step : 8 + step + width]
        total = jnp.where(group == g, dst[16 : 16 + count], total)
    left = jnp.left_shift(1, group)
    place = position * count + lax.broadcasted_iota(jnp.int32, (count, 1), 0)
    begin = jnp.maximum(place - left, 0)
    end = jnp.minimum(place + left - 1, NZ * count - 1)
    counted = (end - begin + 1).astype(f32)
    return (total / counted - centre).astype(bf16)


def local_kernel(
    w0_ref, w1_ref, w2_ref, w3_ref, normed_ref, lo_ref, hi_ref, gain_ref,
    k_ref, v_ref, cols_ref, rows_ref,
    q_ref, o_ref, pool_ref, num_ref, den_ref, w_ref, a_ref, b_ref,
):
    placed_by_source(lax.axis_index("fs"), (w0_ref, w1_ref, w2_ref, w3_ref), w_ref, 384, 896)
    weight = in_order(w_ref)
    halo = jnp.concatenate([lo_ref[...], hi_ref[...]], axis=0).astype(f32)
    halo = rms_normed(halo, gain_ref[...]).astype(bf16)
    left = jnp.concatenate([normed_ref[...], halo], axis=0)
    all_three = jnp.dot(left, weight, preferred_element_type=f32).astype(bf16)
    count = normed_ref.shape[0]
    q = all_three[:count, :128]
    q_ref[...] = q
    o_ref[...] = all_three[:count, 128:256]
    p = all_three[:, 256:512].astype(f32)
    pool_ref[...] = pooled(
        lax.axis_index("sp"), lax.div(lax.axis_index("tp"), 2), p[:count], p[count : count + HALO], p[count + HALO :], a_ref, b_ref
    )
    scores = lax.dot_general(
        q, k_ref[...], (((1,), (1,)), ((), ())), preferred_element_type=f32
    ) * (128**-0.5)
    first = lax.broadcasted_iota(jnp.int32, (count, count), 0)
    second = lax.broadcasted_iota(jnp.int32, (count, count), 1)
    lane = lax.broadcasted_iota(jnp.int32, (count, 128), 1)
    dens = jnp.zeros((count, 128), f32)
    for r in range(2):
        reach = second <= first if r == 0 else second >= first
        m_col = cols_ref[:, 3 * r + 1 : 3 * r + 2]
        a_row = rows_ref[r : r + 1]
        weights = jnp.exp(jnp.where(reach, a_row - m_col, LOWEST)) * scores
        num_ref[r] = jnp.dot(weights.astype(bf16), v_ref[...], preferred_element_type=f32)
        dens = jnp.where(lane == r, jnp.sum(weights, axis=1, keepdims=True), dens)
    den_ref[...] = dens


def final_kernel(
    got_ref, mem_ref, nrm_ref, cols_ref, q_ref, o_ref, num_ref, den_ref,
    gain_ref, pool_ref, w0_ref, w1_ref, w2_ref, w3_ref, keep_ref, give_ref, w_ref,
):
    placed_by_source(lax.axis_index("fs"), (w0_ref, w1_ref, w2_ref, w3_ref), w_ref, 0, 384)
    position = lax.axis_index("sp")
    got_n, got_m, got_f = [], [], []
    for j in range(NZ):
        extra = got_ref[j, 128:PACKET].astype(f32)
        got_n.append(extra[0:1] + extra[1:2] + extra[2:3])
        ends = extra[3:4] + extra[4:5] + extra[5:6]
        got_m.append(jnp.broadcast_to(ends[:, 0:1], (1, 128)))
        got_f.append(jnp.broadcast_to(ends[:, 64:65], (1, 128)))
    q = q_ref[...]
    q_wide = q.astype(f32)
    last = (((1,), (1,)), ((), ()))
    summed = None
    for r in range(2):
        order = range(NZ - 1, -1, -1) if r == 0 else range(NZ)
        levels = [None] * NZ
        passed = jnp.zeros((1, 128), f32)
        for j in order:
            ahead = j < position if r == 0 else j > position
            levels[j] = jnp.where(ahead, got_m[j] + passed, LOWEST)
            passed = passed + jnp.where(ahead, got_f[j], 0.0)
        top = passed
        for j in range(NZ):
            top = jnp.maximum(top, levels[j])
        share = jnp.exp(passed - top)
        memory = share * mem_ref[r]
        norm = share * nrm_ref[r]
        for j in range(NZ):
            share = jnp.exp(levels[j] - top)
            memory = memory + share * got_ref[j, 0:128].astype(f32)
            norm = norm + share * got_n[j]
        high = memory.astype(bf16)
        low = (memory - high.astype(f32)).astype(bf16)
        carried = lax.dot_general(q, high, last, preferred_element_type=f32)
        carried = carried + lax.dot_general(q, low, last, preferred_element_type=f32)
        carried_den = jnp.sum(q_wide * norm, axis=1, keepdims=True)
        b_col = cols_ref[:, 3 * r : 3 * r + 1]
        m_col = cols_ref[:, 3 * r + 1 : 3 * r + 2]
        stab = top[:, 0:1]
        joint = jnp.maximum(stab, m_col)
        carry = jnp.exp(stab - joint)
        keep = jnp.exp(m_col - joint)
        numerator = carry * carried + keep * num_ref[r]
        denominator = carry * carried_den + keep * den_ref[:, r : r + 1]
        floor = jnp.exp(-(b_col + joint))
        part = numerator / jnp.maximum(jnp.abs(denominator), floor)
        summed = part if summed is None else summed + part
    scaled = summed * lax.rsqrt(jnp.mean(summed * summed, axis=-1, keepdims=True) + norm_eps)
    gate = 1.0 / (1.0 + jnp.exp(-o_ref[...].astype(f32)))
    memory_out = (scaled * gain_ref[...] * gate).astype(bf16)
    features = jnp.concatenate([pool_ref[...], memory_out], axis=1)
    result = lax.dot_general(features, in_order(w_ref), last, preferred_element_type=f32)
    core = lax.rem(lax.axis_index("tp"), 2)
    chip = lax.div(lax.axis_index("tp"), 2)
    chips, own = keep_ref.shape[:2]
    for x in range(chips):
        south = result[2 * x * own : (2 * x + 1) * own]
        north = result[(2 * x + 1) * own : (2 * x + 2) * own]
        slot = lax.rem(x + chips - chip, chips)
        keep_ref[slot] = jnp.where(core == 0, south, north).astype(bf16)
        give_ref[slot] = jnp.where(core == 0, north, south).astype(bf16)


def sds(shape, dtype):
    return jax.ShapeDtypeStruct(shape, dtype)


def call(kernel, outs, scalars, *args, flops=0, scratch=(), specs=None):
    many = isinstance(outs, tuple)
    return pl.pallas_call(
        kernel,
        grid=(1,) if specs else (),
        in_specs=specs or [smem] * len(scalars) + [vmem] * len(args),
        out_specs=(vmem,) * len(outs) if many else vmem,
        out_shape=outs,
        scratch_shapes=list(scratch),
        cost_estimate=pl.CostEstimate(flops=flops, bytes_accessed=0, transcendentals=0),
    )(*scalars, *args)


def per_device(
    tokens,
    norm_gain,
    query_weight,
    key_weight,
    value_weight,
    outgate_weight,
    gate_weight,
    gate_bias,
    decay_extra,
    init_memory,
    init_normalizer,
    head_gain,
    pool_weight,
    mem_out_weight,
    pool_out_weight,
):
    count, width = tokens.shape[1:]
    packed, pool_copies = call(
        pack_kernel, (sds((ROWS, 896), bf16), sds((NZ, ROWS, 256), bf16)), (),
        key_weight, value_weight, query_weight, outgate_weight, pool_weight, mem_out_weight,
        pool_out_weight,
        flops=10**6,
    )
    pool_z = lax.all_to_all(pool_copies, "sp", 0, 0, tiled=True).reshape(NZ * ROWS, 256)
    along_z = lax.all_gather(packed, "sp", axis=0, tiled=True)
    kv_z, pool_z = lax.optimization_barrier((along_z[:, :256], pool_z))
    kv_weight = from_everyone(kv_z, "fs")
    own_tokens, along_z = lax.optimization_barrier((tokens[0], along_z))
    normed, cols, rows, begin, end = call(
        gates_kernel,
        (
            sds((count, width), bf16),
            sds((count, 128), f32),
            sds((8, count), f32),
            sds((HALO, width), bf16),
            sds((HALO, width), bf16),
        ),
        (gate_bias.reshape(4),),
        own_tokens,
        norm_gain[None],
        gate_weight[:, 0],
        decay_extra[0, :, 0][:, None],
        flops=4 * 10**9,
    )
    first_rest, rows = lax.optimization_barrier(
        (jnp.concatenate([pool_z, along_z[:, 256:]], axis=1), rows)
    )
    first_from = {}
    for shift in (1, 3):
        first_from[shift] = from_shift(first_rest, "fs", shift)
    length = lax.axis_size("sp")
    low = lax.ppermute(end, "sp", [(i, i + 1) for i in range(length - 1)])
    high = lax.ppermute(begin, "sp", [(i + 1, i) for i in range(length - 1)])
    k, v, packets = call(
        state_kernel,
        (sds((count, 128), bf16), sds((count, 128), bf16), sds((NZ, PACKET, 128), bf16)),
        (), kv_weight, normed, cols, rows,
        flops=2 * 10**9,
    )
    got = lax.all_to_all(packets, "sp", 0, 0, tiled=True)
    later_rest, k = lax.optimization_barrier((first_rest, k))
    first_from[2] = from_shift(later_rest[:, 384:], "fs", 2)
    last_two = from_shift(later_rest[:, :384], "fs", 2)
    q, outgate, pool_out, nums, dens = call(
        local_kernel,
        (
            sds((count, 128), bf16),
            sds((count, 128), bf16),
            sds((count, 256), bf16),
            sds((2, count, 128), f32),
            sds((count, 128), f32),
        ),
        (), first_rest, *(first_from[s] for s in (1, 2, 3)), normed, low, high,
        norm_gain[None], k, v, cols, rows,
        flops=5 * 10**9,
        scratch=[pltpu.VMEM((NY, NZ * ROWS, 512), bf16)]
        + [pltpu.VMEM((count + 32, 256), f32)] * 2,
    )
    cores = 2
    chips = lax.axis_size("tp") // cores
    own = count // (chips * cores)
    keep, give = call(
        final_kernel, (sds((chips, own, width), bf16),) * 2, (),
        got, init_memory[0, :, 0], init_normalizer[0, :, 0][:, None], cols, q, outgate,
        nums, dens, head_gain, pool_out,
        first_rest, first_from[1], last_two, first_from[3],
        flops=2 * 10**9, specs=[vmem] * 10 + [first_columns] * 4,
        scratch=[pltpu.VMEM((NY, NZ * ROWS, 384), bf16)],
    )
    swap = [(i, i ^ 1) for i in range(chips * cores)]
    taken = lax.ppermute(give, "tp", swap)
    pairs = [(keep[x].astype(f32) + taken[x].astype(f32)).astype(bf16) for x in range(chips)]
    total = pairs[0].astype(f32)
    for shift in range(1, chips):
        route = [(i, (i + cores * shift) % (chips * cores)) for i in range(chips * cores)]
        total = total + lax.ppermute(pairs[shift], "tp", route).astype(f32)
    mixed = total.astype(bf16)
    return mixed.reshape(1, own, width)


def solution(mesh):
    placed = (
        P("fs", "sp", None),
        P(),
        P(("sp", "fs"), "tp"),
        P(("sp", "fs"), "tp"),
        P(("sp", "fs"), "tp"),
        P(("sp", "fs"), "tp"),
        P(None, "tp", None),
        P(None, "tp"),
        P("fs", None, "tp", "sp"),
        P("fs", None, "tp", None, None),
        P("fs", None, "tp", None),
        P("tp", None),
        P(("sp", "fs"), "tp"),
        P(("sp", "fs"), "tp"),
        P(("sp", "fs"), "tp"),
    )

    return jax.shard_map(
        per_device,
        mesh=mesh,
        in_specs=placed,
        out_specs=P("fs", ("sp", "tp"), None),
        check_vma=False,
    )
```

```python
import jax
import jax.numpy as jnp
from jax import lax
from jax.experimental import pallas as pl
from jax.experimental.pallas import tpu as pltpu
from jax.sharding import PartitionSpec as P


HALO = 8
norm_eps = 1e-06
NZ = 16
NY = 4
ROWS = 32
LOWEST = -1e30
PACKET = 136

f32 = jnp.float32
bf16 = jnp.bfloat16
smem = pl.BlockSpec(memory_space=pltpu.SMEM)
vmem = pl.BlockSpec(memory_space=pltpu.VMEM)
first_columns = pl.BlockSpec((NZ * ROWS, 384), lambda i: (0, 0), memory_space=pltpu.VMEM)


def from_everyone(x, axis):
    copies = jnp.broadcast_to(x, (lax.axis_size(axis), *x.shape))
    return lax.all_to_all(copies, axis, split_axis=0, concat_axis=0, tiled=True)


def pack_kernel(k_ref, v_ref, q_ref, o_ref, p_ref, m_ref, po_ref, out_ref, copies_ref):
    for z in range(NZ):
        copies_ref[z] = po_ref[...]
    at = 0
    for ref in (k_ref, v_ref, m_ref, q_ref, o_ref, p_ref):
        width = ref.shape[1]
        out_ref[:, at : at + width] = ref[...]
        at += width


def in_order(w_ref):
    return jnp.concatenate(
        [w_ref[y, z * ROWS : (z + 1) * ROWS] for z in range(NZ) for y in range(NY)], axis=0
    )


def from_shift(x, axis, shift):
    count = lax.axis_size(axis)
    return lax.ppermute(x, axis, [(i, (i + shift) % count) for i in range(count)])


def placed_by_source(y, refs, out_ref, lo, hi):
    for shift, ref in enumerate(refs):
        piece = ref[...] if ref.shape[1] == hi - lo else ref[:, lo:hi]
        out_ref[lax.rem(y + NY - shift, NY)] = piece


def rms_normed(x, gain):
    return x * lax.rsqrt(jnp.mean(x * x, axis=-1, keepdims=True) + norm_eps) * gain


def log_sigmoid(x):
    return jnp.minimum(x, 0.0) - jnp.log1p(jnp.exp(-jnp.abs(x)))


def gates_kernel(
    bias_ref, tok_ref, gain_ref, gw_ref, decay_ref, normed_ref, cols_ref, rows_ref,
    begin_ref, end_ref,
):
    x = tok_ref[...].astype(f32)
    begin_ref[...] = tok_ref[:HALO]
    end_ref[...] = tok_ref[tok_ref.shape[0] - HALO :]
    count = x.shape[0]
    normed = rms_normed(x, gain_ref[...]).astype(bf16)
    normed_ref[...] = normed
    pre = lax.dot_general(
        gw_ref[...], normed, (((1,), (1,)), ((), ())), preferred_element_type=f32
    )
    pre = [pre[g : g + 1] + bias_ref[g] for g in range(4)]
    in_rows = (pre[0], pre[2])
    lf_rows = (log_sigmoid(pre[1]) + decay_ref[0], log_sigmoid(pre[3]) + decay_ref[1])
    stacked = jnp.concatenate(
        [in_rows[0], in_rows[1], lf_rows[0], lf_rows[1], jnp.zeros((124, count), f32)], axis=0
    )
    turned = stacked.T
    first = lax.broadcasted_iota(jnp.int32, (count, count), 0)
    second = lax.broadcasted_iota(jnp.int32, (count, count), 1)
    lane = lax.broadcasted_iota(jnp.int32, (count, 128), 1)
    cols = jnp.zeros((count, 128), f32)
    rows = []
    tails = []
    for r in range(2):
        reach = second <= first if r == 0 else second >= first
        reach_t = first <= second if r == 0 else first >= second
        lf_row = lf_rows[r]
        lf_col = turned[:, 2 + r : 3 + r]
        b_col = jnp.sum(jnp.where(reach, lf_row, 0.0), axis=1, keepdims=True)
        b_row = jnp.sum(jnp.where(reach_t, lf_col, 0.0), axis=0, keepdims=True)
        a_row = in_rows[r] - b_row
        a_col = turned[:, r : r + 1] - b_col
        m_col = jnp.max(jnp.where(reach, a_row, LOWEST), axis=1, keepdims=True)
        top = jnp.max(a_row, axis=1, keepdims=True)
        w_col = jnp.exp(a_col - top)
        total = jnp.sum(lf_row, axis=1, keepdims=True)
        for n, col in enumerate((b_col, m_col, w_col)):
            cols = jnp.where(lane == 3 * r + n, col, cols)
        rows.append(a_row)
        tails.append(jnp.broadcast_to(total + top, (1, count)))
        tails.append(jnp.broadcast_to(total, (1, count)))
    cols_ref[...] = cols
    rows_ref[...] = jnp.concatenate(rows + tails + [jnp.zeros((2, count), f32)], axis=0)


def in_three(x):
    high = x.astype(bf16).astype(f32)
    rest = x - high
    mid = rest.astype(bf16).astype(f32)
    low = (rest - mid).astype(bf16).astype(f32)
    return [high, mid, low]


def state_kernel(w_ref, normed_ref, cols_ref, rows_ref, k_ref, v_ref, out_ref):
    position = lax.axis_index("sp")
    weight = in_order(w_ref)
    kv = jnp.dot(normed_ref[...], weight, preferred_element_type=f32).astype(bf16)
    k = kv[:, :128]
    v = kv[:, 128:]
    k_ref[...] = k
    v_ref[...] = v
    scale = 128**-0.5
    k_wide = k.astype(f32)
    v_wide = v.astype(f32)
    packets = []
    for r in range(2):
        w = cols_ref[:, 3 * r + 2 : 3 * r + 3]
        wv = w * v_wide
        high = wv.astype(bf16)
        low = (wv - high.astype(f32)).astype(bf16)
        over_time = (((0,), (0,)), ((), ()))
        memory = lax.dot_general(high, k, over_time, preferred_element_type=f32)
        memory = memory + lax.dot_general(low, k, over_time, preferred_element_type=f32)
        norm = jnp.sum(w * k_wide, axis=0, keepdims=True) * scale
        extra = in_three(norm)
        level = rows_ref[2 + 2 * r : 3 + 2 * r, :128]
        total = rows_ref[3 + 2 * r : 4 + 2 * r, :128]
        lane = lax.broadcasted_iota(jnp.int32, (1, 128), 1)
        extra = extra + in_three(jnp.where(lane < 64, level, total))
        extra = jnp.concatenate(extra + [jnp.zeros((2, 128), f32)], axis=0)
        packets.append(jnp.concatenate([memory * scale, extra], axis=0).astype(bf16))
    for j in range(NZ):

        @pl.when(j > position)
        def _():
            out_ref[j] = packets[0]

        @pl.when(j <= position)
        def _():
            out_ref[j] = packets[1]


def pooled(position, group, centre, low, high, a_ref, b_ref):
    count = centre.shape[0]
    a_ref[0:8] = jnp.zeros_like(a_ref[0:8])
    a_ref[8:16] = low
    a_ref[16 : 16 + count] = centre
    a_ref[16 + count : 24 + count] = high
    a_ref[24 + count : 32 + count] = jnp.zeros_like(a_ref[0:8])
    width = count + 16
    b_ref[...] = jnp.zeros_like(b_ref)
    b_ref[8 : 8 + width] = a_ref[7 : 7 + width] + a_ref[8 : 8 + width]
    total = b_ref[16 : 16 + count]
    refs = (b_ref, a_ref)
    for g in range(1, 4):
        step = 1 << (g - 1)
        src, dst = refs[(g - 1) % 2], refs[g % 2]
        dst[8 : 8 + width] = src[8 - step : 8 - step + width] + src[8 + step : 8 + step + width]
        total = jnp.where(group == g, dst[16 : 16 + count], total)
    left = jnp.left_shift(1, group)
    place = position * count + lax.broadcasted_iota(jnp.int32, (count, 1), 0)
    begin = jnp.maximum(place - left, 0)
    end = jnp.minimum(place + left - 1, NZ * count - 1)
    counted = (end - begin + 1).astype(f32)
    return (total / counted - centre).astype(bf16)


def local_kernel(
    w0_ref, w1_ref, w2_ref, w3_ref, normed_ref, lo_ref, hi_ref, gain_ref,
    k_ref, v_ref, cols_ref, rows_ref,
    q_ref, o_ref, pool_ref, num_ref, den_ref, w_ref, a_ref, b_ref,
):
    placed_by_source(lax.axis_index("fs"), (w0_ref, w1_ref, w2_ref, w3_ref), w_ref, 384, 896)
    weight = in_order(w_ref)
    halo = jnp.concatenate([lo_ref[...], hi_ref[...]], axis=0).astype(f32)
    halo = rms_normed(halo, gain_ref[...]).astype(bf16)
    left = jnp.concatenate([normed_ref[...], halo], axis=0)
    all_three = jnp.dot(left, weight, preferred_element_type=f32).astype(bf16)
    count = normed_ref.shape[0]
    q = all_three[:count, :128]
    q_ref[...] = q
    o_ref[...] = all_three[:count, 128:256]
    p = all_three[:, 256:512].astype(f32)
    pool_ref[...] = pooled(
        lax.axis_index("sp"), lax.div(lax.axis_index("tp"), 2), p[:count], p[count : count + HALO], p[count + HALO :], a_ref, b_ref
    )
    scores = lax.dot_general(
        q, k_ref[...], (((1,), (1,)), ((), ())), preferred_element_type=f32
    ) * (128**-0.5)
    first = lax.broadcasted_iota(jnp.int32, (count, count), 0)
    second = lax.broadcasted_iota(jnp.int32, (count, count), 1)
    lane = lax.broadcasted_iota(jnp.int32, (count, 128), 1)
    dens = jnp.zeros((count, 128), f32)
    for r in range(2):
        reach = second <= first if r == 0 else second >= first
        m_col = cols_ref[:, 3 * r + 1 : 3 * r + 2]
        a_row = rows_ref[r : r + 1]
        weights = jnp.exp(jnp.where(reach, a_row - m_col, LOWEST)) * scores
        num_ref[r] = jnp.dot(weights.astype(bf16), v_ref[...], preferred_element_type=f32)
        dens = jnp.where(lane == r, jnp.sum(weights, axis=1, keepdims=True), dens)
    den_ref[...] = dens


def final_kernel(
    got_ref, mem_ref, nrm_ref, cols_ref, q_ref, o_ref, num_ref, den_ref,
    gain_ref, pool_ref, w0_ref, w1_ref, w2_ref, w3_ref, keep_ref, give_ref, w_ref,
):
    placed_by_source(lax.axis_index("fs"), (w0_ref, w1_ref, w2_ref, w3_ref), w_ref, 0, 384)
    position = lax.axis_index("sp")
    got_n, got_m, got_f = [], [], []
    for j in range(NZ):
        extra = got_ref[j, 128:PACKET].astype(f32)
        got_n.append(extra[0:1] + extra[1:2] + extra[2:3])
        ends = extra[3:4] + extra[4:5] + extra[5:6]
        got_m.append(jnp.broadcast_to(ends[:, 0:1], (1, 128)))
        got_f.append(jnp.broadcast_to(ends[:, 64:65], (1, 128)))
    q = q_ref[...]
    q_wide = q.astype(f32)
    last = (((1,), (1,)), ((), ()))
    summed = None
    for r in range(2):
        order = range(NZ - 1, -1, -1) if r == 0 else range(NZ)
        levels = [None] * NZ
        passed = jnp.zeros((1, 128), f32)
        for j in order:
            ahead = j < position if r == 0 else j > position
            levels[j] = jnp.where(ahead, got_m[j] + passed, LOWEST)
            passed = passed + jnp.where(ahead, got_f[j], 0.0)
        top = passed
        for j in range(NZ):
            top = jnp.maximum(top, levels[j])
        share = jnp.exp(passed - top)
        memory = share * mem_ref[r]
        norm = share * nrm_ref[r]
        for j in range(NZ):
            share = jnp.exp(levels[j] - top)
            memory = memory + share * got_ref[j, 0:128].astype(f32)
            norm = norm + share * got_n[j]
        high = memory.astype(bf16)
        low = (memory - high.astype(f32)).astype(bf16)
        carried = lax.dot_general(q, high, last, preferred_element_type=f32)
        carried = carried + lax.dot_general(q, low, last, preferred_element_type=f32)
        carried_den = jnp.sum(q_wide * norm, axis=1, keepdims=True)
        b_col = cols_ref[:, 3 * r : 3 * r + 1]
        m_col = cols_ref[:, 3 * r + 1 : 3 * r + 2]
        stab = top[:, 0:1]
        joint = jnp.maximum(stab, m_col)
        carry = jnp.exp(stab - joint)
        keep = jnp.exp(m_col - joint)
        numerator = carry * carried + keep * num_ref[r]
        denominator = carry * carried_den + keep * den_ref[:, r : r + 1]
        floor = jnp.exp(-(b_col + joint))
        part = numerator / jnp.maximum(jnp.abs(denominator), floor)
        summed = part if summed is None else summed + part
    scaled = summed * lax.rsqrt(jnp.mean(summed * summed, axis=-1, keepdims=True) + norm_eps)
    gate = 1.0 / (1.0 + jnp.exp(-o_ref[...].astype(f32)))
    memory_out = (scaled * gain_ref[...] * gate).astype(bf16)
    features = jnp.concatenate([pool_ref[...], memory_out], axis=1)
    result = lax.dot_general(features, in_order(w_ref), last, preferred_element_type=f32)
    core = lax.rem(lax.axis_index("tp"), 2)
    own = keep_ref.shape[1]
    for x in range(keep_ref.shape[0]):
        south = result[2 * x * own : (2 * x + 1) * own]
        north = result[(2 * x + 1) * own : (2 * x + 2) * own]
        keep_ref[x] = jnp.where(core == 0, south, north).astype(bf16)
        give_ref[x] = jnp.where(core == 0, north, south).astype(bf16)


def sds(shape, dtype):
    return jax.ShapeDtypeStruct(shape, dtype)


def far(shape, dtype):
    return pltpu.HBM(shape, dtype)


def call(kernel, outs, scalars, *args, flops=0, scratch=(), specs=None, close=None):
    many = isinstance(outs, tuple)
    grant = None
    if close is not None:
        grant = 24 * 2**20
        args = [
            pltpu.with_memory_space_constraint(x, pltpu.VMEM if n == close else pltpu.HBM)
            for n, x in enumerate(args)
        ]
    return pl.pallas_call(
        kernel,
        grid=(1,) if specs else (),
        in_specs=specs or [smem] * len(scalars) + [vmem] * len(args),
        out_specs=(vmem,) * len(outs) if many else vmem,
        out_shape=outs,
        scratch_shapes=list(scratch),
        cost_estimate=pl.CostEstimate(flops=flops, bytes_accessed=0, transcendentals=0),
        compiler_params=pltpu.CompilerParams(vmem_limit_bytes=grant),
    )(*scalars, *args)


def per_device(
    tokens,
    norm_gain,
    query_weight,
    key_weight,
    value_weight,
    outgate_weight,
    gate_weight,
    gate_bias,
    decay_extra,
    init_memory,
    init_normalizer,
    head_gain,
    pool_weight,
    mem_out_weight,
    pool_out_weight,
):
    count, width = tokens.shape[1:]
    packed, pool_copies = call(
        pack_kernel, (sds((ROWS, 896), bf16), sds((NZ, ROWS, 256), bf16)), (),
        key_weight, value_weight, query_weight, outgate_weight, pool_weight, mem_out_weight,
        pool_out_weight,
        flops=10**6,
    )
    pool_z = lax.all_to_all(pool_copies, "sp", 0, 0, tiled=True).reshape(NZ * ROWS, 256)
    along_z = lax.all_gather(packed, "sp", axis=0, tiled=True)
    kv_z, pool_z = lax.optimization_barrier((along_z[:, :256], pool_z))
    kv_weight = from_everyone(kv_z, "fs")
    own_tokens, along_z = lax.optimization_barrier((tokens[0], along_z))
    normed, cols, rows, begin, end = call(
        gates_kernel,
        (
            sds((count, width), bf16),
            sds((count, 128), f32),
            sds((8, count), f32),
            sds((HALO, width), bf16),
            sds((HALO, width), bf16),
        ),
        (gate_bias.reshape(4),),
        own_tokens,
        norm_gain[None],
        gate_weight[:, 0],
        decay_extra[0, :, 0][:, None],
        flops=4 * 10**9,
    )
    first_rest, rows = lax.optimization_barrier(
        (jnp.concatenate([pool_z, along_z[:, 256:]], axis=1), rows)
    )
    first_from = {}
    for shift in (1, 3):
        first_from[shift] = from_shift(first_rest, "fs", shift)
    length = lax.axis_size("sp")
    low = lax.ppermute(end, "sp", [(i, i + 1) for i in range(length - 1)])
    high = lax.ppermute(begin, "sp", [(i + 1, i) for i in range(length - 1)])
    k, v, packets = call(
        state_kernel,
        (far((count, 128), bf16), far((count, 128), bf16), far((NZ, PACKET, 128), bf16)),
        (), kv_weight, normed, cols, rows,
        flops=2 * 10**9, close=0,
    )
    got = lax.all_to_all(packets, "sp", 0, 0, tiled=True)
    later_rest, k = lax.optimization_barrier((first_rest, k))
    first_from[2] = from_shift(later_rest[:, 384:], "fs", 2)
    last_two = from_shift(later_rest[:, :384], "fs", 2)
    q, outgate, pool_out, nums, dens = call(
        local_kernel,
        (
            far((count, 128), bf16),
            far((count, 128), bf16),
            far((count, 256), bf16),
            far((2, count, 128), f32),
            far((count, 128), f32),
        ),
        (), first_rest, *(first_from[s] for s in (1, 2, 3)), normed, low, high,
        norm_gain[None], k, v, cols, rows,
        flops=5 * 10**9, close=2,
        scratch=[pltpu.VMEM((NY, NZ * ROWS, 512), bf16)]
        + [pltpu.VMEM((count + 32, 256), f32)] * 2,
    )
    cores = 2
    chips = lax.axis_size("tp") // cores
    own = count // (chips * cores)
    keep, give = call(
        final_kernel, (sds((chips, own, width), bf16),) * 2, (),
        got, init_memory[0, :, 0], init_normalizer[0, :, 0][:, None], cols, q, outgate,
        nums, dens, head_gain, pool_out,
        first_rest, first_from[1], last_two, first_from[3],
        flops=2 * 10**9, close=0, specs=[vmem] * 10 + [first_columns] * 4,
        scratch=[pltpu.VMEM((NY, NZ * ROWS, 384), bf16)],
    )
    swap = [(i, i ^ 1) for i in range(chips * cores)]
    taken = lax.ppermute(give, "tp", swap)
    pairs = (keep.astype(f32) + taken.astype(f32)).astype(bf16)
    groups = [list(range(c, chips * cores, cores)) for c in range(cores)]
    parts = lax.all_to_all(pairs, "tp", 0, 0, axis_index_groups=groups, tiled=True)
    mixed = jnp.sum(parts.astype(f32), axis=0).astype(bf16)
    return mixed.reshape(1, own, width)


def solution(mesh):
    placed = (
        P("fs", "sp", None),
        P(),
        P(("sp", "fs"), "tp"),
        P(("sp", "fs"), "tp"),
        P(("sp", "fs"), "tp"),
        P(("sp", "fs"), "tp"),
        P(None, "tp", None),
        P(None, "tp"),
        P("fs", None, "tp", "sp"),
        P("fs", None, "tp", None, None),
        P("fs", None, "tp", None),
        P("tp", None),
        P(("sp", "fs"), "tp"),
        P(("sp", "fs"), "tp"),
        P(("sp", "fs"), "tp"),
    )

    return jax.shard_map(
        per_device,
        mesh=mesh,
        in_specs=placed,
        out_specs=P("fs", ("sp", "tp"), None),
        check_vma=False,
    )
```

```python
import jax
import jax.numpy as jnp
from jax import lax
from jax.experimental import pallas as pl
from jax.experimental.pallas import tpu as pltpu
from jax.sharding import PartitionSpec as P


HALO = 8
norm_eps = 1e-06
NZ = 16
NY = 4
ROWS = 32
LOWEST = -1e30
PACKET = 136

f32 = jnp.float32
bf16 = jnp.bfloat16
smem = pl.BlockSpec(memory_space=pltpu.SMEM)
vmem = pl.BlockSpec(memory_space=pltpu.VMEM)
first_columns = pl.BlockSpec((NZ * ROWS, 384), lambda i: (0, 0), memory_space=pltpu.VMEM)


def from_everyone(x, axis):
    copies = jnp.broadcast_to(x, (lax.axis_size(axis), *x.shape))
    return lax.all_to_all(copies, axis, split_axis=0, concat_axis=0, tiled=True)


def pack_kernel(k_ref, v_ref, q_ref, o_ref, p_ref, m_ref, po_ref, out_ref, copies_ref):
    for z in range(NZ):
        copies_ref[z] = po_ref[...]
    at = 0
    for ref in (k_ref, v_ref, m_ref, q_ref, o_ref, p_ref):
        width = ref.shape[1]
        out_ref[:, at : at + width] = ref[...]
        at += width


def in_order(w_ref):
    return jnp.concatenate(
        [w_ref[y, z * ROWS : (z + 1) * ROWS] for z in range(NZ) for y in range(NY)], axis=0
    )


def from_shift(x, axis, shift):
    count = lax.axis_size(axis)
    return lax.ppermute(x, axis, [(i, (i + shift) % count) for i in range(count)])


def placed_by_source(y, refs, out_ref, lo, hi):
    for shift, ref in enumerate(refs):
        piece = ref[...] if ref.shape[1] == hi - lo else ref[:, lo:hi]
        out_ref[lax.rem(y + NY - shift, NY)] = piece


def rms_normed(x, gain):
    return x * lax.rsqrt(jnp.mean(x * x, axis=-1, keepdims=True) + norm_eps) * gain


def log_sigmoid(x):
    return jnp.minimum(x, 0.0) - jnp.log1p(jnp.exp(-jnp.abs(x)))


def gates_kernel(
    bias_ref, tok_ref, gain_ref, gw_ref, decay_ref, normed_ref, cols_ref, rows_ref,
    begin_ref, end_ref,
):
    x = tok_ref[...].astype(f32)
    begin_ref[...] = tok_ref[:HALO]
    end_ref[...] = tok_ref[tok_ref.shape[0] - HALO :]
    count = x.shape[0]
    normed = rms_normed(x, gain_ref[...]).astype(bf16)
    normed_ref[...] = normed
    pre = lax.dot_general(
        gw_ref[...], normed, (((1,), (1,)), ((), ())), preferred_element_type=f32
    )
    pre = [pre[g : g + 1] + bias_ref[g] for g in range(4)]
    in_rows = (pre[0], pre[2])
    lf_rows = (log_sigmoid(pre[1]) + decay_ref[0], log_sigmoid(pre[3]) + decay_ref[1])
    stacked = jnp.concatenate(
        [in_rows[0], in_rows[1], lf_rows[0], lf_rows[1], jnp.zeros((124, count), f32)], axis=0
    )
    turned = stacked.T
    first = lax.broadcasted_iota(jnp.int32, (count, count), 0)
    second = lax.broadcasted_iota(jnp.int32, (count, count), 1)
    lane = lax.broadcasted_iota(jnp.int32, (count, 128), 1)
    cols = jnp.zeros((count, 128), f32)
    rows = []
    tails = []
    for r in range(2):
        reach = second <= first if r == 0 else second >= first
        reach_t = first <= second if r == 0 else first >= second
        lf_row = lf_rows[r]
        lf_col = turned[:, 2 + r : 3 + r]
        b_col = jnp.sum(jnp.where(reach, lf_row, 0.0), axis=1, keepdims=True)
        b_row = jnp.sum(jnp.where(reach_t, lf_col, 0.0), axis=0, keepdims=True)
        a_row = in_rows[r] - b_row
        a_col = turned[:, r : r + 1] - b_col
        m_col = jnp.max(jnp.where(reach, a_row, LOWEST), axis=1, keepdims=True)
        top = jnp.max(a_row, axis=1, keepdims=True)
        w_col = jnp.exp(a_col - top)
        total = jnp.sum(lf_row, axis=1, keepdims=True)
        for n, col in enumerate((b_col, m_col, w_col)):
            cols = jnp.where(lane == 3 * r + n, col, cols)
        rows.append(a_row)
        tails.append(jnp.broadcast_to(total + top, (1, count)))
        tails.append(jnp.broadcast_to(total, (1, count)))
    cols_ref[...] = cols
    rows_ref[...] = jnp.concatenate(rows + tails + [jnp.zeros((2, count), f32)], axis=0)


def in_three(x):
    high = x.astype(bf16).astype(f32)
    rest = x - high
    mid = rest.astype(bf16).astype(f32)
    low = (rest - mid).astype(bf16).astype(f32)
    return [high, mid, low]


def state_kernel(w_ref, normed_ref, cols_ref, rows_ref, k_ref, v_ref, out_ref):
    position = lax.axis_index("sp")
    weight = in_order(w_ref)
    kv = jnp.dot(normed_ref[...], weight, preferred_element_type=f32).astype(bf16)
    k = kv[:, :128]
    v = kv[:, 128:]
    k_ref[...] = k
    v_ref[...] = v
    scale = 128**-0.5
    k_wide = k.astype(f32)
    v_wide = v.astype(f32)
    packets = []
    for r in range(2):
        w = cols_ref[:, 3 * r + 2 : 3 * r + 3]
        wv = w * v_wide
        high = wv.astype(bf16)
        low = (wv - high.astype(f32)).astype(bf16)
        over_time = (((0,), (0,)), ((), ()))
        memory = lax.dot_general(high, k, over_time, preferred_element_type=f32)
        memory = memory + lax.dot_general(low, k, over_time, preferred_element_type=f32)
        norm = jnp.sum(w * k_wide, axis=0, keepdims=True) * scale
        extra = in_three(norm)
        level = rows_ref[2 + 2 * r : 3 + 2 * r, :128]
        total = rows_ref[3 + 2 * r : 4 + 2 * r, :128]
        lane = lax.broadcasted_iota(jnp.int32, (1, 128), 1)
        extra = extra + in_three(jnp.where(lane < 64, level, total))
        extra = jnp.concatenate(extra + [jnp.zeros((2, 128), f32)], axis=0)
        packets.append(jnp.concatenate([memory * scale, extra], axis=0).astype(bf16))
    for j in range(NZ):

        @pl.when(j > position)
        def _():
            out_ref[j] = packets[0]

        @pl.when(j <= position)
        def _():
            out_ref[j] = packets[1]


def pooled(position, group, centre, low, high, a_ref, b_ref):
    count = centre.shape[0]
    a_ref[0:8] = jnp.zeros_like(a_ref[0:8])
    a_ref[8:16] = low
    a_ref[16 : 16 + count] = centre
    a_ref[16 + count : 24 + count] = high
    a_ref[24 + count : 32 + count] = jnp.zeros_like(a_ref[0:8])
    width = count + 16
    b_ref[...] = jnp.zeros_like(b_ref)
    b_ref[8 : 8 + width] = a_ref[7 : 7 + width] + a_ref[8 : 8 + width]
    total = b_ref[16 : 16 + count]
    refs = (b_ref, a_ref)
    for g in range(1, 4):
        step = 1 << (g - 1)
        src, dst = refs[(g - 1) % 2], refs[g % 2]
        dst[8 : 8 + width] = src[8 - step : 8 - step + width] + src[8 + step : 8 + step + width]
        total = jnp.where(group == g, dst[16 : 16 + count], total)
    left = jnp.left_shift(1, group)
    place = position * count + lax.broadcasted_iota(jnp.int32, (count, 1), 0)
    begin = jnp.maximum(place - left, 0)
    end = jnp.minimum(place + left - 1, NZ * count - 1)
    counted = (end - begin + 1).astype(f32)
    return (total / counted - centre).astype(bf16)


def local_kernel(
    w0_ref, w1_ref, w2_ref, w3_ref, normed_ref, lo_ref, hi_ref, gain_ref,
    k_ref, v_ref, cols_ref, rows_ref,
    q_ref, o_ref, pool_ref, num_ref, den_ref, w_ref, a_ref, b_ref,
):
    placed_by_source(lax.axis_index("fs"), (w0_ref, w1_ref, w2_ref, w3_ref), w_ref, 384, 896)
    weight = in_order(w_ref)
    halo = jnp.concatenate([lo_ref[...], hi_ref[...]], axis=0).astype(f32)
    halo = rms_normed(halo, gain_ref[...]).astype(bf16)
    left = jnp.concatenate([normed_ref[...], halo], axis=0)
    all_three = jnp.dot(left, weight, preferred_element_type=f32).astype(bf16)
    count = normed_ref.shape[0]
    q = all_three[:count, :128]
    q_ref[...] = q
    o_ref[...] = all_three[:count, 128:256]
    p = all_three[:, 256:512].astype(f32)
    pool_ref[...] = pooled(
        lax.axis_index("sp"), lax.div(lax.axis_index("tp"), 2), p[:count], p[count : count + HALO], p[count + HALO :], a_ref, b_ref
    )
    scores = lax.dot_general(
        q, k_ref[...], (((1,), (1,)), ((), ())), preferred_element_type=f32
    ) * (128**-0.5)
    first = lax.broadcasted_iota(jnp.int32, (count, count), 0)
    second = lax.broadcasted_iota(jnp.int32, (count, count), 1)
    lane = lax.broadcasted_iota(jnp.int32, (count, 128), 1)
    dens = jnp.zeros((count, 128), f32)
    for r in range(2):
        reach = second <= first if r == 0 else second >= first
        m_col = cols_ref[:, 3 * r + 1 : 3 * r + 2]
        a_row = rows_ref[r : r + 1]
        weights = jnp.exp(jnp.where(reach, a_row - m_col, LOWEST)) * scores
        num_ref[r] = jnp.dot(weights.astype(bf16), v_ref[...], preferred_element_type=f32)
        dens = jnp.where(lane == r, jnp.sum(weights, axis=1, keepdims=True), dens)
    den_ref[...] = dens


def final_kernel(
    got_ref, mem_ref, nrm_ref, cols_ref, q_ref, o_ref, num_ref, den_ref,
    gain_ref, pool_ref, w0_ref, w1_ref, w2_ref, w3_ref, out_ref, w_ref,
):
    placed_by_source(lax.axis_index("fs"), (w0_ref, w1_ref, w2_ref, w3_ref), w_ref, 0, 384)
    position = lax.axis_index("sp")
    got_n, got_m, got_f = [], [], []
    for j in range(NZ):
        extra = got_ref[j, 128:PACKET].astype(f32)
        got_n.append(extra[0:1] + extra[1:2] + extra[2:3])
        ends = extra[3:4] + extra[4:5] + extra[5:6]
        got_m.append(jnp.broadcast_to(ends[:, 0:1], (1, 128)))
        got_f.append(jnp.broadcast_to(ends[:, 64:65], (1, 128)))
    q = q_ref[...]
    q_wide = q.astype(f32)
    last = (((1,), (1,)), ((), ()))
    summed = None
    for r in range(2):
        order = range(NZ - 1, -1, -1) if r == 0 else range(NZ)
        levels = [None] * NZ
        passed = jnp.zeros((1, 128), f32)
        for j in order:
            ahead = j < position if r == 0 else j > position
            levels[j] = jnp.where(ahead, got_m[j] + passed, LOWEST)
            passed = passed + jnp.where(ahead, got_f[j], 0.0)
        top = passed
        for j in range(NZ):
            top = jnp.maximum(top, levels[j])
        share = jnp.exp(passed - top)
        memory = share * mem_ref[r]
        norm = share * nrm_ref[r]
        for j in range(NZ):
            share = jnp.exp(levels[j] - top)
            memory = memory + share * got_ref[j, 0:128].astype(f32)
            norm = norm + share * got_n[j]
        high = memory.astype(bf16)
        low = (memory - high.astype(f32)).astype(bf16)
        carried = lax.dot_general(q, high, last, preferred_element_type=f32)
        carried = carried + lax.dot_general(q, low, last, preferred_element_type=f32)
        carried_den = jnp.sum(q_wide * norm, axis=1, keepdims=True)
        b_col = cols_ref[:, 3 * r : 3 * r + 1]
        m_col = cols_ref[:, 3 * r + 1 : 3 * r + 2]
        stab = top[:, 0:1]
        joint = jnp.maximum(stab, m_col)
        carry = jnp.exp(stab - joint)
        keep = jnp.exp(m_col - joint)
        numerator = carry * carried + keep * num_ref[r]
        denominator = carry * carried_den + keep * den_ref[:, r : r + 1]
        floor = jnp.exp(-(b_col + joint))
        part = numerator / jnp.maximum(jnp.abs(denominator), floor)
        summed = part if summed is None else summed + part
    scaled = summed * lax.rsqrt(jnp.mean(summed * summed, axis=-1, keepdims=True) + norm_eps)
    gate = 1.0 / (1.0 + jnp.exp(-o_ref[...].astype(f32)))
    memory_out = (scaled * gain_ref[...] * gate).astype(bf16)
    features = jnp.concatenate([pool_ref[...], memory_out], axis=1)
    result = lax.dot_general(features, in_order(w_ref), last, preferred_element_type=f32)
    out_ref[...] = result.astype(bf16)


def sds(shape, dtype):
    return jax.ShapeDtypeStruct(shape, dtype)


def far(shape, dtype):
    return pltpu.HBM(shape, dtype)


def call(kernel, outs, scalars, *args, flops=0, scratch=(), specs=None, close=-1):
    many = isinstance(outs, tuple)
    args = [
        pltpu.with_memory_space_constraint(x, pltpu.VMEM if n == close else pltpu.HBM)
        for n, x in enumerate(args)
    ]
    return pl.pallas_call(
        kernel,
        grid=(1,) if specs else (),
        in_specs=specs or [smem] * len(scalars) + [vmem] * len(args),
        out_specs=(vmem,) * len(outs) if many else vmem,
        out_shape=outs,
        scratch_shapes=list(scratch),
        cost_estimate=pl.CostEstimate(flops=flops, bytes_accessed=0, transcendentals=0),
        compiler_params=pltpu.CompilerParams(vmem_limit_bytes=24 * 2**20),
    )(*scalars, *args)


def per_device(
    tokens,
    norm_gain,
    query_weight,
    key_weight,
    value_weight,
    outgate_weight,
    gate_weight,
    gate_bias,
    decay_extra,
    init_memory,
    init_normalizer,
    head_gain,
    pool_weight,
    mem_out_weight,
    pool_out_weight,
):
    count, width = tokens.shape[1:]
    packed, pool_copies = call(
        pack_kernel, (sds((ROWS, 896), bf16), sds((NZ, ROWS, 256), bf16)), (),
        key_weight, value_weight, query_weight, outgate_weight, pool_weight, mem_out_weight,
        pool_out_weight,
        flops=10**6,
    )
    pool_z = lax.all_to_all(pool_copies, "sp", 0, 0, tiled=True).reshape(NZ * ROWS, 256)
    along_z = lax.all_gather(packed, "sp", axis=0, tiled=True)
    kv_z, pool_z = lax.optimization_barrier((along_z[:, :256], pool_z))
    kv_weight = from_everyone(kv_z, "fs")
    own_tokens, along_z = lax.optimization_barrier((tokens[0], along_z))
    normed, cols, rows, begin, end = call(
        gates_kernel,
        (
            far((count, width), bf16),
            far((count, 128), f32),
            far((8, count), f32),
            sds((HALO, width), bf16),
            sds((HALO, width), bf16),
        ),
        (gate_bias.reshape(4),),
        own_tokens,
        norm_gain[None],
        gate_weight[:, 0],
        decay_extra[0, :, 0][:, None],
        flops=4 * 10**9,
    )
    first_rest, rows = lax.optimization_barrier(
        (jnp.concatenate([pool_z, along_z[:, 256:]], axis=1), rows)
    )
    first_from = {}
    for shift in (1, 3):
        first_from[shift] = from_shift(first_rest, "fs", shift)
    length = lax.axis_size("sp")
    low = lax.ppermute(end, "sp", [(i, i + 1) for i in range(length - 1)])
    high = lax.ppermute(begin, "sp", [(i + 1, i) for i in range(length - 1)])
    k, v, packets = call(
        state_kernel,
        (far((count, 128), bf16), far((count, 128), bf16), sds((NZ, PACKET, 128), bf16)),
        (), kv_weight, normed, cols, rows,
        flops=2 * 10**9, close=0,
    )
    got = lax.all_to_all(packets, "sp", 0, 0, tiled=True)
    later_rest, k = lax.optimization_barrier((first_rest, k))
    first_from[2] = from_shift(later_rest[:, 384:], "fs", 2)
    last_two = from_shift(later_rest[:, :384], "fs", 2)
    q, outgate, pool_out, nums, dens = call(
        local_kernel,
        (
            far((count, 128), bf16),
            far((count, 128), bf16),
            far((count, 256), bf16),
            far((2, count, 128), f32),
            far((count, 128), f32),
        ),
        (), first_rest, *(first_from[s] for s in (1, 2, 3)), normed, low, high,
        norm_gain[None], k, v, cols, rows,
        flops=5 * 10**9, close=2,
        scratch=[pltpu.VMEM((NY, NZ * ROWS, 512), bf16)]
        + [pltpu.VMEM((count + 32, 256), f32)] * 2,
    )
    own = count // lax.axis_size("tp")
    partial = call(
        final_kernel, sds((count, width), bf16), (),
        got, init_memory[0, :, 0], init_normalizer[0, :, 0][:, None], cols, q, outgate,
        nums, dens, head_gain, pool_out,
        first_rest, first_from[1], last_two, first_from[3],
        flops=2 * 10**9, close=0, specs=[vmem] * 10 + [first_columns] * 4,
        scratch=[pltpu.VMEM((NY, NZ * ROWS, 384), bf16)],
    )
    parts = lax.all_to_all(partial.reshape(-1, own, width), "tp", 0, 0, tiled=True)
    mixed = jnp.sum(parts.astype(f32), axis=0).astype(bf16)
    return mixed.reshape(1, own, width)


def solution(mesh):
    placed = (
        P("fs", "sp", None),
        P(),
        P(("sp", "fs"), "tp"),
        P(("sp", "fs"), "tp"),
        P(("sp", "fs"), "tp"),
        P(("sp", "fs"), "tp"),
        P(None, "tp", None),
        P(None, "tp"),
        P("fs", None, "tp", "sp"),
        P("fs", None, "tp", None, None),
        P("fs", None, "tp", None),
        P("tp", None),
        P(("sp", "fs"), "tp"),
        P(("sp", "fs"), "tp"),
        P(("sp", "fs"), "tp"),
    )

    return jax.shard_map(
        per_device,
        mesh=mesh,
        in_specs=placed,
        out_specs=P("fs", ("sp", "tp"), None),
        check_vma=False,
    )
```

```python
import jax
import jax.numpy as jnp
from jax import lax
from jax.experimental import pallas as pl
from jax.experimental.pallas import tpu as pltpu
from jax.sharding import PartitionSpec as P


HALO = 8
norm_eps = 1e-06
NZ = 16
NY = 4
ROWS = 32
LOWEST = -1e30
PACKET = 136

f32 = jnp.float32
bf16 = jnp.bfloat16
smem = pl.BlockSpec(memory_space=pltpu.SMEM)
vmem = pl.BlockSpec(memory_space=pltpu.VMEM)
first_columns = pl.BlockSpec((NZ * ROWS, 384), lambda i: (0, 0), memory_space=pltpu.VMEM)


def from_everyone(x, axis):
    copies = jnp.broadcast_to(x, (lax.axis_size(axis), *x.shape))
    return lax.all_to_all(copies, axis, split_axis=0, concat_axis=0, tiled=True)


def pack_kernel(k_ref, v_ref, q_ref, o_ref, p_ref, m_ref, po_ref, out_ref, copies_ref):
    for z in range(NZ):
        copies_ref[z] = po_ref[...]
    at = 0
    for ref in (k_ref, v_ref, m_ref, q_ref, o_ref, p_ref):
        width = ref.shape[1]
        out_ref[:, at : at + width] = ref[...]
        at += width


def in_order(w_ref):
    return jnp.concatenate(
        [w_ref[y, z * ROWS : (z + 1) * ROWS] for z in range(NZ) for y in range(NY)], axis=0
    )


def from_shift(x, axis, shift):
    count = lax.axis_size(axis)
    return lax.ppermute(x, axis, [(i, (i + shift) % count) for i in range(count)])


def placed_by_source(y, refs, out_ref, lo, hi):
    for shift, ref in enumerate(refs):
        piece = ref[...] if ref.shape[1] == hi - lo else ref[:, lo:hi]
        out_ref[lax.rem(y + NY - shift, NY)] = piece


def rms_normed(x, gain):
    return x * lax.rsqrt(jnp.mean(x * x, axis=-1, keepdims=True) + norm_eps) * gain


def log_sigmoid(x):
    return jnp.minimum(x, 0.0) - jnp.log1p(jnp.exp(-jnp.abs(x)))


def gates_kernel(
    bias_ref, tok_ref, gain_ref, gw_ref, decay_ref, normed_ref, cols_ref, rows_ref,
    begin_ref, end_ref,
):
    x = tok_ref[...].astype(f32)
    begin_ref[...] = tok_ref[:HALO]
    end_ref[...] = tok_ref[tok_ref.shape[0] - HALO :]
    count = x.shape[0]
    normed = rms_normed(x, gain_ref[...]).astype(bf16)
    normed_ref[...] = normed
    pre = lax.dot_general(
        gw_ref[...], normed, (((1,), (1,)), ((), ())), preferred_element_type=f32
    )
    pre = [pre[g : g + 1] + bias_ref[g] for g in range(4)]
    in_rows = (pre[0], pre[2])
    lf_rows = (log_sigmoid(pre[1]) + decay_ref[0], log_sigmoid(pre[3]) + decay_ref[1])
    stacked = jnp.concatenate(
        [in_rows[0], in_rows[1], lf_rows[0], lf_rows[1], jnp.zeros((124, count), f32)], axis=0
    )
    turned = stacked.T
    first = lax.broadcasted_iota(jnp.int32, (count, count), 0)
    second = lax.broadcasted_iota(jnp.int32, (count, count), 1)
    lane = lax.broadcasted_iota(jnp.int32, (count, 128), 1)
    cols = jnp.zeros((count, 128), f32)
    rows = []
    tails = []
    for r in range(2):
        reach = second <= first if r == 0 else second >= first
        reach_t = first <= second if r == 0 else first >= second
        lf_row = lf_rows[r]
        lf_col = turned[:, 2 + r : 3 + r]
        b_col = jnp.sum(jnp.where(reach, lf_row, 0.0), axis=1, keepdims=True)
        b_row = jnp.sum(jnp.where(reach_t, lf_col, 0.0), axis=0, keepdims=True)
        a_row = in_rows[r] - b_row
        a_col = turned[:, r : r + 1] - b_col
        m_col = jnp.max(jnp.where(reach, a_row, LOWEST), axis=1, keepdims=True)
        top = jnp.max(a_row, axis=1, keepdims=True)
        w_col = jnp.exp(a_col - top)
        total = jnp.sum(lf_row, axis=1, keepdims=True)
        for n, col in enumerate((b_col, m_col, w_col)):
            cols = jnp.where(lane == 3 * r + n, col, cols)
        rows.append(a_row)
        tails.append(jnp.broadcast_to(total + top, (1, count)))
        tails.append(jnp.broadcast_to(total, (1, count)))
    cols_ref[...] = cols
    rows_ref[...] = jnp.concatenate(rows + tails + [jnp.zeros((2, count), f32)], axis=0)


def in_three(x):
    high = x.astype(bf16).astype(f32)
    rest = x - high
    mid = rest.astype(bf16).astype(f32)
    low = (rest - mid).astype(bf16).astype(f32)
    return [high, mid, low]


def state_kernel(w_ref, normed_ref, cols_ref, rows_ref, k_ref, v_ref, out_ref):
    position = lax.axis_index("sp")
    weight = in_order(w_ref)
    kv = jnp.dot(normed_ref[...], weight, preferred_element_type=f32).astype(bf16)
    k = kv[:, :128]
    v = kv[:, 128:]
    k_ref[...] = k
    v_ref[...] = v
    scale = 128**-0.5
    k_wide = k.astype(f32)
    v_wide = v.astype(f32)
    packets = []
    for r in range(2):
        w = cols_ref[:, 3 * r + 2 : 3 * r + 3]
        wv = w * v_wide
        high = wv.astype(bf16)
        low = (wv - high.astype(f32)).astype(bf16)
        over_time = (((0,), (0,)), ((), ()))
        memory = lax.dot_general(high, k, over_time, preferred_element_type=f32)
        memory = memory + lax.dot_general(low, k, over_time, preferred_element_type=f32)
        norm = jnp.sum(w * k_wide, axis=0, keepdims=True) * scale
        extra = in_three(norm)
        level = rows_ref[2 + 2 * r : 3 + 2 * r, :128]
        total = rows_ref[3 + 2 * r : 4 + 2 * r, :128]
        lane = lax.broadcasted_iota(jnp.int32, (1, 128), 1)
        extra = extra + in_three(jnp.where(lane < 64, level, total))
        extra = jnp.concatenate(extra + [jnp.zeros((2, 128), f32)], axis=0)
        packets.append(jnp.concatenate([memory * scale, extra], axis=0).astype(bf16))
    for j in range(NZ):

        @pl.when(j > position)
        def _():
            out_ref[j] = packets[0]

        @pl.when(j <= position)
        def _():
            out_ref[j] = packets[1]


def pooled(position, group, centre, low, high, a_ref, b_ref):
    count = centre.shape[0]
    a_ref[0:8] = jnp.zeros_like(a_ref[0:8])
    a_ref[8:16] = low
    a_ref[16 : 16 + count] = centre
    a_ref[16 + count : 24 + count] = high
    a_ref[24 + count : 32 + count] = jnp.zeros_like(a_ref[0:8])
    width = count + 16
    b_ref[...] = jnp.zeros_like(b_ref)
    b_ref[8 : 8 + width] = a_ref[7 : 7 + width] + a_ref[8 : 8 + width]
    total = b_ref[16 : 16 + count]
    refs = (b_ref, a_ref)
    for g in range(1, 4):
        step = 1 << (g - 1)
        src, dst = refs[(g - 1) % 2], refs[g % 2]
        dst[8 : 8 + width] = src[8 - step : 8 - step + width] + src[8 + step : 8 + step + width]
        total = jnp.where(group == g, dst[16 : 16 + count], total)
    left = jnp.left_shift(1, group)
    place = position * count + lax.broadcasted_iota(jnp.int32, (count, 1), 0)
    begin = jnp.maximum(place - left, 0)
    end = jnp.minimum(place + left - 1, NZ * count - 1)
    counted = (end - begin + 1).astype(f32)
    return (total / counted - centre).astype(bf16)


def local_kernel(
    w0_ref, w1_ref, w2_ref, w3_ref, normed_ref, lo_ref, hi_ref, gain_ref,
    k_ref, v_ref, cols_ref, rows_ref,
    q_ref, o_ref, pool_ref, num_ref, den_ref, w_ref, a_ref, b_ref,
):
    placed_by_source(lax.axis_index("fs"), (w0_ref, w1_ref, w2_ref, w3_ref), w_ref, 384, 896)
    weight = in_order(w_ref)
    halo = jnp.concatenate([lo_ref[...], hi_ref[...]], axis=0).astype(f32)
    halo = rms_normed(halo, gain_ref[...]).astype(bf16)
    left = jnp.concatenate([normed_ref[...], halo], axis=0)
    all_three = jnp.dot(left, weight, preferred_element_type=f32).astype(bf16)
    count = normed_ref.shape[0]
    q = all_three[:count, :128]
    q_ref[...] = q
    o_ref[...] = all_three[:count, 128:256]
    p = all_three[:, 256:512].astype(f32)
    pool_ref[...] = pooled(
        lax.axis_index("sp"), lax.div(lax.axis_index("tp"), 2), p[:count], p[count : count + HALO], p[count + HALO :], a_ref, b_ref
    )
    scores = lax.dot_general(
        q, k_ref[...], (((1,), (1,)), ((), ())), preferred_element_type=f32
    ) * (128**-0.5)
    first = lax.broadcasted_iota(jnp.int32, (count, count), 0)
    second = lax.broadcasted_iota(jnp.int32, (count, count), 1)
    lane = lax.broadcasted_iota(jnp.int32, (count, 128), 1)
    dens = jnp.zeros((count, 128), f32)
    for r in range(2):
        reach = second <= first if r == 0 else second >= first
        m_col = cols_ref[:, 3 * r + 1 : 3 * r + 2]
        a_row = rows_ref[r : r + 1]
        weights = jnp.exp(jnp.where(reach, a_row - m_col, LOWEST)) * scores
        num_ref[r] = jnp.dot(weights.astype(bf16), v_ref[...], preferred_element_type=f32)
        dens = jnp.where(lane == r, jnp.sum(weights, axis=1, keepdims=True), dens)
    den_ref[...] = dens


def final_kernel(
    got_ref, mem_ref, nrm_ref, cols_ref, q_ref, o_ref, num_ref, den_ref,
    gain_ref, pool_ref, w0_ref, w1_ref, w2_ref, w3_ref, keep_ref, give_ref, w_ref,
):
    placed_by_source(lax.axis_index("fs"), (w0_ref, w1_ref, w2_ref, w3_ref), w_ref, 0, 384)
    position = lax.axis_index("sp")
    got_n, got_m, got_f = [], [], []
    for j in range(NZ):
        extra = got_ref[j, 128:PACKET].astype(f32)
        got_n.append(extra[0:1] + extra[1:2] + extra[2:3])
        ends = extra[3:4] + extra[4:5] + extra[5:6]
        got_m.append(jnp.broadcast_to(ends[:, 0:1], (1, 128)))
        got_f.append(jnp.broadcast_to(ends[:, 64:65], (1, 128)))
    q = q_ref[...]
    q_wide = q.astype(f32)
    last = (((1,), (1,)), ((), ()))
    summed = None
    for r in range(2):
        order = range(NZ - 1, -1, -1) if r == 0 else range(NZ)
        levels = [None] * NZ
        passed = jnp.zeros((1, 128), f32)
        for j in order:
            ahead = j < position if r == 0 else j > position
            levels[j] = jnp.where(ahead, got_m[j] + passed, LOWEST)
            passed = passed + jnp.where(ahead, got_f[j], 0.0)
        top = passed
        for j in range(NZ):
            top = jnp.maximum(top, levels[j])
        share = jnp.exp(passed - top)
        memory = share * mem_ref[r]
        norm = share * nrm_ref[r]
        for j in range(NZ):
            share = jnp.exp(levels[j] - top)
            memory = memory + share * got_ref[j, 0:128].astype(f32)
            norm = norm + share * got_n[j]
        high = memory.astype(bf16)
        low = (memory - high.astype(f32)).astype(bf16)
        carried = lax.dot_general(q, high, last, preferred_element_type=f32)
        carried = carried + lax.dot_general(q, low, last, preferred_element_type=f32)
        carried_den = jnp.sum(q_wide * norm, axis=1, keepdims=True)
        b_col = cols_ref[:, 3 * r : 3 * r + 1]
        m_col = cols_ref[:, 3 * r + 1 : 3 * r + 2]
        stab = top[:, 0:1]
        joint = jnp.maximum(stab, m_col)
        carry = jnp.exp(stab - joint)
        keep = jnp.exp(m_col - joint)
        numerator = carry * carried + keep * num_ref[r]
        denominator = carry * carried_den + keep * den_ref[:, r : r + 1]
        floor = jnp.exp(-(b_col + joint))
        part = numerator / jnp.maximum(jnp.abs(denominator), floor)
        summed = part if summed is None else summed + part
    scaled = summed * lax.rsqrt(jnp.mean(summed * summed, axis=-1, keepdims=True) + norm_eps)
    gate = 1.0 / (1.0 + jnp.exp(-o_ref[...].astype(f32)))
    memory_out = (scaled * gain_ref[...] * gate).astype(bf16)
    features = jnp.concatenate([pool_ref[...], memory_out], axis=1)
    result = lax.dot_general(features, in_order(w_ref), last, preferred_element_type=f32)
    core = lax.rem(lax.axis_index("tp"), 2)
    own = keep_ref.shape[1]
    for x in range(keep_ref.shape[0]):
        south = result[2 * x * own : (2 * x + 1) * own]
        north = result[(2 * x + 1) * own : (2 * x + 2) * own]
        keep_ref[x] = jnp.where(core == 0, south, north).astype(bf16)
        give_ref[x] = jnp.where(core == 0, north, south).astype(bf16)


def sds(shape, dtype):
    return jax.ShapeDtypeStruct(shape, dtype)


def far(shape, dtype):
    return pltpu.HBM(shape, dtype)


def call(kernel, outs, scalars, *args, flops=0, scratch=(), specs=None, close=-1):
    many = isinstance(outs, tuple)
    args = [
        pltpu.with_memory_space_constraint(x, pltpu.VMEM if n == close else pltpu.HBM)
        for n, x in enumerate(args)
    ]
    return pl.pallas_call(
        kernel,
        grid=(1,) if specs else (),
        in_specs=specs or [smem] * len(scalars) + [vmem] * len(args),
        out_specs=(vmem,) * len(outs) if many else vmem,
        out_shape=outs,
        scratch_shapes=list(scratch),
        cost_estimate=pl.CostEstimate(flops=flops, bytes_accessed=0, transcendentals=0),
        compiler_params=pltpu.CompilerParams(vmem_limit_bytes=24 * 2**20),
    )(*scalars, *args)


def per_device(
    tokens,
    norm_gain,
    query_weight,
    key_weight,
    value_weight,
    outgate_weight,
    gate_weight,
    gate_bias,
    decay_extra,
    init_memory,
    init_normalizer,
    head_gain,
    pool_weight,
    mem_out_weight,
    pool_out_weight,
):
    count, width = tokens.shape[1:]
    packed, pool_copies = call(
        pack_kernel, (sds((ROWS, 896), bf16), sds((NZ, ROWS, 256), bf16)), (),
        key_weight, value_weight, query_weight, outgate_weight, pool_weight, mem_out_weight,
        pool_out_weight,
        flops=10**6,
    )
    pool_z = lax.all_to_all(pool_copies, "sp", 0, 0, tiled=True).reshape(NZ * ROWS, 256)
    own_tokens, packed = lax.optimization_barrier((tokens[0], packed))
    normed, cols, rows, begin, end = call(
        gates_kernel,
        (
            far((count, width), bf16),
            far((count, 128), f32),
            far((8, count), f32),
            sds((HALO, width), bf16),
            sds((HALO, width), bf16),
        ),
        (gate_bias.reshape(4),),
        own_tokens,
        norm_gain[None],
        gate_weight[:, 0],
        decay_extra[0, :, 0][:, None],
        flops=4 * 10**9,
    )
    packed, normed = lax.optimization_barrier((packed, normed))
    along_z = lax.all_gather(packed, "sp", axis=0, tiled=True)
    kv_z, pool_z = lax.optimization_barrier((along_z[:, :256], pool_z))
    kv_weight = from_everyone(kv_z, "fs")
    first_rest, rows = lax.optimization_barrier(
        (jnp.concatenate([pool_z, along_z[:, 256:]], axis=1), rows)
    )
    first_from = {}
    for shift in (1, 3):
        first_from[shift] = from_shift(first_rest, "fs", shift)
    length = lax.axis_size("sp")
    low = lax.ppermute(end, "sp", [(i, i + 1) for i in range(length - 1)])
    high = lax.ppermute(begin, "sp", [(i + 1, i) for i in range(length - 1)])
    k, v, packets = call(
        state_kernel,
        (far((count, 128), bf16), far((count, 128), bf16), sds((NZ, PACKET, 128), bf16)),
        (), kv_weight, normed, cols, rows,
        flops=2 * 10**9, close=0,
    )
    got = lax.all_to_all(packets, "sp", 0, 0, tiled=True)
    later_rest, k = lax.optimization_barrier((first_rest, k))
    first_from[2] = from_shift(later_rest[:, 384:], "fs", 2)
    last_two = from_shift(later_rest[:, :384], "fs", 2)
    q, outgate, pool_out, nums, dens = call(
        local_kernel,
        (
            far((count, 128), bf16),
            far((count, 128), bf16),
            far((count, 256), bf16),
            far((2, count, 128), f32),
            far((count, 128), f32),
        ),
        (), first_rest, *(first_from[s] for s in (1, 2, 3)), normed, low, high,
        norm_gain[None], k, v, cols, rows,
        flops=5 * 10**9, close=2,
        scratch=[pltpu.VMEM((NY, NZ * ROWS, 512), bf16)]
        + [pltpu.VMEM((count + 32, 256), f32)] * 2,
    )
    cores = 2
    chips = lax.axis_size("tp") // cores
    own = count // (chips * cores)
    keep, give = call(
        final_kernel, (sds((chips, own, width), bf16),) * 2, (),
        got, init_memory[0, :, 0], init_normalizer[0, :, 0][:, None], cols, q, outgate,
        nums, dens, head_gain, pool_out,
        first_rest, first_from[1], last_two, first_from[3],
        flops=2 * 10**9, close=0, specs=[vmem] * 10 + [first_columns] * 4,
        scratch=[pltpu.VMEM((NY, NZ * ROWS, 384), bf16)],
    )
    swap = [(i, i ^ 1) for i in range(chips * cores)]
    taken = lax.ppermute(give, "tp", swap)
    pairs = (keep.astype(f32) + taken.astype(f32)).astype(bf16)
    groups = [list(range(c, chips * cores, cores)) for c in range(cores)]
    parts = lax.all_to_all(pairs, "tp", 0, 0, axis_index_groups=groups, tiled=True)
    mixed = jnp.sum(parts.astype(f32), axis=0).astype(bf16)
    return mixed.reshape(1, own, width)


def solution(mesh):
    placed = (
        P("fs", "sp", None),
        P(),
        P(("sp", "fs"), "tp"),
        P(("sp", "fs"), "tp"),
        P(("sp", "fs"), "tp"),
        P(("sp", "fs"), "tp"),
        P(None, "tp", None),
        P(None, "tp"),
        P("fs", None, "tp", "sp"),
        P("fs", None, "tp", None, None),
        P("fs", None, "tp", None),
        P("tp", None),
        P(("sp", "fs"), "tp"),
        P(("sp", "fs"), "tp"),
        P(("sp", "fs"), "tp"),
    )

    return jax.shard_map(
        per_device,
        mesh=mesh,
        in_specs=placed,
        out_specs=P("fs", ("sp", "tp"), None),
        check_vma=False,
    )
```
